32 devices in a mesh: sp: 4 (over z), fs: 4 (over y, core), tp: 2 (over x).
Axes of the slice: x: 2, y: 2, z: 4, core: 2. Of those that a mesh axis runs over, the one named last changes fastest.
Arguments:
- tokens: bfloat16 [4, 768, 2048], P('fs', 'sp'), may hold values from -6 to 6
- decay_pace: float32 [4, 768], P('fs', 'sp'), may hold values from 0.5 to 2, as said below
- start_state: float32 [4, 16, 64, 64], P('fs', 'tp'), may hold values from -80 to 80
- norm_gain: float32 [2048], replicated, may hold values from 0.1 to 1.9
- conv_value: bfloat16 [2048, 512], P(('sp', 'fs'), 'tp'), may hold values from -0.125 to 0.125
- conv_admit: bfloat16 [2048, 512], P(('sp', 'fs'), 'tp'), may hold values from -0.125 to 0.125
- conv_gate: bfloat16 [2048, 512], P(('sp', 'fs'), 'tp'), may hold values from -0.125 to 0.125
- state_query: bfloat16 [2048, 1024], P(('sp', 'fs'), 'tp'), may hold values from -0.125 to 0.125
- state_key: bfloat16 [2048, 1024], P(('sp', 'fs'), 'tp'), may hold values from -0.125 to 0.125
- state_value: bfloat16 [2048, 1024], P(('sp', 'fs'), 'tp'), may hold values from -0.125 to 0.125
- state_decay: bfloat16 [2048, 1024], P(('sp', 'fs'), 'tp'), may hold values from -0.125 to 0.125
- state_gate: bfloat16 [2048, 1024], P(('sp', 'fs'), 'tp'), may hold values from -0.125 to 0.125
- conv_taps: float32 [31, 512], P(None, 'tp'), may hold values from -4 to 4
- conv_gain: float32 [512], P('tp'), may hold values from 0.1 to 1.9
- point_weight: bfloat16 [512, 512], replicated, may hold values from -0.25 to 0.25
- decay_base: float32 [1024], P('tp'), may hold values from -13 to -3
- correction: float32 [1024], P('tp'), may hold values from 0 to 0.9
- group_gain: float32 [1024], P('tp'), may hold values from 0.1 to 1.9
- output_conv: bfloat16 [512, 2048], P('tp', ('sp', 'fs')), may hold values from -0.25 to 0.25
- output_state: bfloat16 [1024, 2048], P('tp', ('sp', 'fs')), may hold values from -0.1875 to 0.1875
Outputs:
- mixed: bfloat16 [4, 768, 2048], P('fs', ('sp', 'tp'))
The draws below stay inside these ranges and needn't reach their ends.
Inputs may be any that keep to these rules, and one draw needn't show every extreme that they name: `decay_pace`: constant over runs of positions, a quarter of 192 long.
All inputs are finite; a program needn't handle non-finite values.
Results may differ from the reference program's by a relative error of at most 0.017.
Values may be sent and summed in bfloat16 or wider, within the bound.
A program may use at most 64 MiB of HBM per device.

```python
import jax
import jax.numpy as jnp
from jax import lax

D = 2048
CB = 512
C_HEADS = 16
HEAD = 64
KERNEL = 31
TOK_DEV = 192
C = 1024
SEQ = 768
SEQS = 4


def log_uniform(key, shape, lower, upper):
    fraction = jax.random.uniform(key, shape, jnp.float32)
    return jnp.exp(jnp.log(lower) + fraction * (jnp.log(upper) - jnp.log(lower)))


def fast_channels(key):
    picks = jax.random.randint(jax.random.fold_in(key, 11), (C_HEADS,), 0, 10)
    chosen = picks < 5
    return jnp.repeat(chosen, HEAD)


def draw_decay_base(key, part):
    fast = fast_channels(key)
    slow_rate = log_uniform(jax.random.fold_in(key, 3), (C,), 0.15, 0.8) / SEQ
    fast_rate = log_uniform(jax.random.fold_in(key, 4), (C,), 0.012, 0.04)
    return jnp.clip(jnp.log(jnp.where(fast, fast_rate, slow_rate)), -13.0, -3.0)


def draw_correction(key, part):
    fast = fast_channels(key)
    slow_value = jnp.minimum(log_uniform(jax.random.fold_in(key, 5), (C,), 0.1, 0.6) * HEAD / SEQ, 0.9)
    fast_value = jax.random.uniform(jax.random.fold_in(key, 6), (C,), jnp.float32, 0.2, 0.9)
    return jnp.where(fast, fast_value, slow_value)


def draw_decay_pace(key, part):
    stretch = max(TOK_DEV // 4, 1)
    values = log_uniform(key, (SEQS, SEQ // stretch), 0.5, 2.0)
    return jnp.repeat(values, stretch, axis=1)


def draw_conv_taps(key, part):
    group = max(CB // 16, 1)
    factor = log_uniform(jax.random.fold_in(key, 8), (CB // group,), 1.0 / 3.0, 3.0)
    taps = jax.random.normal(jax.random.fold_in(key, 9), (KERNEL, CB), jnp.float32) * KERNEL ** (-0.5)
    return jnp.clip(taps * jnp.repeat(factor, group)[None, :], -4.0, 4.0)


def block_levels(key, shape, split, low, top_value):
    gain, own = 1.0, jax.random.fold_in(key, 6)
    for axis_at, blocks in split:
        heights = jnp.exp(jax.random.uniform(jax.random.fold_in(own, axis_at), (blocks,), jnp.float32, low / len(split), top_value / len(split)))
        gain = gain * jnp.repeat(heights, shape[axis_at] // blocks).reshape([-1 if axis == axis_at else 1 for axis in range(len(shape))])
    return gain


def bell_draw(stream_key, shape, scale, reach, shards=(), held_as=jnp.bfloat16):
    loudness = block_levels(stream_key, shape, shards, -0.22, 0.18) if shards else 1.0
    values = jax.random.normal(stream_key, shape, jnp.float32) * scale * loudness
    return jnp.minimum(jnp.maximum(values, -reach), reach).astype(held_as)


def setup_inputs(seed: int = 0) -> dict:
    seeds = jax.random.split(jax.random.key(seed), 21)
    return {
        "tokens": bell_draw(seeds[0], (SEQS, SEQ, D), 1.0, 6.0, ((0, 4), (1, 4))),
        "decay_pace": draw_decay_pace(jax.random.fold_in(seeds[20], 71), 0),
        "start_state": bell_draw(seeds[2], (SEQS, C_HEADS, HEAD, HEAD), (0.5 * SEQ ** 0.5), 80.0, ((0, 4), (1, 2)), jnp.float32),
        "norm_gain": jnp.clip(1.0 + 0.18 * jax.random.normal(seeds[3], (D,), jnp.float32), 0.1, 1.9),
        "conv_value": bell_draw(seeds[4], (D, CB), D ** -0.5, 0.125, ((0, 16), (1, 2))),
        "conv_admit": bell_draw(seeds[5], (D, CB), D ** -0.5, 0.125, ((0, 16), (1, 2))),
        "conv_gate": bell_draw(seeds[6], (D, CB), D ** -0.5, 0.125, ((0, 16), (1, 2))),
        "state_query": bell_draw(seeds[7], (D, C), D ** -0.5, 0.125, ((0, 16), (1, 2))),
        "state_key": bell_draw(seeds[8], (D, C), D ** -0.5, 0.125, ((0, 16), (1, 2))),
        "state_value": bell_draw(seeds[9], (D, C), D ** -0.5, 0.125, ((0, 16), (1, 2))),
        "state_decay": bell_draw(seeds[10], (D, C), D ** -0.5, 0.125, ((0, 16), (1, 2))),
        "state_gate": bell_draw(seeds[11], (D, C), D ** -0.5, 0.125, ((0, 16), (1, 2))),
        "conv_taps": draw_conv_taps(jax.random.fold_in(seeds[20], 71), 0),
        "conv_gain": jnp.clip(1.0 + 0.18 * jax.random.normal(seeds[13], (CB,), jnp.float32), 0.1, 1.9),
        "point_weight": bell_draw(seeds[14], (CB, CB), CB ** -0.5, 0.25),
        "decay_base": draw_decay_base(jax.random.fold_in(seeds[20], 71), 0),
        "correction": draw_correction(jax.random.fold_in(seeds[20], 71), 0),
        "group_gain": jnp.clip(1.0 + 0.18 * jax.random.normal(seeds[17], (C,), jnp.float32), 0.1, 1.9),
        "output_conv": bell_draw(seeds[18], (CB, D), CB ** -0.5, 0.25, ((0, 2), (1, 16))),
        "output_state": bell_draw(seeds[19], (C, D), C ** -0.5, 0.1875, ((0, 2), (1, 16))),
    }


NORM_FLOOR = 0.1
CHANNEL_FLOOR = 0.1
GROUP_FLOOR = 1.0

def project(normed_rows, weight, shape):
    return jnp.dot(normed_rows, weight, preferred_element_type=jnp.float32).astype(jnp.bfloat16).reshape(shape)

def reference(tokens, decay_pace, start_state, norm_gain, conv_value, conv_admit, conv_gate, state_query, state_key, state_value, state_decay, state_gate, conv_taps, conv_gain, point_weight, decay_base, correction, group_gain, output_conv, output_state):
    seqs, length, width = tokens.shape
    floats = tokens.astype(jnp.float32)
    inverse = lax.rsqrt(lax.optimization_barrier(jnp.mean(floats * floats, axis=-1, keepdims=True)) + NORM_FLOOR)
    normed = (floats * inverse * norm_gain).astype(jnp.bfloat16).reshape(seqs * length, width)
    conv_shape = (seqs, length, CB)
    value = project(normed, conv_value, conv_shape).astype(jnp.float32)
    admit = project(normed, conv_admit, conv_shape).astype(jnp.float32)
    gate_conv = project(normed, conv_gate, conv_shape).astype(jnp.float32)
    rounded = lax.optimization_barrier((value * jax.nn.sigmoid(admit)).astype(jnp.bfloat16))
    conv_input = rounded.astype(jnp.float32)
    padded = jnp.pad(conv_input, ((0, 0), (KERNEL - 1, 0), (0, 0)))
    conv_sum = jnp.zeros(conv_shape, jnp.float32)
    for offset in range(KERNEL):
        conv_sum = conv_sum + conv_taps[offset] * padded[:, offset:offset + length]
    mean = lax.optimization_barrier(jnp.mean(conv_sum, axis=-1, keepdims=True))
    spread = lax.optimization_barrier(jnp.mean(conv_sum * conv_sum, axis=-1, keepdims=True)) - mean * mean
    shaped = jax.nn.silu((conv_sum - mean) * lax.rsqrt(spread + CHANNEL_FLOOR) * conv_gain).astype(jnp.bfloat16)
    pointwise = jnp.dot(shaped.reshape(-1, CB), point_weight, preferred_element_type=jnp.float32).reshape(conv_shape)
    conv_out = (pointwise * jax.nn.silu(gate_conv)).astype(jnp.bfloat16)
    head_shape = (seqs, length, C_HEADS, HEAD)
    query = project(normed, state_query, head_shape).astype(jnp.float32)
    keys = project(normed, state_key, head_shape).astype(jnp.float32)
    values = project(normed, state_value, head_shape).astype(jnp.float32)
    decay_in = project(normed, state_decay, (seqs, length, C)).astype(jnp.float32)
    gate_state = project(normed, state_gate, (seqs, length, C)).astype(jnp.float32)
    log_keep = -jnp.exp(decay_base + jnp.tanh(decay_in)) * decay_pace[:, :, None]
    keep = jnp.exp(log_keep).reshape(head_shape)
    unit = keys * lax.rsqrt(jnp.maximum(lax.optimization_barrier(jnp.sum(keys * keys, axis=-1, keepdims=True)), 1.0))
    remove = -unit
    write = unit * correction.reshape(C_HEADS, HEAD)

    def advance(state, inputs):
        query_now, keep_now, key_now, value_now, remove_now, write_now = inputs
        removed = jnp.einsum('shvk,shk->shv', state, remove_now, precision=lax.Precision.HIGHEST)
        state = state * keep_now[:, :, None, :] + removed[..., None] * write_now[:, :, None, :] + value_now[..., None] * key_now[:, :, None, :]
        return (state, jnp.einsum('shvk,shk->shv', state, query_now, precision=lax.Precision.HIGHEST))
    inputs = tuple((jnp.moveaxis(array, 1, 0) for array in (query, keep, keys, values, remove, write)))
    final_state, outputs = lax.scan(advance, start_state.astype(jnp.float32), inputs)
    outputs = jnp.moveaxis(outputs, 0, 1)
    centered = outputs - lax.optimization_barrier(jnp.mean(outputs, axis=-1, keepdims=True))
    variance = lax.optimization_barrier(jnp.mean(centered * centered, axis=-1, keepdims=True))
    grouped = centered * lax.rsqrt(variance + GROUP_FLOOR) * group_gain.reshape(C_HEADS, HEAD)
    state_out = (grouped.reshape(seqs, length, C) * jax.nn.silu(gate_state)).astype(jnp.bfloat16)
    joined = jnp.concatenate([conv_out, state_out], axis=-1).reshape(seqs * length, CB + C)
    weight = jnp.concatenate([output_conv, output_state], axis=0)
    mixed = jnp.dot(joined, weight, preferred_element_type=jnp.float32).astype(jnp.bfloat16)
    return mixed.reshape(seqs, length, width)
```

```python
import functools

import jax
import jax.numpy as jnp
from jax import lax
from jax.experimental import pallas as pl
from jax.experimental.pallas import tpu as pltpu
from jax.sharding import PartitionSpec as P

NORM_FLOOR = 0.1
CHANNEL_FLOOR = 0.1
GROUP_FLOOR = 1.0


def passed_along(value, axis, steps):
    count = lax.axis_size(axis)
    leading, last = (max(0, -steps), min(count, count - steps))
    return lax.ppermute(value, axis, [(source, source + steps) for source in range(leading, last)])


def entering_2(value, axis, join, neutral):
    place = lax.axis_index(axis)
    gathered = jax.tree.map(
        lambda a, kind: lax.all_gather(a.astype(kind), axis),
        value,
        jax.tree.map(lambda a: jnp.bfloat16 if a.dtype == jnp.float32 else a.dtype, value),
    )
    state = jax.tree.map(lambda a, e: jnp.zeros_like(a) + jnp.asarray(e, a.dtype), value, neutral)

    def one(lap, state):
        return join(
            state,
            jax.tree.map(
                lambda a, own: lax.dynamic_index_in_dim(a, lap, 0, False).astype(own.dtype),
                gathered,
                value,
            ),
        )

    return lax.fori_loop(0, place, one, state)


def apply_map(matrix, right):
    return jnp.einsum("hbti,hbic->hbtc", matrix, right, precision=lax.Precision.HIGHEST)


def pair_terms(left, right, mask):
    return jnp.einsum("hbtc,hbic->hbti", left, right, precision=lax.Precision.HIGHEST) * mask


def compose(earlier, later):
    first = jnp.matmul(earlier[0], later[0], precision=lax.Precision.HIGHEST)
    second = jnp.matmul(earlier[1], later[0], precision=lax.Precision.HIGHEST) + later[1]
    return (first, second)


def block_terms(query, keys, values, unit, write, log_keep):
    size = query.shape[-1]
    span = query.shape[2]
    total_log = jnp.cumsum(log_keep, axis=2)
    before_log = total_log - log_keep
    last_log = total_log[:, :, span - 1 :, :]
    lead_remove = -unit * jnp.exp(before_log)
    lead_query = query * jnp.exp(total_log)
    back_write = write * jnp.exp(-total_log)
    back_key = keys * jnp.exp(-total_log)
    places = jnp.arange(span)
    strict = (places[:, None] > places[None, :]).astype(jnp.float32)
    weak = (places[:, None] >= places[None, :]).astype(jnp.float32)
    remove_write = pair_terms(lead_remove, back_write, strict)
    remove_key = pair_terms(lead_remove, back_key, strict)
    query_write = pair_terms(lead_query, back_write, weak)
    query_key = pair_terms(lead_query, back_key, weak)
    right_side = jnp.concatenate([apply_map(remove_key, values), lead_remove], axis=-1)
    system = jnp.eye(span, dtype=jnp.float32) - remove_write
    solved = jax.scipy.linalg.solve_triangular(system, right_side, lower=True, unit_diagonal=True)
    own_part = solved[..., :size]
    start_part = solved[..., size:]
    local_out = apply_map(query_write, own_part) + apply_map(query_key, values)
    start_map = lead_query + apply_map(query_write, start_part)
    tail_write = write * jnp.exp(last_log - total_log)
    tail_key = keys * jnp.exp(last_log - total_log)
    carry_map = jnp.einsum(
        "hbtk,hbtj->hbkj", start_part, tail_write, precision=lax.Precision.HIGHEST
    ) + jnp.eye(size, dtype=jnp.float32) * jnp.exp(last_log)
    carry_add = jnp.einsum(
        "hbtv,hbtj->hbvj", own_part, tail_write, precision=lax.Precision.HIGHEST
    ) + jnp.einsum("hbtv,hbtj->hbvj", values, tail_key, precision=lax.Precision.HIGHEST)
    return (local_out, start_map, carry_map, carry_add)


def body(
    tokens,
    decay_pace,
    start_state,
    norm_gain,
    conv_value,
    conv_admit,
    conv_gate,
    state_query,
    state_key,
    state_value,
    state_decay,
    state_gate,
    conv_taps,
    conv_gain,
    point_weight,
    decay_base,
    correction,
    group_gain,
    output_conv,
    output_state,
):
    width = tokens.shape[-1]
    rows = tokens.reshape(-1, width)
    length = rows.shape[0]
    floats = rows.astype(jnp.float32)
    inverse = lax.rsqrt(jnp.mean(floats * floats, axis=1, keepdims=True) + NORM_FLOOR)
    normed = (floats * inverse * norm_gain).astype(jnp.bfloat16)
    shards = (
        conv_value,
        conv_admit,
        conv_gate,
        state_query,
        state_key,
        state_value,
        state_decay,
        state_gate,
    )
    stacked = jnp.concatenate(shards, axis=1)
    projected = jnp.dot(
        normed,
        lax.all_gather(stacked, ("sp", "fs"), axis=0, tiled=True),
        preferred_element_type=jnp.float32,
    ).astype(jnp.bfloat16)
    pieces = []
    offset = 0
    for shard in shards:
        pieces.append(projected[:, offset : offset + shard.shape[1]].astype(jnp.float32))
        offset = offset + shard.shape[1]
    value, admit, gate_conv, query, keys, values, decay_in, gate_state = pieces
    channels = value.shape[1]
    kernel = conv_taps.shape[0]
    conv_input = (value * jax.nn.sigmoid(admit)).astype(jnp.bfloat16)
    earlier = passed_along(conv_input[length - (kernel - 1) :], "sp", 1)
    padded = jnp.concatenate([earlier, conv_input], axis=0).astype(jnp.float32)
    conv_sum = jnp.zeros((length, channels), jnp.float32)
    for place in range(kernel):
        conv_sum = conv_sum + conv_taps[place] * padded[place : place + length]
    local_point = lax.dynamic_slice_in_dim(
        point_weight, lax.axis_index("tp") * channels, channels, 1
    )
    whole_sum, whole_gain = (
        lax.all_gather(conv_sum.astype(jnp.bfloat16), "tp", axis=1, tiled=True).astype(
            conv_sum.dtype
        ),
        lax.all_gather(conv_gain.astype(jnp.bfloat16), "tp", axis=0, tiled=True).astype(
            conv_gain.dtype
        ),
    )
    mean = jnp.mean(whole_sum, axis=1, keepdims=True)
    spread = jnp.mean(whole_sum * whole_sum, axis=1, keepdims=True) - mean * mean
    shaped = jax.nn.silu(
        (whole_sum - mean) * lax.rsqrt(spread + CHANNEL_FLOOR) * whole_gain
    ).astype(jnp.bfloat16)
    pointwise = jnp.dot(shaped, local_point, preferred_element_type=jnp.float32)
    conv_out = (pointwise * jax.nn.silu(gate_conv)).astype(jnp.bfloat16)
    size = start_state.shape[-1]
    heads = query.shape[1] // size
    span = min(64, length)
    blocks = length // span
    log_keep = -jnp.exp(decay_base + jnp.tanh(decay_in)) * decay_pace.reshape(-1)[:, None]
    key_heads = keys.reshape(length, heads, size)
    unit = key_heads * lax.rsqrt(
        jnp.maximum(jnp.sum(key_heads * key_heads, axis=-1, keepdims=True), 1.0)
    )
    write = unit * correction.reshape(heads, size)

    def arrange(array):
        return array.reshape(blocks, span, heads, size).transpose(2, 0, 1, 3)

    local_out, start_map, carry_map, carry_add = block_terms(
        arrange(query),
        arrange(keys),
        arrange(values),
        arrange(unit),
        arrange(write),
        arrange(log_keep),
    )
    identity = (
        jnp.broadcast_to(jnp.eye(size, dtype=jnp.float32), (heads, size, size)),
        jnp.zeros((heads, size, size), jnp.float32),
    )

    def along(carried, block_pair):
        return (compose(carried, block_pair), carried)

    device_pair, prefixes = lax.scan(
        along, identity, (jnp.moveaxis(carry_map, 1, 0), jnp.moveaxis(carry_add, 1, 0))
    )
    prior_map, prior_add = entering_2(device_pair, "sp", compose, identity)
    begin = start_state.reshape(heads, size, size)
    entering = jnp.matmul(begin, prior_map, precision=lax.Precision.HIGHEST) + prior_add
    block_starts = (
        jnp.matmul(entering[None], prefixes[0], precision=lax.Precision.HIGHEST) + prefixes[1]
    )
    block_starts = jnp.moveaxis(block_starts, 0, 1)
    outputs = local_out + jnp.einsum(
        "hbtk,hbvk->hbtv", start_map, block_starts, precision=lax.Precision.HIGHEST
    )
    outputs = outputs.transpose(1, 2, 0, 3).reshape(length, heads, size)
    centered = outputs - jnp.mean(outputs, axis=-1, keepdims=True)
    variance = jnp.mean(centered * centered, axis=-1, keepdims=True)
    grouped = centered * lax.rsqrt(variance + GROUP_FLOOR) * group_gain.reshape(heads, size)
    state_out = (grouped.reshape(length, heads * size) * jax.nn.silu(gate_state)).astype(
        jnp.bfloat16
    )
    local_mix = jnp.concatenate([conv_out, state_out], axis=1)
    moved = lax.all_to_all(local_mix, "tp", split_axis=0, concat_axis=1, tiled=True)
    conv_rows, state_rows = (
        lax.all_gather(output_conv, "tp", axis=0, tiled=True),
        lax.all_gather(output_state, "tp", axis=0, tiled=True),
    )
    groups = lax.axis_size("tp")
    joined = jnp.concatenate(
        [conv_rows.reshape(groups, channels, -1), state_rows.reshape(groups, heads * size, -1)],
        axis=1,
    )
    joined = joined.reshape(groups * (channels + heads * size), -1)
    mixed = jnp.dot(
        moved,
        lax.all_gather(joined, ("sp", "fs"), axis=1, tiled=True),
        preferred_element_type=jnp.float32,
    )
    return mixed.astype(jnp.bfloat16).reshape(1, -1, width)


def halves(array):
    high = array.astype(jnp.bfloat16)
    low = (array - high.astype(jnp.float32)).astype(jnp.bfloat16)
    return (high, low)


def product(left, right, dims=((1,), (0,))):
    def one(a, b):
        return lax.dot_general(a, b, (dims, ((), ())), preferred_element_type=jnp.float32)

    return one(left[0], right[0]) + (one(left[0], right[1]) + one(left[1], right[0]))


PIECES = 7
STATES = 5


def layer_kernel(
    span,
    group,
    tokens_ref,
    query_ref,
    key_ref,
    value_ref,
    decay_ref,
    gate_ref,
    conv_value_ref,
    conv_admit_ref,
    conv_gate_ref,
    params_ref,
    begin_ref,
    taps_ref,
    point_ref,
    out_conv_ref,
    out_state_ref,
    out_ref,
    sequence,
    weights,
    packed,
    conv_pack,
    gate_pack,
    paces,
    gains,
    wout,
    proj,
    pace_col,
    local_ref,
    map_ref,
    carry_ref,
    add_ref,
    conv_ref,
    state_buf,
    side_buf,
    joined,
    sides,
    result,
    t_send,
    t_recv,
    x_send,
    x_recv,
    p_send,
    p_recv,
    w_send,
    w_recv,
    y_send,
    y_recv,
    c_send,
    c_recv,
    r_send,
    r_recv,
    g_send,
    g_recv,
    o_send,
    o_recv,
    oz_send,
    oz_recv,
    oy_send,
    oy_recv,
    on_send,
    on_recv,
    or_send,
    or_recv,
    es_send,
    es_recv,
    ec_send,
    ec_recv,
    xs_send,
    xs_recv,
    xc_send,
    xc_recv,
    f_send,
    f_recv,
):
    f32 = jnp.float32
    bf16 = jnp.bfloat16
    along = paces.shape[0]
    place = lax.axis_index("sp")
    seat = lax.axis_index("fs")
    side = lax.axis_index("tp")
    other = 1 - side
    near = seat + 1 - 2 * lax.rem(seat, 2)
    far = lax.rem(seat + 2, 4)
    beyond = lax.rem(near + 2, 4)
    row_y = lax.div(seat, 2)
    mine = lax.rem(seat, 2) == side

    length, width = tokens_ref.shape[1:]
    half = length // 2
    total = along * length
    parts = next(n for n in (3, 2, 1) if half % (16 * n) == 0)
    chunk = half // parts
    depth = query_ref.shape[0]
    wide = query_ref.shape[1] // along
    channels = conv_value_ref.shape[1] // along
    size = begin_ref.shape[-1]
    heads = wide // size
    conv_rows = out_conv_ref.shape[0]
    state_rows = out_state_ref.shape[0]
    joint = conv_rows + state_rows
    columns = out_conv_ref.shape[1]
    conv_at = STATES * wide
    small = paces.shape[2]

    pending = []

    def ahead(steps):
        return lax.rem(place + steps, along)

    def behind(steps):
        return lax.rem(place + along - steps, along)

    def aligned(value, size_of):
        return pl.multiple_of(value * size_of, size_of)

    def remote(source, target, send_sem, recv_sem, where):
        return pltpu.make_async_remote_copy(
            src_ref=source,
            dst_ref=target,
            send_sem=send_sem,
            recv_sem=recv_sem,
            device_id=where,
            device_id_type=pl.DeviceIdType.MESH,
        )

    def guarded(valid, action):
        if valid is None:
            action()
        else:
            pl.when(valid)(action)

    def send(source, target, send_sem, recv_sem, where, valid=None):
        copy = remote(source, target, send_sem, recv_sem, where)
        guarded(valid, copy.start)
        pending.append((valid, copy))

    def arrive(target, send_sem, recv_sem, where, valid=None):
        guarded(valid, remote(target, target, send_sem, recv_sem, where).wait_recv)

    barrier = pltpu.get_barrier_semaphore()
    partners = [{"sp": ahead(s)} for s in range(1, along)]
    partners += [{"fs": near}, {"fs": far}, {"tp": other}]
    for partner in partners:
        pl.semaphore_signal(
            barrier, inc=1, device_id=partner, device_id_type=pl.DeviceIdType.MESH
        )

    state_refs = (query_ref, key_ref, value_ref, decay_ref, gate_ref)

    def rows_of(sp_at, fs_at):
        return pl.ds(aligned(sp_at * 4 + fs_at, depth), depth)

    def packed_of(sp_at, fs_at):
        return pl.ds(aligned(sp_at * 4 + fs_at, depth // 2), depth // 2)

    def own_columns(ref, at):
        return ref[:, pl.ds(aligned(at, wide), wide)]

    for at in range(along):
        cut = slice(at * channels, (at + 1) * channels)
        conv_pack[at] = jnp.concatenate(
            [conv_value_ref[:, cut].astype(f32), conv_admit_ref[:, cut].astype(f32)], axis=1
        ).astype(bf16)
        gate_pack[at] = jnp.concatenate(
            [
                conv_gate_ref[: depth // 2, cut].astype(f32),
                conv_gate_ref[depth // 2 :, cut].astype(f32),
            ],
            axis=1,
        ).astype(bf16)
    own_rows = rows_of(place, seat)
    for at, ref in enumerate(state_refs):
        weights[own_rows, at * wide : (at + 1) * wide] = own_columns(ref, place)
    weights[own_rows, conv_at : conv_at + 2 * channels] = conv_pack[place]
    packed[packed_of(place, seat), :] = gate_pack[place]
    paces[place] = params_ref[:, :small]
    gains[side] = params_ref[:, : gains.shape[2]]

    tile = 32

    def normalise(turn, _):
        floats = tokens_ref[0, pl.ds(aligned(turn, tile), tile), :].astype(f32)
        inverse = lax.rsqrt(jnp.mean(floats * floats, axis=1, keepdims=True) + NORM_FLOOR)
        at = pl.ds(pl.multiple_of(place * length + turn * tile, tile), tile)
        sequence[at, :] = (floats * inverse * params_ref[0:1, :]).astype(bf16)
        return 0

    lax.fori_loop(0, length // tile, normalise, 0)

    def own_block(at):
        return wout.at[:, pl.ds(aligned(at, columns), columns)]

    @pl.when(mine)
    def _():
        at = pl.ds(aligned(place * 2 + row_y, columns), columns)
        wout[pl.ds(aligned(side, joint), conv_rows), at] = out_conv_ref[...]
        wout[pl.ds(pl.multiple_of(side * joint + conv_rows, 16), state_rows), at] = (
            out_state_ref[...]
        )

    pl.semaphore_wait(barrier, len(partners))

    def tokens_at(sp_at, side_at, part):
        first = sp_at * length + side_at * half + part * chunk
        return sequence.at[pl.ds(pl.multiple_of(first, 16), chunk)]

    hops = (
        ({"sp": ahead(1)}, lambda d: place >= d, lambda d: behind(d), place < along - 1),
        ({"sp": behind(1)}, lambda d: place + d < along, lambda d: ahead(d), place > 0),
    )

    for part in range(parts):
        for way, (onward, _, _, open_end) in enumerate(hops):
            here = tokens_at(place, side, part)
            send(here, here, t_send.at[way, 1, part], t_recv.at[way, 1, part], onward, open_end)

    def out_piece(side_at, at):
        cut = pl.ds(aligned(at, columns), columns)
        return (
            wout.at[pl.ds(aligned(side_at, joint), conv_rows), cut],
            wout.at[pl.ds(pl.multiple_of(side_at * joint + conv_rows, 16), state_rows), cut],
        )

    own_at = place * 2 + row_y
    theirs = jnp.logical_not(mine)
    for at, (source, target) in enumerate(zip((out_conv_ref, out_state_ref), out_piece(side, own_at))):
        send(source, target, o_send.at[at], o_recv.at[at], {"tp": other}, theirs)
    own_gain = gains.at[side]
    send(
        params_ref.at[:, pl.ds(0, gains.shape[2])],
        own_gain,
        g_send.at[0],
        g_recv.at[0],
        {"tp": other},
    )

    def piece(sp_at, fs_at, at):
        rows = rows_of(sp_at, fs_at)
        if at < STATES:
            return weights.at[rows, pl.ds(at * wide, wide)]
        if at == STATES:
            return weights.at[rows, pl.ds(conv_at, 2 * channels)]
        return packed.at[packed_of(sp_at, fs_at)]

    groups = ((0, 1, 2, 3), (4, 5), (6,))

    def grouped(sp_at, fs_at, which):
        rows = rows_of(sp_at, fs_at)
        if which == 0:
            return weights.at[rows, pl.ds(0, 4 * wide)]
        if which == 1:
            return weights.at[rows, pl.ds(4 * wide, wide + 2 * channels)]
        return packed.at[packed_of(sp_at, fs_at)]

    def spread(s, which):
        here = grouped(behind(s), seat, which)
        if s > 0:
            for at in groups[which]:
                arrive(
                    piece(behind(s), seat, at), w_send.at[s, at], w_recv.at[s, at], {"sp": ahead(s)}
                )
        send(here, here, y_send.at[s, which], y_recv.at[s, which], {"fs": far})
        send(here, here, c_send.at[s, which], c_recv.at[s, which], {"fs": near})

    def relay(s, which):
        here = grouped(behind(s), far, which)
        arrive(here, y_send.at[s, which], y_recv.at[s, which], {"fs": far})
        send(here, here, r_send.at[s, which], r_recv.at[s, which], {"fs": near})

    for which in range(3):
        spread(0, which)

    def tokens_on(d):
        for part in range(parts):
            for way, (onward, valid, source, open_end) in enumerate(hops):
                here = tokens_at(source(d), side, part)
                arrive(here, t_send.at[way, d, part], t_recv.at[way, d, part], onward, valid(d))
                if d < along - 1:
                    send(
                        here,
                        here,
                        t_send.at[way, d + 1, part],
                        t_recv.at[way, d + 1, part],
                        onward,
                        valid(d) & open_end,
                    )
                send(
                    here,
                    here,
                    x_send.at[way, d, part],
                    x_recv.at[way, d, part],
                    {"tp": other},
                    valid(d),
                )

    order = sorted(range(1, along), key=lambda s: min(s, along - s))
    for d in range(1, along - 1):
        tokens_on(d)
    for s in range(1, along):
        send(
            params_ref.at[:, pl.ds(0, small)],
            paces.at[place],
            p_send.at[s],
            p_recv.at[s],
            {"sp": ahead(s)},
        )
    for which in groups:
        for s in reversed(order):
            for at in which:
                if at < STATES:
                    source = state_refs[at].at[:, pl.ds(aligned(ahead(s), wide), wide)]
                elif at == STATES:
                    source = conv_pack.at[ahead(s)]
                else:
                    source = gate_pack.at[ahead(s)]
                send(
                    source, piece(place, seat, at), w_send.at[s, at], w_recv.at[s, at],
                    {"sp": ahead(s)},
                )
    tokens_on(along - 1)

    tasks = [(s, 0) for s in order] + [(s, which) for s in order for which in (1, 2)]
    late = [(0, which) for which in range(3)]
    for task in tasks:
        spread(*task)
        relay(*late.pop(0))
        late.append(task)
    for task in late:
        relay(*task)

    def out_hop(way, d, valid):
        onward, _, source, open_end = hops[way]
        here = own_block(source(d) * 2 + row_y)
        arrive(here, oz_send.at[way, d], oz_recv.at[way, d], onward, valid)

    for at, target in enumerate(out_piece(other, own_at)):
        arrive(target, o_send.at[at], o_recv.at[at], {"tp": other}, mine)
    here = own_block(own_at)
    for way, (onward, _, _, open_end) in enumerate(hops):
        send(here, here, oz_send.at[way, 1], oz_recv.at[way, 1], onward, mine & open_end)
    send(here, here, oy_send.at[place], oy_recv.at[place], {"fs": far}, mine)
    send(here, here, on_send.at[place], on_recv.at[place], {"fs": near}, mine)

    def out_on(d):
        for way, (onward, valid, source, open_end) in enumerate(hops):
            at = source(d)
            here = own_block(at * 2 + row_y)
            ready = mine & valid(d)
            arrive(here, oz_send.at[way, d], oz_recv.at[way, d], onward, ready)
            if d < along - 1:
                send(
                    here,
                    here,
                    oz_send.at[way, d + 1],
                    oz_recv.at[way, d + 1],
                    onward,
                    ready & open_end,
                )
            send(here, here, oy_send.at[at], oy_recv.at[at], {"fs": far}, ready)
            send(here, here, on_send.at[at], on_recv.at[at], {"fs": near}, ready)

    for s in range(along):
        for which in range(3):
            arrive(
                grouped(behind(s), near, which), c_send.at[s, which], c_recv.at[s, which],
                {"fs": near},
            )
            arrive(
                grouped(behind(s), beyond, which), r_send.at[s, which], r_recv.at[s, which],
                {"fs": near},
            )
    for s in order:
        arrive(paces.at[behind(s)], p_send.at[s], p_recv.at[s], {"sp": ahead(s)})
    for d in range(1, along):
        for part in range(parts):
            for way, (_, valid, source, _) in enumerate(hops):
                arrive(
                    tokens_at(source(d), other, part),
                    x_send.at[way, d, part],
                    x_recv.at[way, d, part],
                    {"tp": other},
                    valid(d),
                )

    gate_at = conv_at + 2 * channels

    def unpack(turn, _):
        both = packed[pl.ds(aligned(turn, depth // 2), depth // 2), :].astype(f32)
        at = pl.ds(aligned(turn, depth), depth // 2)
        weights[at, gate_at : gate_at + channels] = both[:, :channels].astype(bf16)
        at = pl.ds(pl.multiple_of(turn * depth + depth // 2, depth // 2), depth // 2)
        weights[at, gate_at : gate_at + channels] = both[:, channels:].astype(bf16)
        return 0

    lax.fori_loop(0, along * 4, unpack, 0)

    big = next(n for n in (256, 192, 128, 64) if total % n == 0)

    def multiply(turn, _):
        at = pl.ds(aligned(turn, big), big)
        proj[at, :] = jnp.dot(
            sequence[at, :], weights[...], preferred_element_type=f32
        ).astype(bf16)
        return 0

    lax.fori_loop(0, total // big, multiply, 0)

    blocks = total // span
    row = lax.broadcasted_iota(jnp.int32, (span, span), 0)
    col = lax.broadcasted_iota(jnp.int32, (span, span), 1)
    eye = (row == col).astype(f32)
    for at in range(along):
        for part in range(length // span):
            line = paces[at][5:6, part * span : (part + 1) * span]
            first = at * length + part * span
            pace_col[first : first + span, :] = jnp.sum(eye * line, axis=1, keepdims=True)

    kernel = taps_ref.shape[0]
    lead_rows = conv_ref.shape[0] - total
    pair = pl.ds(aligned(lax.div(place * channels, 128), 128), 128)
    both_taps = taps_ref[:, pair]
    taps = jnp.where(
        lax.rem(place * channels, 128) == 0, both_taps[:, :channels], both_taps[:, 128 - channels :]
    )
    conv_ref[0:lead_rows, :] = jnp.zeros((lead_rows, channels), f32)
    for block in range(blocks):
        rows = pl.ds(block * span, span)
        value = proj[rows, conv_at : conv_at + channels].astype(f32)
        admit = proj[rows, conv_at + channels : conv_at + 2 * channels].astype(f32)
        conv_ref[pl.ds(lead_rows + block * span, span), :] = (
            (value * jax.nn.sigmoid(admit)).astype(bf16).astype(f32)
        )
    for block in range(blocks):
        summed = jnp.zeros((span, channels), f32)
        for tap in range(kernel):
            first = lead_rows - (kernel - 1) + block * span + tap
            summed = summed + taps[tap : tap + 1, :] * conv_ref[pl.ds(first, span), :]
        rows = pl.ds(block * span, span)
        gate = proj[rows, gate_at : gate_at + channels].astype(f32)
        side_buf[rows, :] = jnp.concatenate([summed, gate], axis=1).astype(bf16)

    def rows_for(at):
        return pl.ds(at * length, length)

    for at in range(along):
        target = sides.at[side, place]

        @pl.when(place == at)
        def _():
            sides[side, place] = side_buf[rows_for(at), :]

        away = place != at
        send(
            side_buf.at[rows_for(at)], target, ec_send.at[at], ec_recv.at[place], {"sp": at}, away
        )
        send(
            side_buf.at[rows_for(at)],
            target,
            xc_send.at[place],
            xc_recv.at[place],
            {"tp": other},
            place == at,
        )

    begins = [begin_ref[0, place * heads + head] for head in range(heads)]
    own_cut = pl.ds(aligned(place, wide), wide)
    base = params_ref[1:2, own_cut]
    strength = params_ref[2:3, own_cut]
    gain = params_ref[3:4, own_cut]

    strict = (row > col).astype(f32)
    weak = (row >= col).astype(f32)
    masks = jnp.concatenate(
        [jnp.concatenate([strict, strict], axis=1), jnp.concatenate([weak, weak], axis=1)], axis=0
    )
    square = (
        lax.broadcasted_iota(jnp.int32, (size, size), 0)
        == lax.broadcasted_iota(jnp.int32, (size, size), 1)
    ).astype(f32)
    least = min(8, span)
    same = (lax.div(row, least) == lax.div(col, least)).astype(f32)
    merges = []
    reach = least
    while reach < span:
        merges.append(
            (
                (lax.div(row, 2 * reach) == lax.div(col, 2 * reach))
                & (lax.div(row, reach) != lax.div(col, reach))
            ).astype(f32)
        )
        reach = 2 * reach
    weak_bf = weak.astype(bf16)

    def step(turn, _):
        items = []
        for part in range(group):
            block = turn * group + part
            rows = pl.ds(pl.multiple_of(block * span, span), span)
            query = proj[rows, 0:wide].astype(f32)
            keys = proj[rows, wide : 2 * wide].astype(f32)
            values = proj[rows, 2 * wide : 3 * wide].astype(f32)
            decay_in = proj[rows, 3 * wide : 4 * wide].astype(f32)
            log_keep = -jnp.exp(base + jnp.tanh(decay_in)) * pace_col[rows, :]
            high = log_keep.astype(bf16)
            rest = log_keep - high.astype(f32)
            mid = rest.astype(bf16)
            low = (rest - mid.astype(f32)).astype(bf16)
            summed = (
                jnp.dot(weak_bf, high, preferred_element_type=f32)
                + jnp.dot(weak_bf, mid, preferred_element_type=f32)
                + jnp.dot(weak_bf, low, preferred_element_type=f32)
            )
            last = summed[span - 1 : span, :]
            lead = jnp.exp(summed - log_keep)
            grown = jnp.exp(summed)
            back = jnp.exp(-summed)
            tail = jnp.exp(last - summed)
            ended = jnp.exp(last)
            for head in range(heads):
                at = slice(head * size, (head + 1) * size)
                key = keys[:, at]
                unit = key * lax.rsqrt(
                    jnp.maximum(jnp.sum(key * key, axis=1, keepdims=True), 1.0)
                )
                write = unit * strength[:, at]
                lead_remove = -unit * lead[:, at]
                lead_query = query[:, at] * grown[:, at]
                items.append(
                    dict(
                        at=(block, head),
                        value=values[:, at],
                        lead_remove=lead_remove,
                        lead_query=lead_query,
                        left=jnp.concatenate([lead_remove, lead_query], axis=0),
                        right=jnp.concatenate([write * back[:, at], key * back[:, at]], axis=0),
                        tail_write=write * tail[:, at],
                        tail_key=key * tail[:, at],
                        ended=ended[:, at],
                    )
                )
        for item in items:
            item["pair"] = (
                product(halves(item["left"]), halves(item["right"]), ((1,), (1,))) * masks
            )
        for item in items:
            item["system"] = item["pair"][:span, :span]
            item["power"] = halves(item["system"] * same)
            item["inverse"] = eye + item["system"] * same
        reach = 2
        while reach < least:
            for item in items:
                item["power"] = halves(product(item["power"], item["power"]))
            for item in items:
                item["inverse"] = item["inverse"] + product(
                    halves(item["inverse"]), item["power"]
                )
            reach = 2 * reach
        for item in items:
            padded = jnp.concatenate([jnp.zeros_like(item["value"]), item["value"]], axis=0)
            item["mixed"] = product(halves(item["pair"]), halves(padded))
        for merge in merges:
            for item in items:
                item["inside"] = halves(item["inverse"])
                item["next"] = halves(product(halves(item["system"] * merge), item["inside"]))
            for item in items:
                item["inverse"] = item["inverse"] + product(item["inside"], item["next"])
        for item in items:
            right_side = jnp.concatenate([item["mixed"][:span], item["lead_remove"]], axis=1)
            item["solved"] = halves(product(halves(item["inverse"]), halves(right_side)))
        for item in items:
            block, head = item["at"]
            seen = product(halves(item["pair"][span:, :span]), item["solved"])
            local_ref[head, block] = seen[:, :size] + item["mixed"][span:]
            map_ref[head, block] = item["lead_query"] + seen[:, size:]
            carried = product(item["solved"], halves(item["tail_write"]), ((0,), (0,)))
            carry_ref[head, block] = carried[size:] + square * item["ended"]
            add_ref[head, block] = carried[:size] + product(
                halves(item["value"]), halves(item["tail_key"]), ((0,), (0,))
            )
        return 0

    turns = blocks // group
    done = 0
    for d in range(1, along):
        upto = turns * d // (along - 1)
        if upto > done:
            lax.fori_loop(done, upto, step, 0)
            done = upto
        out_on(d)

    for at in range(along):
        ready = mine
        here = own_block(at * 2 + 1 - row_y)
        arrive(here, oy_send.at[at], oy_recv.at[at], {"fs": far}, ready)
        send(here, here, or_send.at[at], or_recv.at[at], {"fs": near}, ready)

    for s in order:
        here = sides.at[side, behind(s)]
        arrive(here, ec_send.at[0], ec_recv.at[behind(s)], {"sp": ahead(s)})
        send(here, here, xc_send.at[behind(s)], xc_recv.at[behind(s)], {"tp": other})

    def joined_at(side_at, sp_at):
        first = side_at * joint + conv_rows + sp_at * wide
        return joined.at[:, pl.ds(pl.multiple_of(first, 128), wide)]

    states = list(begins)
    for block in range(blocks):
        rows = pl.ds(block * span, span)
        gate = proj[rows, 4 * wide : 5 * wide].astype(f32)
        pieces = []
        for head in range(heads):
            state = halves(states[head])
            out = local_ref[head, block] + product(
                halves(map_ref[head, block]), state, ((1,), (1,))
            )
            states[head] = product(state, halves(carry_ref[head, block])) + add_ref[head, block]
            centered = out - jnp.mean(out, axis=1, keepdims=True)
            variance = jnp.mean(centered * centered, axis=1, keepdims=True)
            pieces.append(centered * lax.rsqrt(variance + GROUP_FLOOR))
        scaled = jnp.concatenate(pieces, axis=1) * gain
        state_buf[rows, :] = (scaled * gate * jax.nn.sigmoid(gate)).astype(bf16)
        if (block + 1) * span % length == 0:
            at = (block + 1) * span // length - 1
            target = joined_at(side, place)

            @pl.when(place == at)
            def _():
                joined[:, pl.ds(
                    pl.multiple_of(side * joint + conv_rows + place * wide, 128), wide
                )] = state_buf[rows_for(at), :]

            source = state_buf.at[rows_for(at)]
            send(source, target, es_send.at[at], es_recv.at[place], {"sp": at}, place != at)
            send(
                source,
                target,
                xs_send.at[place],
                xs_recv.at[place],
                {"tp": other},
                place == at,
            )

    for at in range(along):
        arrive(sides.at[other, at], xc_send.at[at], xc_recv.at[at], {"tp": other})
    arrive(gains.at[other], g_send.at[0], g_recv.at[0], {"tp": other})
    whole_gain = jnp.concatenate([gains[0][4:5, :], gains[1][4:5, :]], axis=1)
    piece_rows = next(n for n in (64, 48, 32, 16) if length % n == 0)

    def convolved(turn, _):
        at = pl.ds(aligned(turn, piece_rows), piece_rows)
        sums = jnp.concatenate(
            [
                sides[s, p, at, 0:channels].astype(f32)
                for s in range(2)
                for p in range(along)
            ],
            axis=1,
        )
        gates = jnp.concatenate(
            [
                sides[s, p, at, channels : 2 * channels].astype(f32)
                for s in range(2)
                for p in range(along)
            ],
            axis=1,
        )
        mean = jnp.mean(sums, axis=1, keepdims=True)
        spread_of = jnp.mean(sums * sums, axis=1, keepdims=True) - mean * mean
        shaped = jax.nn.silu(
            (sums - mean) * lax.rsqrt(spread_of + CHANNEL_FLOOR) * whole_gain
        ).astype(bf16)
        pointwise = jnp.dot(shaped, point_ref[...], preferred_element_type=f32)
        conv_out = (pointwise * jax.nn.silu(gates)).astype(bf16)
        joined[at, 0:conv_rows] = conv_out[:, :conv_rows]
        joined[at, joint : joint + conv_rows] = conv_out[:, conv_rows:]
        return 0

    lax.fori_loop(0, length // piece_rows, convolved, 0)

    for s in order:
        here = joined_at(side, behind(s))
        arrive(here, es_send.at[0], es_recv.at[behind(s)], {"sp": ahead(s)})
        send(here, here, xs_send.at[behind(s)], xs_recv.at[behind(s)], {"tp": other})
    for at in range(along):
        for y_at, (n_send, n_recv) in ((row_y, (on_send, on_recv)), (1 - row_y, (or_send, or_recv))):
            arrive(
                own_block(at * 2 + y_at), n_send.at[at], n_recv.at[at], {"fs": near}, theirs
            )
    for at in range(along):
        arrive(joined_at(other, at), xs_send.at[at], xs_recv.at[at], {"tp": other})

    count = wout.shape[1] // columns
    step_of = 2 if count % 2 == 0 else 1
    ours = pl.ds(pl.multiple_of(side * half, 16), half)
    others = pl.ds(pl.multiple_of(other * half, 16), half)

    def out_cut(at, side_at):
        return pl.ds(aligned(2 * at + side_at, columns), columns)

    for first in range(0, count, step_of):
        cut = slice(first * columns, (first + step_of) * columns)
        result[:, cut] = jnp.dot(
            joined[...], wout[:, cut], preferred_element_type=f32
        ).astype(bf16)
        for at in range(first, first + step_of):
            piece_cut = pl.ds(at * columns, columns)
            send(
                result.at[others, piece_cut],
                out_ref.at[:, out_cut(at, side)],
                f_send.at[at],
                f_recv.at[at],
                {"tp": other},
            )
    for at in range(count):
        out_ref[:, out_cut(at, side)] = result[ours, at * columns : (at + 1) * columns]
    for at in range(count):
        arrive(out_ref.at[:, out_cut(at, other)], f_send.at[at], f_recv.at[at], {"tp": other})
    for valid, copy in pending:
        guarded(valid, copy.wait_send)


def fused_body(
    tokens,
    decay_pace,
    start_state,
    norm_gain,
    conv_value,
    conv_admit,
    conv_gate,
    state_query,
    state_key,
    state_value,
    state_decay,
    state_gate,
    conv_taps,
    conv_gain,
    point_weight,
    decay_base,
    correction,
    group_gain,
    output_conv,
    output_state,
):
    along = lax.axis_size("sp")
    _, length, width = tokens.shape
    depth, wide = state_query.shape[0], state_query.shape[1] // along
    channels = conv_value.shape[1] // along
    size = start_state.shape[-1]
    heads = wide // size
    total = along * length
    span = 64
    blocks = total // span
    group = next(n for n in (4, 3, 2, 1) if blocks % n == 0)
    kernel = conv_taps.shape[0]
    joint = output_conv.shape[0] + output_state.shape[0]
    columns = output_conv.shape[1]
    gain_lanes = conv_gain.shape[0]
    pace_lanes = -(-length // 128) * 128
    lines = [
        norm_gain,
        decay_base,
        correction,
        group_gain,
        conv_gain,
        decay_pace.reshape(-1),
    ]
    params = jnp.stack([jnp.pad(line, (0, width - line.shape[0])) for line in lines])
    params = jnp.pad(params, ((0, 8 - len(lines)), (0, 0)))

    f32, bf16 = jnp.float32, jnp.bfloat16
    half = length // 2
    parts = next(n for n in (3, 2, 1) if half % (16 * n) == 0)
    lead_rows = -(-(kernel - 1) // 8) * 8
    dma = pltpu.SemaphoreType.DMA
    maps = pltpu.VMEM((heads, blocks, size, size), f32)
    owners = wout_blocks = along * 2

    def both(*shape):
        return [dma(shape), dma(shape)]

    mixed = pl.pallas_call(
        functools.partial(layer_kernel, span, group),
        out_shape=jax.ShapeDtypeStruct((half, width), bf16),
        in_specs=[pl.BlockSpec(memory_space=pltpu.VMEM)] * 15,
        out_specs=pl.BlockSpec(memory_space=pltpu.VMEM),
        scratch_shapes=[
            pltpu.VMEM((total, width), bf16),
            pltpu.VMEM((width, 5 * wide + 3 * channels), bf16),
            pltpu.VMEM((width // 2, 2 * channels), bf16),
            pltpu.VMEM((along, depth, 2 * channels), bf16),
            pltpu.VMEM((along, depth // 2, 2 * channels), bf16),
            pltpu.VMEM((along, 8, pace_lanes), f32),
            pltpu.VMEM((2, 8, gain_lanes), f32),
            pltpu.VMEM((2 * joint, wout_blocks * columns), bf16),
            pltpu.VMEM((total, 5 * wide + 3 * channels), bf16),
            pltpu.VMEM((total, 1), f32),
            pltpu.VMEM((heads, blocks, span, size), f32),
            pltpu.VMEM((heads, blocks, span, size), f32),
            maps,
            maps,
            pltpu.VMEM((lead_rows + total, channels), f32),
            pltpu.VMEM((total, wide), bf16),
            pltpu.VMEM((total, 2 * channels), bf16),
            pltpu.VMEM((length, 2 * joint), bf16),
            pltpu.VMEM((2, along, length, 2 * channels), bf16),
            pltpu.VMEM((length, wout_blocks * columns), bf16),
        ]
        + both(2, along, parts)
        + both(2, along, parts)
        + both(along)
        + both(along, PIECES)
        + both(along, 3)
        + both(along, 3)
        + both(along, 3)
        + both(1)
        + both(2)
        + both(2, along)
        + both(along)
        + both(along)
        + both(along)
        + both(along)
        + both(along)
        + both(along)
        + both(along)
        + both(owners),
        compiler_params=pltpu.CompilerParams(
            collective_id=0, has_side_effects=True, vmem_limit_bytes=56 * 1024 * 1024
        ),
        cost_estimate=pl.CostEstimate(
            flops=60_000_000_000, bytes_accessed=8_000_000, transcendentals=0
        ),
        name="layer",
    )(
        tokens,
        state_query,
        state_key,
        state_value,
        state_decay,
        state_gate,
        conv_value,
        conv_admit,
        conv_gate,
        params,
        start_state,
        conv_taps,
        point_weight,
        output_conv,
        output_state,
    )
    return mixed.reshape(1, half, width)


def dispatch(*arrays):
    along = lax.axis_size("sp")
    tokens, start_state, conv_value, query, output_conv, output_state = (
        arrays[0],
        arrays[2],
        arrays[4],
        arrays[7],
        arrays[18],
        arrays[19],
    )
    depth, width = query.shape[0], tokens.shape[2]
    size = start_state.shape[-1]
    fits = (
        along > 2
        and lax.axis_size("fs") == 4
        and lax.axis_size("tp") == 2
        and tokens.shape[1] % 64 == 0
        and tokens.shape[0] == 1
        and start_state.shape[1] % along == 0
        and size == 64
        and query.shape[1] == along * 128
        and conv_value.shape[1] == along * 64
        and depth % 32 == 0
        and depth * along * 4 == width
        and output_conv.shape[0] == along * 64
        and output_state.shape[0] == along * 128
        and output_conv.shape[1] == 128
        and width == along * 4 * 128
    )
    return (fused_body if fits else body)(*arrays)


def solution(mesh):
    return jax.shard_map(
        dispatch,
        mesh=mesh,
        in_specs=(
            P("fs", "sp", None),
            P("fs", "sp"),
            P("fs", "tp", None, None),
            P(),
            P(("sp", "fs"), "tp"),
            P(("sp", "fs"), "tp"),
            P(("sp", "fs"), "tp"),
            P(("sp", "fs"), "tp"),
            P(("sp", "fs"), "tp"),
            P(("sp", "fs"), "tp"),
            P(("sp", "fs"), "tp"),
            P(("sp", "fs"), "tp"),
            P(None, "tp"),
            P("tp"),
            P(),
            P("tp"),
            P("tp"),
            P("tp"),
            P("tp", ("sp", "fs")),
            P("tp", ("sp", "fs")),
        ),
        out_specs=P("fs", ("sp", "tp"), None),
        check_vma=False,
    )
```

```python
import functools

import jax
import jax.numpy as jnp
from jax import lax
from jax.experimental import pallas as pl
from jax.experimental.pallas import tpu as pltpu
from jax.sharding import PartitionSpec as P

NORM_FLOOR = 0.1
CHANNEL_FLOOR = 0.1
GROUP_FLOOR = 1.0


def passed_along(value, axis, steps):
    count = lax.axis_size(axis)
    leading, last = (max(0, -steps), min(count, count - steps))
    return lax.ppermute(value, axis, [(source, source + steps) for source in range(leading, last)])


def entering_2(value, axis, join, neutral):
    place = lax.axis_index(axis)
    gathered = jax.tree.map(
        lambda a, kind: lax.all_gather(a.astype(kind), axis),
        value,
        jax.tree.map(lambda a: jnp.bfloat16 if a.dtype == jnp.float32 else a.dtype, value),
    )
    state = jax.tree.map(lambda a, e: jnp.zeros_like(a) + jnp.asarray(e, a.dtype), value, neutral)

    def one(lap, state):
        return join(
            state,
            jax.tree.map(
                lambda a, own: lax.dynamic_index_in_dim(a, lap, 0, False).astype(own.dtype),
                gathered,
                value,
            ),
        )

    return lax.fori_loop(0, place, one, state)


def apply_map(matrix, right):
    return jnp.einsum("hbti,hbic->hbtc", matrix, right, precision=lax.Precision.HIGHEST)


def pair_terms(left, right, mask):
    return jnp.einsum("hbtc,hbic->hbti", left, right, precision=lax.Precision.HIGHEST) * mask


def compose(earlier, later):
    first = jnp.matmul(earlier[0], later[0], precision=lax.Precision.HIGHEST)
    second = jnp.matmul(earlier[1], later[0], precision=lax.Precision.HIGHEST) + later[1]
    return (first, second)


def block_terms(query, keys, values, unit, write, log_keep):
    size = query.shape[-1]
    span = query.shape[2]
    total_log = jnp.cumsum(log_keep, axis=2)
    before_log = total_log - log_keep
    last_log = total_log[:, :, span - 1 :, :]
    lead_remove = -unit * jnp.exp(before_log)
    lead_query = query * jnp.exp(total_log)
    back_write = write * jnp.exp(-total_log)
    back_key = keys * jnp.exp(-total_log)
    places = jnp.arange(span)
    strict = (places[:, None] > places[None, :]).astype(jnp.float32)
    weak = (places[:, None] >= places[None, :]).astype(jnp.float32)
    remove_write = pair_terms(lead_remove, back_write, strict)
    remove_key = pair_terms(lead_remove, back_key, strict)
    query_write = pair_terms(lead_query, back_write, weak)
    query_key = pair_terms(lead_query, back_key, weak)
    right_side = jnp.concatenate([apply_map(remove_key, values), lead_remove], axis=-1)
    system = jnp.eye(span, dtype=jnp.float32) - remove_write
    solved = jax.scipy.linalg.solve_triangular(system, right_side, lower=True, unit_diagonal=True)
    own_part = solved[..., :size]
    start_part = solved[..., size:]
    local_out = apply_map(query_write, own_part) + apply_map(query_key, values)
    start_map = lead_query + apply_map(query_write, start_part)
    tail_write = write * jnp.exp(last_log - total_log)
    tail_key = keys * jnp.exp(last_log - total_log)
    carry_map = jnp.einsum(
        "hbtk,hbtj->hbkj", start_part, tail_write, precision=lax.Precision.HIGHEST
    ) + jnp.eye(size, dtype=jnp.float32) * jnp.exp(last_log)
    carry_add = jnp.einsum(
        "hbtv,hbtj->hbvj", own_part, tail_write, precision=lax.Precision.HIGHEST
    ) + jnp.einsum("hbtv,hbtj->hbvj", values, tail_key, precision=lax.Precision.HIGHEST)
    return (local_out, start_map, carry_map, carry_add)


def body(
    tokens,
    decay_pace,
    start_state,
    norm_gain,
    conv_value,
    conv_admit,
    conv_gate,
    state_query,
    state_key,
    state_value,
    state_decay,
    state_gate,
    conv_taps,
    conv_gain,
    point_weight,
    decay_base,
    correction,
    group_gain,
    output_conv,
    output_state,
):
    width = tokens.shape[-1]
    rows = tokens.reshape(-1, width)
    length = rows.shape[0]
    floats = rows.astype(jnp.float32)
    inverse = lax.rsqrt(jnp.mean(floats * floats, axis=1, keepdims=True) + NORM_FLOOR)
    normed = (floats * inverse * norm_gain).astype(jnp.bfloat16)
    shards = (
        conv_value,
        conv_admit,
        conv_gate,
        state_query,
        state_key,
        state_value,
        state_decay,
        state_gate,
    )
    stacked = jnp.concatenate(shards, axis=1)
    projected = jnp.dot(
        normed,
        lax.all_gather(stacked, ("sp", "fs"), axis=0, tiled=True),
        preferred_element_type=jnp.float32,
    ).astype(jnp.bfloat16)
    pieces = []
    offset = 0
    for shard in shards:
        pieces.append(projected[:, offset : offset + shard.shape[1]].astype(jnp.float32))
        offset = offset + shard.shape[1]
    value, admit, gate_conv, query, keys, values, decay_in, gate_state = pieces
    channels = value.shape[1]
    kernel = conv_taps.shape[0]
    conv_input = (value * jax.nn.sigmoid(admit)).astype(jnp.bfloat16)
    earlier = passed_along(conv_input[length - (kernel - 1) :], "sp", 1)
    padded = jnp.concatenate([earlier, conv_input], axis=0).astype(jnp.float32)
    conv_sum = jnp.zeros((length, channels), jnp.float32)
    for place in range(kernel):
        conv_sum = conv_sum + conv_taps[place] * padded[place : place + length]
    local_point = lax.dynamic_slice_in_dim(
        point_weight, lax.axis_index("tp") * channels, channels, 1
    )
    whole_sum, whole_gain = (
        lax.all_gather(conv_sum.astype(jnp.bfloat16), "tp", axis=1, tiled=True).astype(
            conv_sum.dtype
        ),
        lax.all_gather(conv_gain.astype(jnp.bfloat16), "tp", axis=0, tiled=True).astype(
            conv_gain.dtype
        ),
    )
    mean = jnp.mean(whole_sum, axis=1, keepdims=True)
    spread = jnp.mean(whole_sum * whole_sum, axis=1, keepdims=True) - mean * mean
    shaped = jax.nn.silu(
        (whole_sum - mean) * lax.rsqrt(spread + CHANNEL_FLOOR) * whole_gain
    ).astype(jnp.bfloat16)
    pointwise = jnp.dot(shaped, local_point, preferred_element_type=jnp.float32)
    conv_out = (pointwise * jax.nn.silu(gate_conv)).astype(jnp.bfloat16)
    size = start_state.shape[-1]
    heads = query.shape[1] // size
    span = min(64, length)
    blocks = length // span
    log_keep = -jnp.exp(decay_base + jnp.tanh(decay_in)) * decay_pace.reshape(-1)[:, None]
    key_heads = keys.reshape(length, heads, size)
    unit = key_heads * lax.rsqrt(
        jnp.maximum(jnp.sum(key_heads * key_heads, axis=-1, keepdims=True), 1.0)
    )
    write = unit * correction.reshape(heads, size)

    def arrange(array):
        return array.reshape(blocks, span, heads, size).transpose(2, 0, 1, 3)

    local_out, start_map, carry_map, carry_add = block_terms(
        arrange(query),
        arrange(keys),
        arrange(values),
        arrange(unit),
        arrange(write),
        arrange(log_keep),
    )
    identity = (
        jnp.broadcast_to(jnp.eye(size, dtype=jnp.float32), (heads, size, size)),
        jnp.zeros((heads, size, size), jnp.float32),
    )

    def along(carried, block_pair):
        return (compose(carried, block_pair), carried)

    device_pair, prefixes = lax.scan(
        along, identity, (jnp.moveaxis(carry_map, 1, 0), jnp.moveaxis(carry_add, 1, 0))
    )
    prior_map, prior_add = entering_2(device_pair, "sp", compose, identity)
    begin = start_state.reshape(heads, size, size)
    entering = jnp.matmul(begin, prior_map, precision=lax.Precision.HIGHEST) + prior_add
    block_starts = (
        jnp.matmul(entering[None], prefixes[0], precision=lax.Precision.HIGHEST) + prefixes[1]
    )
    block_starts = jnp.moveaxis(block_starts, 0, 1)
    outputs = local_out + jnp.einsum(
        "hbtk,hbvk->hbtv", start_map, block_starts, precision=lax.Precision.HIGHEST
    )
    outputs = outputs.transpose(1, 2, 0, 3).reshape(length, heads, size)
    centered = outputs - jnp.mean(outputs, axis=-1, keepdims=True)
    variance = jnp.mean(centered * centered, axis=-1, keepdims=True)
    grouped = centered * lax.rsqrt(variance + GROUP_FLOOR) * group_gain.reshape(heads, size)
    state_out = (grouped.reshape(length, heads * size) * jax.nn.silu(gate_state)).astype(
        jnp.bfloat16
    )
    local_mix = jnp.concatenate([conv_out, state_out], axis=1)
    moved = lax.all_to_all(local_mix, "tp", split_axis=0, concat_axis=1, tiled=True)
    conv_rows, state_rows = (
        lax.all_gather(output_conv, "tp", axis=0, tiled=True),
        lax.all_gather(output_state, "tp", axis=0, tiled=True),
    )
    groups = lax.axis_size("tp")
    joined = jnp.concatenate(
        [conv_rows.reshape(groups, channels, -1), state_rows.reshape(groups, heads * size, -1)],
        axis=1,
    )
    joined = joined.reshape(groups * (channels + heads * size), -1)
    mixed = jnp.dot(
        moved,
        lax.all_gather(joined, ("sp", "fs"), axis=1, tiled=True),
        preferred_element_type=jnp.float32,
    )
    return mixed.astype(jnp.bfloat16).reshape(1, -1, width)


def halves(array):
    high = array.astype(jnp.bfloat16)
    low = (array - high.astype(jnp.float32)).astype(jnp.bfloat16)
    return (high, low)


def product(left, right, dims=((1,), (0,))):
    def one(a, b):
        return lax.dot_general(a, b, (dims, ((), ())), preferred_element_type=jnp.float32)

    return one(left[0], right[0]) + (one(left[0], right[1]) + one(left[1], right[0]))


STATES = 5


def layer_kernel(
    span,
    group,
    tokens_ref,
    query_ref,
    key_ref,
    value_ref,
    decay_ref,
    gate_ref,
    conv_value_ref,
    conv_admit_ref,
    conv_gate_ref,
    norm_gain_ref,
    base_ref,
    strength_ref,
    group_gain_ref,
    conv_gain_ref,
    pace_ref,
    begin_ref,
    taps_ref,
    point_ref,
    out_conv_ref,
    out_state_ref,
    out_ref,
    sequence,
    weights,
    packed,
    conv_pack,
    gate_pack,
    paces,
    gains,
    wout,
    proj,
    pace_col,
    local_ref,
    map_ref,
    carry_ref,
    add_ref,
    conv_ref,
    state_buf,
    side_buf,
    joined,
    sides,
    result,
    t_send,
    t_recv,
    x_send,
    x_recv,
    p_send,
    p_recv,
    w_send,
    w_recv,
    y_send,
    y_recv,
    c_send,
    c_recv,
    r_send,
    r_recv,
    g_send,
    g_recv,
    o_send,
    o_recv,
    oz_send,
    oz_recv,
    oy_send,
    oy_recv,
    on_send,
    on_recv,
    or_send,
    or_recv,
    es_send,
    es_recv,
    ec_send,
    ec_recv,
    xs_send,
    xs_recv,
    xc_send,
    xc_recv,
    f_send,
    f_recv,
    own_sem,
):
    f32 = jnp.float32
    bf16 = jnp.bfloat16
    along = paces.shape[0]
    place = lax.axis_index("sp")
    seat = lax.axis_index("fs")
    side = lax.axis_index("tp")
    other = 1 - side
    near = seat + 1 - 2 * lax.rem(seat, 2)
    far = lax.rem(seat + 2, 4)
    beyond = lax.rem(near + 2, 4)
    row_y = lax.div(seat, 2)
    mine = lax.rem(seat, 2) == side

    length, width = tokens_ref.shape[1:]
    half = length // 2
    total = along * length
    parts = next(n for n in (3, 2, 1) if half % (16 * n) == 0)
    chunk = half // parts
    depth = query_ref.shape[0]
    wide = query_ref.shape[1] // along
    channels = conv_value_ref.shape[1] // along
    size = begin_ref.shape[-1]
    heads = wide // size
    conv_rows = out_conv_ref.shape[0]
    state_rows = out_state_ref.shape[0]
    joint = conv_rows + state_rows
    columns = out_conv_ref.shape[1]
    conv_at = STATES * wide

    pending = []

    def ahead(steps):
        return lax.rem(place + steps, along)

    def behind(steps):
        return lax.rem(place + along - steps, along)

    def aligned(value, size_of):
        return pl.multiple_of(value * size_of, size_of)

    def remote(source, target, send_sem, recv_sem, where):
        return pltpu.make_async_remote_copy(
            src_ref=source,
            dst_ref=target,
            send_sem=send_sem,
            recv_sem=recv_sem,
            device_id=where,
            device_id_type=pl.DeviceIdType.MESH,
        )

    def guarded(valid, action):
        if valid is None:
            action()
        else:
            pl.when(valid)(action)

    def send(source, target, send_sem, recv_sem, where, valid=None, lone=False):
        copy = remote(source, target, send_sem, recv_sem, where)
        guarded(valid, copy.start)
        if lone:
            pending.append((valid, copy))

    def sent(whole, send_sem, where, valid=None):
        pending.append((valid, remote(whole, whole, send_sem, send_sem, where)))

    def arrive(target, send_sem, recv_sem, where, valid=None):
        guarded(valid, remote(target, target, send_sem, recv_sem, where).wait_recv)

    barrier = pltpu.get_barrier_semaphore()
    partners = [{"sp": ahead(s)} for s in range(1, along)]
    partners += [{"fs": near}, {"fs": far}, {"tp": other}]
    for partner in partners:
        pl.semaphore_signal(
            barrier, inc=1, device_id=partner, device_id_type=pl.DeviceIdType.MESH
        )

    state_refs = (query_ref, key_ref, value_ref, decay_ref, gate_ref)

    def rows_of(sp_at, fs_at):
        return pl.ds(aligned(sp_at * 4 + fs_at, depth), depth)

    def packed_of(sp_at, fs_at):
        return pl.ds(aligned(sp_at * 4 + fs_at, depth // 2), depth // 2)

    def own_columns(ref, at):
        return ref[:, pl.ds(aligned(at, wide), wide)]

    for at in range(along):
        cut = slice(at * channels, (at + 1) * channels)
        conv_pack[at] = jnp.concatenate(
            [conv_value_ref[:, cut].astype(f32), conv_admit_ref[:, cut].astype(f32)], axis=1
        ).astype(bf16)
        gate_pack[at] = jnp.concatenate(
            [
                conv_gate_ref[: depth // 2, cut].astype(f32),
                conv_gate_ref[depth // 2 :, cut].astype(f32),
            ],
            axis=1,
        ).astype(bf16)
    own_rows = rows_of(place, seat)
    for at, ref in enumerate(state_refs):
        weights[own_rows, at * wide : (at + 1) * wide] = own_columns(ref, place)
    weights[own_rows, conv_at : conv_at + 2 * channels] = conv_pack[place]
    packed[packed_of(place, seat), :] = gate_pack[place]
    paces[place] = pace_ref[...]
    gains[side] = conv_gain_ref[...]

    tile = 32

    def normalise(turn, _):
        floats = tokens_ref[0, pl.ds(aligned(turn, tile), tile), :].astype(f32)
        inverse = lax.rsqrt(jnp.mean(floats * floats, axis=1, keepdims=True) + NORM_FLOOR)
        at = pl.ds(pl.multiple_of(place * length + turn * tile, tile), tile)
        sequence[at, :] = (floats * inverse * norm_gain_ref[...]).astype(bf16)
        return 0

    lax.fori_loop(0, length // tile, normalise, 0)

    def own_block(at):
        return wout.at[:, pl.ds(aligned(at, columns), columns)]

    @pl.when(mine)
    def _():
        at = pl.ds(aligned(place * 2 + row_y, columns), columns)
        wout[pl.ds(aligned(side, joint), conv_rows), at] = out_conv_ref[...]
        wout[pl.ds(pl.multiple_of(side * joint + conv_rows, 16), state_rows), at] = (
            out_state_ref[...]
        )

    pl.semaphore_wait(barrier, len(partners))

    def tokens_at(sp_at, side_at, part):
        first = sp_at * length + side_at * half + part * chunk
        return sequence.at[pl.ds(pl.multiple_of(first, 16), chunk)]

    hops = (
        ({"sp": ahead(1)}, lambda d: place >= d, lambda d: behind(d), place < along - 1),
        ({"sp": behind(1)}, lambda d: place + d < along, lambda d: ahead(d), place > 0),
    )

    def half_of(sp_at, side_at):
        first = sp_at * length + side_at * half
        return sequence.at[pl.ds(pl.multiple_of(first, 16), half)]

    own_slot = (place, along)
    for part in range(parts):
        for way, (onward, _, _, open_end) in enumerate(hops):
            here = tokens_at(place, side, part)
            send(here, here, t_send.at[own_slot[way]], t_recv.at[place, part], onward, open_end)

    def out_piece(side_at, at):
        cut = pl.ds(aligned(at, columns), columns)
        return (
            wout.at[pl.ds(aligned(side_at, joint), conv_rows), cut],
            wout.at[pl.ds(pl.multiple_of(side_at * joint + conv_rows, 16), state_rows), cut],
        )

    own_at = place * 2 + row_y
    theirs = jnp.logical_not(mine)
    for source, target in zip((out_conv_ref, out_state_ref), out_piece(side, own_at)):
        send(source, target, o_send.at[0], o_recv.at[0], {"tp": other}, theirs)

    def out_half(side_at):
        return wout.at[pl.ds(aligned(side_at, joint), joint), pl.ds(aligned(own_at, columns), columns)]

    sent(out_half(side), o_send.at[0], {"tp": other}, theirs)
    own_gain = gains.at[side]
    send(
        conv_gain_ref,
        own_gain,
        g_send.at[0],
        g_recv.at[0],
        {"tp": other},
        lone=True,
    )

    def piece(sp_at, fs_at, at):
        rows = rows_of(sp_at, fs_at)
        if at < STATES:
            return weights.at[rows, pl.ds(at * wide, wide)]
        if at == STATES:
            return weights.at[rows, pl.ds(conv_at, 2 * channels)]
        return packed.at[packed_of(sp_at, fs_at)]

    groups = ((0, 1, 2, 3), (4, 5), (6,))

    def grouped(sp_at, fs_at, which):
        rows = rows_of(sp_at, fs_at)
        if which == 0:
            return weights.at[rows, pl.ds(0, 4 * wide)]
        if which == 1:
            return weights.at[rows, pl.ds(4 * wide, wide + 2 * channels)]
        return packed.at[packed_of(sp_at, fs_at)]

    for way, (onward, _, _, open_end) in enumerate(hops):
        sent(half_of(place, side), t_send.at[own_slot[way]], onward, open_end)

    def tokens_on(d):
        for part in range(parts):
            for onward, valid, source, open_end in hops:
                at = source(d)
                here = tokens_at(at, side, part)
                arrive(here, t_send.at[at], t_recv.at[at, part], onward, valid(d))
                if d < along - 1:
                    send(
                        here, here, t_send.at[at], t_recv.at[at, part], onward, valid(d) & open_end
                    )
                send(here, here, x_send.at[0], x_recv.at[0], {"tp": other}, valid(d))
        if d < along - 1:
            for onward, valid, source, open_end in hops:
                at = source(d)
                sent(half_of(at, side), t_send.at[at], onward, valid(d) & open_end)

    def pass_on(at, which, ready=None):
        here = grouped(at, seat, which)
        send(here, here, y_send.at[which], y_recv.at[at, which], {"fs": far}, ready)
        send(here, here, c_send.at[which], c_recv.at[which], {"fs": near}, ready)

    def spread(d, which):
        for onward, valid, source, _ in hops:
            at = source(d)
            here = grouped(at, seat, which)
            arrive(here, w_send.at[which], w_recv.at[at, which], onward, valid(d))
            pass_on(at, which, valid(d))

    def relay(d, which):
        for _, valid, source, _ in hops if d else hops[:1]:
            at = source(d) if d else place
            ready = valid(d) if d else None
            here = grouped(at, far, which)
            arrive(here, y_send.at[which], y_recv.at[at, which], {"fs": far}, ready)
            send(here, here, r_send.at[which], r_recv.at[which], {"fs": near}, ready)

    def several(count, which):
        if which == 0:
            return weights.at[pl.ds(0, count * depth), pl.ds(0, 4 * wide)]
        if which == 1:
            return weights.at[pl.ds(0, count * depth), pl.ds(4 * wide, wide + 2 * channels)]
        return packed.at[pl.ds(0, count * depth // 2)]

    def hand_out(way, d, which):
        target = (ahead, behind)[way](d)
        reach_of = (place + d < along, place >= d)[way]
        for at in groups[which]:
            if at < STATES:
                source = state_refs[at].at[:, pl.ds(aligned(target, wide), wide)]
            elif at == STATES:
                source = conv_pack.at[target]
            else:
                source = gate_pack.at[target]
            send(
                source,
                piece(place, seat, at),
                w_send.at[which],
                w_recv.at[place, which],
                {"sp": target},
                reach_of,
            )

    for d in range(1, along):
        for way in range(2):
            hand_out(way, d, 0)
    for which in range(3):
        pass_on(place, which)
        sent(several(along - 1, which), w_send.at[which], {"sp": ahead(1)})
        sent(several(along, which), y_send.at[which], {"fs": far})
        sent(several(along, which), c_send.at[which], {"fs": near})
        sent(several(along, which), r_send.at[which], {"fs": near})
    order = sorted(range(1, along), key=lambda s: min(s, along - s))
    for s in order:
        send(pace_ref, paces.at[place], p_send.at[s], p_recv.at[s], {"sp": ahead(s)}, lone=True)

    def sides_out():
        for d in range(1, along):
            for which in (1, 2):
                for way in range(2):
                    hand_out(way, d, which)

    tokens_on(1)
    spread(1, 0)
    for which in range(3):
        relay(0, which)
    tokens_on(2)
    relay(1, 0)
    spread(2, 0)
    for d in range(3, along):
        tokens_on(d)
    sides_out()
    for d in range(3, along):
        spread(d, 0)
    for d in range(2, along):
        relay(d, 0)
    arrive(out_half(other), o_send.at[0], o_recv.at[0], {"tp": other}, mine)
    here = own_block(own_at)
    for way, (onward, _, _, open_end) in enumerate(hops):
        send(here, here, oz_send.at[own_slot[way]], oz_recv.at[place], onward, mine & open_end)
        sent(here, oz_send.at[own_slot[way]], onward, mine & open_end)
    send(here, here, oy_send.at[0], oy_recv.at[place], {"fs": far}, mine)
    send(here, here, on_send.at[0], on_recv.at[0], {"fs": near}, mine)

    def out_on(d):
        for onward, valid, source, open_end in hops:
            at = source(d)
            here = own_block(at * 2 + row_y)
            ready = mine & valid(d)
            arrive(here, oz_send.at[at], oz_recv.at[at], onward, ready)
            if d < along - 1:
                send(here, here, oz_send.at[at], oz_recv.at[at], onward, ready & open_end)
                sent(here, oz_send.at[at], onward, ready & open_end)
            send(here, here, oy_send.at[0], oy_recv.at[at], {"fs": far}, ready)
            send(here, here, on_send.at[0], on_recv.at[0], {"fs": near}, ready)

    every = wout.at[:, pl.ds(0, along * columns)]

    def settled(which):
        arrive(several(along, which), c_send.at[which], c_recv.at[which], {"fs": near})
        arrive(several(along, which), r_send.at[which], r_recv.at[which], {"fs": near})

    for s in order:
        arrive(paces.at[behind(s)], p_send.at[s], p_recv.at[s], {"sp": ahead(s)})
    blocks = total // span
    row = lax.broadcasted_iota(jnp.int32, (span, span), 0)
    col = lax.broadcasted_iota(jnp.int32, (span, span), 1)
    eye = (row == col).astype(f32)
    for at in range(along):
        for part in range(length // span):
            line = paces[at][:, part * span : (part + 1) * span]
            first = at * length + part * span
            pace_col[first : first + span, :] = jnp.sum(eye * line, axis=1, keepdims=True)
    crossed = sequence.at[pl.ds(0, (along - 1) * half)]
    arrive(crossed, x_send.at[0], x_recv.at[0], {"tp": other})
    sent(crossed, x_send.at[0], {"tp": other})
    settled(0)

    gate_at = conv_at + 2 * channels

    def unpack(turn, _):
        both = packed[pl.ds(aligned(turn, depth // 2), depth // 2), :].astype(f32)
        at = pl.ds(aligned(turn, depth), depth // 2)
        weights[at, gate_at : gate_at + channels] = both[:, :channels].astype(bf16)
        at = pl.ds(pl.multiple_of(turn * depth + depth // 2, depth // 2), depth // 2)
        weights[at, gate_at : gate_at + channels] = both[:, channels:].astype(bf16)
        return 0

    big = next(n for n in (256, 192, 128, 64) if total % n == 0)

    def multiply(first, last):
        def one(turn, _):
            at = pl.ds(aligned(turn, big), big)
            proj[at, first:last] = jnp.dot(
                sequence[at, :], weights[:, first:last], preferred_element_type=f32
            ).astype(bf16)
            return 0

        lax.fori_loop(0, total // big, one, 0)

    multiply(0, 4 * wide)

    begins = [begin_ref[0, place * heads + head] for head in range(heads)]
    own_cut = pl.ds(aligned(place, wide), wide)
    base = base_ref[:, own_cut]
    strength = strength_ref[:, own_cut]
    gain = group_gain_ref[:, own_cut]

    strict = (row > col).astype(f32)
    weak = (row >= col).astype(f32)
    masks = jnp.concatenate(
        [jnp.concatenate([strict, strict], axis=1), jnp.concatenate([weak, weak], axis=1)], axis=0
    )
    square = (
        lax.broadcasted_iota(jnp.int32, (size, size), 0)
        == lax.broadcasted_iota(jnp.int32, (size, size), 1)
    ).astype(f32)
    least = min(8, span)
    same = (lax.div(row, least) == lax.div(col, least)).astype(f32)
    merges = []
    reach = least
    while reach < span:
        merges.append(
            (
                (lax.div(row, 2 * reach) == lax.div(col, 2 * reach))
                & (lax.div(row, reach) != lax.div(col, reach))
            ).astype(f32)
        )
        reach = 2 * reach
    weak_bf = weak.astype(bf16)

    def step(turn, _):
        items = []
        for part in range(group):
            block = turn * group + part
            rows = pl.ds(pl.multiple_of(block * span, span), span)
            query = proj[rows, 0:wide].astype(f32)
            keys = proj[rows, wide : 2 * wide].astype(f32)
            values = proj[rows, 2 * wide : 3 * wide].astype(f32)
            decay_in = proj[rows, 3 * wide : 4 * wide].astype(f32)
            log_keep = -jnp.exp(base + jnp.tanh(decay_in)) * pace_col[rows, :]
            high = log_keep.astype(bf16)
            rest = log_keep - high.astype(f32)
            mid = rest.astype(bf16)
            low = (rest - mid.astype(f32)).astype(bf16)
            summed = (
                jnp.dot(weak_bf, high, preferred_element_type=f32)
                + jnp.dot(weak_bf, mid, preferred_element_type=f32)
                + jnp.dot(weak_bf, low, preferred_element_type=f32)
            )
            last = summed[span - 1 : span, :]
            lead = jnp.exp(summed - log_keep)
            grown = jnp.exp(summed)
            back = jnp.exp(-summed)
            tail = jnp.exp(last - summed)
            ended = jnp.exp(last)
            for head in range(heads):
                at = slice(head * size, (head + 1) * size)
                key = keys[:, at]
                unit = key * lax.rsqrt(
                    jnp.maximum(jnp.sum(key * key, axis=1, keepdims=True), 1.0)
                )
                write = unit * strength[:, at]
                lead_remove = -unit * lead[:, at]
                lead_query = query[:, at] * grown[:, at]
                items.append(
                    dict(
                        at=(block, head),
                        value=values[:, at],
                        lead_remove=lead_remove,
                        lead_query=lead_query,
                        left=jnp.concatenate([lead_remove, lead_query], axis=0),
                        right=jnp.concatenate([write * back[:, at], key * back[:, at]], axis=0),
                        tail_write=write * tail[:, at],
                        tail_key=key * tail[:, at],
                        ended=ended[:, at],
                    )
                )
        for item in items:
            item["pair"] = (
                product(halves(item["left"]), halves(item["right"]), ((1,), (1,))) * masks
            )
        for item in items:
            item["system"] = item["pair"][:span, :span]
            item["power"] = halves(item["system"] * same)
            item["inverse"] = eye + item["system"] * same
        reach = 2
        while reach < least:
            for item in items:
                item["power"] = halves(product(item["power"], item["power"]))
            for item in items:
                item["inverse"] = item["inverse"] + product(
                    halves(item["inverse"]), item["power"]
                )
            reach = 2 * reach
        for item in items:
            padded = jnp.concatenate([jnp.zeros_like(item["value"]), item["value"]], axis=0)
            item["mixed"] = product(halves(item["pair"]), halves(padded))
        for merge in merges:
            for item in items:
                item["inside"] = halves(item["inverse"])
                item["next"] = halves(product(halves(item["system"] * merge), item["inside"]))
            for item in items:
                item["inverse"] = item["inverse"] + product(item["inside"], item["next"])
        for item in items:
            right_side = jnp.concatenate([item["mixed"][:span], item["lead_remove"]], axis=1)
            item["solved"] = halves(product(halves(item["inverse"]), halves(right_side)))
        for item in items:
            block, head = item["at"]
            seen = product(halves(item["pair"][span:, :span]), item["solved"])
            local_ref[head, block] = seen[:, :size] + item["mixed"][span:]
            map_ref[head, block] = item["lead_query"] + seen[:, size:]
            carried = product(item["solved"], halves(item["tail_write"]), ((0,), (0,)))
            carry_ref[head, block] = carried[size:] + square * item["ended"]
            add_ref[head, block] = carried[:size] + product(
                halves(item["value"]), halves(item["tail_key"]), ((0,), (0,))
            )
        return 0

    def rows_for(at):
        return pl.ds(at * length, length)

    def convolve():
        kernel = taps_ref.shape[0]
        lead_rows = conv_ref.shape[0] - total
        pair = pl.ds(aligned(lax.div(place * channels, 128), 128), 128)
        both_taps = taps_ref[:, pair]
        taps = jnp.where(
            lax.rem(place * channels, 128) == 0, both_taps[:, :channels], both_taps[:, 128 - channels :]
        )
        conv_ref[0:lead_rows, :] = jnp.zeros((lead_rows, channels), f32)
        for block in range(blocks):
            rows = pl.ds(block * span, span)
            value = proj[rows, conv_at : conv_at + channels].astype(f32)
            admit = proj[rows, conv_at + channels : conv_at + 2 * channels].astype(f32)
            conv_ref[pl.ds(lead_rows + block * span, span), :] = (
                (value * jax.nn.sigmoid(admit)).astype(bf16).astype(f32)
            )
        for block in range(blocks):
            summed = jnp.zeros((span, channels), f32)
            for tap in range(kernel):
                first = lead_rows - (kernel - 1) + block * span + tap
                summed = summed + taps[tap : tap + 1, :] * conv_ref[pl.ds(first, span), :]
            rows = pl.ds(block * span, span)
            gate = proj[rows, gate_at : gate_at + channels].astype(f32)
            side_buf[rows, :] = jnp.concatenate([summed, gate], axis=1).astype(bf16)

        for at in range(along):
            target = sides.at[side, place]

            @pl.when(place == at)
            def _():
                sides[side, place] = side_buf[rows_for(at), :]

            away = place != at
            send(
                side_buf.at[rows_for(at)], target, ec_send.at[0], ec_recv.at[place], {"sp": at}, away
            )
            send(
                side_buf.at[rows_for(at)],
                target,
                xc_send.at[0],
                xc_recv.at[0],
                {"tp": other},
                place == at,
            )

    def sides_between():
        for which in (1, 2):
            for d in (1, *range(3, along), 2):
                spread(d, which)
            for d in (1, *range(3, along), 2):
                relay(d, which)
        out_on(1)

    def gates_between():
        for which in (1, 2):
            settled(which)
        lax.fori_loop(0, along * 4, unpack, 0)
        multiply(4 * wide, weights.shape[1])
        convolve()

    turns = blocks // group
    first, second = turns // 3, 2 * turns // 3
    lax.fori_loop(0, first, step, 0)
    sides_between()
    lax.fori_loop(first, second, step, 0)
    gates_between()
    lax.fori_loop(second, turns, step, 0)
    for d in range(2, along - 1):
        out_on(d)

    for s in order:
        here = sides.at[side, behind(s)]
        arrive(here, ec_send.at[0], ec_recv.at[behind(s)], {"sp": ahead(s)})
        send(here, here, xc_send.at[0], xc_recv.at[0], {"tp": other})

    def joined_at(side_at, sp_at):
        first = side_at * joint + conv_rows + sp_at * wide
        return joined.at[:, pl.ds(pl.multiple_of(first, 128), wide)]

    states = list(begins)
    for block in range(blocks):
        rows = pl.ds(block * span, span)
        gate = proj[rows, 4 * wide : 5 * wide].astype(f32)
        pieces = []
        for head in range(heads):
            state = halves(states[head])
            out = local_ref[head, block] + product(
                halves(map_ref[head, block]), state, ((1,), (1,))
            )
            states[head] = product(state, halves(carry_ref[head, block])) + add_ref[head, block]
            centered = out - jnp.mean(out, axis=1, keepdims=True)
            variance = jnp.mean(centered * centered, axis=1, keepdims=True)
            pieces.append(centered * lax.rsqrt(variance + GROUP_FLOOR))
        scaled = jnp.concatenate(pieces, axis=1) * gain
        state_buf[rows, :] = (scaled * gate * jax.nn.sigmoid(gate)).astype(bf16)
        if (block + 1) * span % length == 0:
            at = (block + 1) * span // length - 1
            target = joined_at(side, place)

            @pl.when(place == at)
            def _():
                joined[:, pl.ds(
                    pl.multiple_of(side * joint + conv_rows + place * wide, 128), wide
                )] = state_buf[rows_for(at), :]

            source = state_buf.at[rows_for(at)]
            send(source, target, es_send.at[0], es_recv.at[place], {"sp": at}, place != at)
            send(
                source,
                target,
                xs_send.at[0],
                xs_recv.at[0],
                {"tp": other},
                place == at,
            )

    out_on(along - 1)
    for at in range(along):
        ready = mine
        here = own_block(at * 2 + 1 - row_y)
        arrive(here, oy_send.at[0], oy_recv.at[at], {"fs": far}, ready)
        send(here, here, or_send.at[0], or_recv.at[0], {"fs": near}, ready)

    arrive(sides.at[other], xc_send.at[0], xc_recv.at[0], {"tp": other})
    arrive(gains.at[other], g_send.at[0], g_recv.at[0], {"tp": other})
    whole_gain = jnp.concatenate([gains[0], gains[1]], axis=1)
    piece_rows = next(n for n in (64, 48, 32, 16) if length % n == 0)

    def convolved(turn, _):
        at = pl.ds(aligned(turn, piece_rows), piece_rows)
        sums = jnp.concatenate(
            [
                sides[s, p, at, 0:channels].astype(f32)
                for s in range(2)
                for p in range(along)
            ],
            axis=1,
        )
        gates = jnp.concatenate(
            [
                sides[s, p, at, channels : 2 * channels].astype(f32)
                for s in range(2)
                for p in range(along)
            ],
            axis=1,
        )
        mean = jnp.mean(sums, axis=1, keepdims=True)
        spread_of = jnp.mean(sums * sums, axis=1, keepdims=True) - mean * mean
        shaped = jax.nn.silu(
            (sums - mean) * lax.rsqrt(spread_of + CHANNEL_FLOOR) * whole_gain
        ).astype(bf16)
        pointwise = jnp.dot(shaped, point_ref[...], preferred_element_type=f32)
        conv_out = (pointwise * jax.nn.silu(gates)).astype(bf16)
        joined[at, 0:conv_rows] = conv_out[:, :conv_rows]
        joined[at, joint : joint + conv_rows] = conv_out[:, conv_rows:]
        return 0

    lax.fori_loop(0, length // piece_rows, convolved, 0)

    for s in order:
        here = joined_at(side, behind(s))
        arrive(here, es_send.at[0], es_recv.at[behind(s)], {"sp": ahead(s)})
        send(here, here, xs_send.at[0], xs_recv.at[0], {"tp": other})
    arrive(every, on_send.at[0], on_recv.at[0], {"fs": near}, theirs)
    arrive(every, or_send.at[0], or_recv.at[0], {"fs": near}, theirs)
    arrive(state_buf, xs_send.at[0], xs_recv.at[0], {"tp": other})

    count = wout.shape[1] // columns
    step_of = 2 if count % 2 == 0 else 1
    ours = pl.ds(pl.multiple_of(side * half, 16), half)
    others = pl.ds(pl.multiple_of(other * half, 16), half)

    def out_cut(at, side_at):
        return pl.ds(aligned(2 * at + side_at, columns), columns)

    for first in range(0, count, step_of):
        cut = slice(first * columns, (first + step_of) * columns)
        result[:, cut] = jnp.dot(
            joined[...], wout[:, cut], preferred_element_type=f32
        ).astype(bf16)
        for at in range(first, first + step_of):
            piece_cut = pl.ds(at * columns, columns)
            send(
                result.at[others, piece_cut],
                out_ref.at[:, out_cut(at, side)],
                f_send.at[0],
                f_recv.at[0],
                {"tp": other},
            )
            kept = pltpu.make_async_copy(
                result.at[ours, piece_cut], out_ref.at[:, out_cut(at, side)], own_sem.at[0]
            )
            kept.start()
    halfway = result.at[pl.ds(0, half)]
    arrive(halfway, f_send.at[0], f_recv.at[0], {"tp": other})
    pltpu.make_async_copy(halfway, halfway, own_sem.at[0]).wait()
    away_rows = pl.ds(0, (along - 1) * length)
    sent(side_buf.at[away_rows], ec_send.at[0], {"sp": ahead(1)})
    sent(state_buf.at[away_rows], es_send.at[0], {"sp": ahead(1)})
    sent(side_buf, xc_send.at[0], {"tp": other})
    sent(state_buf, xs_send.at[0], {"tp": other})
    sent(every, oy_send.at[0], {"fs": far}, mine)
    sent(every, on_send.at[0], {"fs": near}, mine)
    sent(every, or_send.at[0], {"fs": near}, mine)
    sent(halfway, f_send.at[0], {"tp": other})
    for valid, copy in pending:
        guarded(valid, copy.wait_send)


def fused_body(
    tokens,
    decay_pace,
    start_state,
    norm_gain,
    conv_value,
    conv_admit,
    conv_gate,
    state_query,
    state_key,
    state_value,
    state_decay,
    state_gate,
    conv_taps,
    conv_gain,
    point_weight,
    decay_base,
    correction,
    group_gain,
    output_conv,
    output_state,
):
    along = lax.axis_size("sp")
    _, length, width = tokens.shape
    depth, wide = state_query.shape[0], state_query.shape[1] // along
    channels = conv_value.shape[1] // along
    size = start_state.shape[-1]
    heads = wide // size
    total = along * length
    span = 64
    blocks = total // span
    group = next(n for n in (4, 3, 2, 1) if blocks % n == 0)
    kernel = conv_taps.shape[0]
    joint = output_conv.shape[0] + output_state.shape[0]
    columns = output_conv.shape[1]
    gain_lanes = conv_gain.shape[0]
    f32, bf16 = jnp.float32, jnp.bfloat16
    half = length // 2
    parts = next(n for n in (3, 2, 1) if half % (16 * n) == 0)
    lead_rows = -(-(kernel - 1) // 8) * 8
    dma = pltpu.SemaphoreType.DMA
    maps = pltpu.VMEM((heads, blocks, size, size), f32)
    wout_blocks = along * 2

    def both(*shape):
        return [dma(shape), dma(shape)]

    mixed = pl.pallas_call(
        functools.partial(layer_kernel, span, group),
        out_shape=jax.ShapeDtypeStruct((half, width), bf16),
        in_specs=[pl.BlockSpec(memory_space=pltpu.VMEM)] * 20,
        out_specs=pl.BlockSpec(memory_space=pl.ANY),
        scratch_shapes=[
            pltpu.VMEM((total, width), bf16),
            pltpu.VMEM((width, 5 * wide + 3 * channels), bf16),
            pltpu.VMEM((width // 2, 2 * channels), bf16),
            pltpu.VMEM((along, depth, 2 * channels), bf16),
            pltpu.VMEM((along, depth // 2, 2 * channels), bf16),
            pltpu.VMEM((along, 1, length), f32),
            pltpu.VMEM((2, 1, gain_lanes), f32),
            pltpu.VMEM((2 * joint, wout_blocks * columns), bf16),
            pltpu.VMEM((total, 5 * wide + 3 * channels), bf16),
            pltpu.VMEM((total, 1), f32),
            pltpu.VMEM((heads, blocks, span, size), f32),
            pltpu.VMEM((heads, blocks, span, size), f32),
            maps,
            maps,
            pltpu.VMEM((lead_rows + total, channels), f32),
            pltpu.VMEM((total, wide), bf16),
            pltpu.VMEM((total, 2 * channels), bf16),
            pltpu.VMEM((length, 2 * joint), bf16),
            pltpu.VMEM((2, along, length, 2 * channels), bf16),
            pltpu.VMEM((length, wout_blocks * columns), bf16),
        ]
        + [dma((along + 1,)), dma((along, parts))]
        + both(1)
        + both(along)
        + [dma((3,)), dma((along, 3))]
        + [dma((3,)), dma((along, 3))]
        + both(3)
        + both(3)
        + both(1)
        + both(1)
        + [dma((along + 1,)), dma((along,))]
        + [dma((1,)), dma((along,))]
        + both(1)
        + both(1)
        + [dma((1,)), dma((along,))]
        + [dma((1,)), dma((along,))]
        + both(1)
        + both(1)
        + both(1)
        + [dma((1,))],
        compiler_params=pltpu.CompilerParams(
            collective_id=0, has_side_effects=True, vmem_limit_bytes=56 * 1024 * 1024
        ),
        cost_estimate=pl.CostEstimate(
            flops=60_000_000_000, bytes_accessed=8_000_000, transcendentals=0
        ),
        name="layer",
    )(
        tokens,
        state_query,
        state_key,
        state_value,
        state_decay,
        state_gate,
        conv_value,
        conv_admit,
        conv_gate,
        norm_gain[None],
        decay_base[None],
        correction[None],
        group_gain[None],
        conv_gain[None],
        decay_pace,
        start_state,
        conv_taps,
        point_weight,
        output_conv,
        output_state,
    )
    return mixed.reshape(1, half, width)


def dispatch(*arrays):
    along = lax.axis_size("sp")
    tokens, start_state, conv_value, query, output_conv, output_state = (
        arrays[0],
        arrays[2],
        arrays[4],
        arrays[7],
        arrays[18],
        arrays[19],
    )
    depth, width = query.shape[0], tokens.shape[2]
    size = start_state.shape[-1]
    fits = (
        along > 2
        and lax.axis_size("fs") == 4
        and lax.axis_size("tp") == 2
        and tokens.shape[1] % 64 == 0
        and tokens.shape[0] == 1
        and start_state.shape[1] % along == 0
        and size == 64
        and query.shape[1] == along * 128
        and conv_value.shape[1] == along * 64
        and depth % 32 == 0
        and depth * along * 4 == width
        and output_conv.shape[0] == along * 64
        and output_state.shape[0] == along * 128
        and output_conv.shape[1] == 128
        and width == along * 4 * 128
    )
    return (fused_body if fits else body)(*arrays)


def solution(mesh):
    return jax.shard_map(
        dispatch,
        mesh=mesh,
        in_specs=(
            P("fs", "sp", None),
            P("fs", "sp"),
            P("fs", "tp", None, None),
            P(),
            P(("sp", "fs"), "tp"),
            P(("sp", "fs"), "tp"),
            P(("sp", "fs"), "tp"),
            P(("sp", "fs"), "tp"),
            P(("sp", "fs"), "tp"),
            P(("sp", "fs"), "tp"),
            P(("sp", "fs"), "tp"),
            P(("sp", "fs"), "tp"),
            P(None, "tp"),
            P("tp"),
            P(),
            P("tp"),
            P("tp"),
            P("tp"),
            P("tp", ("sp", "fs")),
            P("tp", ("sp", "fs")),
        ),
        out_specs=P("fs", ("sp", "tp"), None),
        check_vma=False,
    )
```

```python
import functools

import jax
import jax.numpy as jnp
from jax import lax
from jax.experimental import pallas as pl
from jax.experimental.pallas import tpu as pltpu
from jax.sharding import PartitionSpec as P

NORM_FLOOR = 0.1
CHANNEL_FLOOR = 0.1
GROUP_FLOOR = 1.0


def passed_along(value, axis, steps):
    count = lax.axis_size(axis)
    leading, last = (max(0, -steps), min(count, count - steps))
    return lax.ppermute(value, axis, [(source, source + steps) for source in range(leading, last)])


def entering_2(value, axis, join, neutral):
    place = lax.axis_index(axis)
    gathered = jax.tree.map(
        lambda a, kind: lax.all_gather(a.astype(kind), axis),
        value,
        jax.tree.map(lambda a: jnp.bfloat16 if a.dtype == jnp.float32 else a.dtype, value),
    )
    state = jax.tree.map(lambda a, e: jnp.zeros_like(a) + jnp.asarray(e, a.dtype), value, neutral)

    def one(lap, state):
        return join(
            state,
            jax.tree.map(
                lambda a, own: lax.dynamic_index_in_dim(a, lap, 0, False).astype(own.dtype),
                gathered,
                value,
            ),
        )

    return lax.fori_loop(0, place, one, state)


def apply_map(matrix, right):
    return jnp.einsum("hbti,hbic->hbtc", matrix, right, precision=lax.Precision.HIGHEST)


def pair_terms(left, right, mask):
    return jnp.einsum("hbtc,hbic->hbti", left, right, precision=lax.Precision.HIGHEST) * mask


def compose(earlier, later):
    first = jnp.matmul(earlier[0], later[0], precision=lax.Precision.HIGHEST)
    second = jnp.matmul(earlier[1], later[0], precision=lax.Precision.HIGHEST) + later[1]
    return (first, second)


def block_terms(query, keys, values, unit, write, log_keep):
    size = query.shape[-1]
    span = query.shape[2]
    total_log = jnp.cumsum(log_keep, axis=2)
    before_log = total_log - log_keep
    last_log = total_log[:, :, span - 1 :, :]
    lead_remove = -unit * jnp.exp(before_log)
    lead_query = query * jnp.exp(total_log)
    back_write = write * jnp.exp(-total_log)
    back_key = keys * jnp.exp(-total_log)
    places = jnp.arange(span)
    strict = (places[:, None] > places[None, :]).astype(jnp.float32)
    weak = (places[:, None] >= places[None, :]).astype(jnp.float32)
    remove_write = pair_terms(lead_remove, back_write, strict)
    remove_key = pair_terms(lead_remove, back_key, strict)
    query_write = pair_terms(lead_query, back_write, weak)
    query_key = pair_terms(lead_query, back_key, weak)
    right_side = jnp.concatenate([apply_map(remove_key, values), lead_remove], axis=-1)
    system = jnp.eye(span, dtype=jnp.float32) - remove_write
    solved = jax.scipy.linalg.solve_triangular(system, right_side, lower=True, unit_diagonal=True)
    own_part = solved[..., :size]
    start_part = solved[..., size:]
    local_out = apply_map(query_write, own_part) + apply_map(query_key, values)
    start_map = lead_query + apply_map(query_write, start_part)
    tail_write = write * jnp.exp(last_log - total_log)
    tail_key = keys * jnp.exp(last_log - total_log)
    carry_map = jnp.einsum(
        "hbtk,hbtj->hbkj", start_part, tail_write, precision=lax.Precision.HIGHEST
    ) + jnp.eye(size, dtype=jnp.float32) * jnp.exp(last_log)
    carry_add = jnp.einsum(
        "hbtv,hbtj->hbvj", own_part, tail_write, precision=lax.Precision.HIGHEST
    ) + jnp.einsum("hbtv,hbtj->hbvj", values, tail_key, precision=lax.Precision.HIGHEST)
    return (local_out, start_map, carry_map, carry_add)


def body(
    tokens,
    decay_pace,
    start_state,
    norm_gain,
    conv_value,
    conv_admit,
    conv_gate,
    state_query,
    state_key,
    state_value,
    state_decay,
    state_gate,
    conv_taps,
    conv_gain,
    point_weight,
    decay_base,
    correction,
    group_gain,
    output_conv,
    output_state,
):
    width = tokens.shape[-1]
    rows = tokens.reshape(-1, width)
    length = rows.shape[0]
    floats = rows.astype(jnp.float32)
    inverse = lax.rsqrt(jnp.mean(floats * floats, axis=1, keepdims=True) + NORM_FLOOR)
    normed = (floats * inverse * norm_gain).astype(jnp.bfloat16)
    shards = (
        conv_value,
        conv_admit,
        conv_gate,
        state_query,
        state_key,
        state_value,
        state_decay,
        state_gate,
    )
    stacked = jnp.concatenate(shards, axis=1)
    projected = jnp.dot(
        normed,
        lax.all_gather(stacked, ("sp", "fs"), axis=0, tiled=True),
        preferred_element_type=jnp.float32,
    ).astype(jnp.bfloat16)
    pieces = []
    offset = 0
    for shard in shards:
        pieces.append(projected[:, offset : offset + shard.shape[1]].astype(jnp.float32))
        offset = offset + shard.shape[1]
    value, admit, gate_conv, query, keys, values, decay_in, gate_state = pieces
    channels = value.shape[1]
    kernel = conv_taps.shape[0]
    conv_input = (value * jax.nn.sigmoid(admit)).astype(jnp.bfloat16)
    earlier = passed_along(conv_input[length - (kernel - 1) :], "sp", 1)
    padded = jnp.concatenate([earlier, conv_input], axis=0).astype(jnp.float32)
    conv_sum = jnp.zeros((length, channels), jnp.float32)
    for place in range(kernel):
        conv_sum = conv_sum + conv_taps[place] * padded[place : place + length]
    local_point = lax.dynamic_slice_in_dim(
        point_weight, lax.axis_index("tp") * channels, channels, 1
    )
    whole_sum, whole_gain = (
        lax.all_gather(conv_sum.astype(jnp.bfloat16), "tp", axis=1, tiled=True).astype(
            conv_sum.dtype
        ),
        lax.all_gather(conv_gain.astype(jnp.bfloat16), "tp", axis=0, tiled=True).astype(
            conv_gain.dtype
        ),
    )
    mean = jnp.mean(whole_sum, axis=1, keepdims=True)
    spread = jnp.mean(whole_sum * whole_sum, axis=1, keepdims=True) - mean * mean
    shaped = jax.nn.silu(
        (whole_sum - mean) * lax.rsqrt(spread + CHANNEL_FLOOR) * whole_gain
    ).astype(jnp.bfloat16)
    pointwise = jnp.dot(shaped, local_point, preferred_element_type=jnp.float32)
    conv_out = (pointwise * jax.nn.silu(gate_conv)).astype(jnp.bfloat16)
    size = start_state.shape[-1]
    heads = query.shape[1] // size
    span = min(64, length)
    blocks = length // span
    log_keep = -jnp.exp(decay_base + jnp.tanh(decay_in)) * decay_pace.reshape(-1)[:, None]
    key_heads = keys.reshape(length, heads, size)
    unit = key_heads * lax.rsqrt(
        jnp.maximum(jnp.sum(key_heads * key_heads, axis=-1, keepdims=True), 1.0)
    )
    write = unit * correction.reshape(heads, size)

    def arrange(array):
        return array.reshape(blocks, span, heads, size).transpose(2, 0, 1, 3)

    local_out, start_map, carry_map, carry_add = block_terms(
        arrange(query),
        arrange(keys),
        arrange(values),
        arrange(unit),
        arrange(write),
        arrange(log_keep),
    )
    identity = (
        jnp.broadcast_to(jnp.eye(size, dtype=jnp.float32), (heads, size, size)),
        jnp.zeros((heads, size, size), jnp.float32),
    )

    def along(carried, block_pair):
        return (compose(carried, block_pair), carried)

    device_pair, prefixes = lax.scan(
        along, identity, (jnp.moveaxis(carry_map, 1, 0), jnp.moveaxis(carry_add, 1, 0))
    )
    prior_map, prior_add = entering_2(device_pair, "sp", compose, identity)
    begin = start_state.reshape(heads, size, size)
    entering = jnp.matmul(begin, prior_map, precision=lax.Precision.HIGHEST) + prior_add
    block_starts = (
        jnp.matmul(entering[None], prefixes[0], precision=lax.Precision.HIGHEST) + prefixes[1]
    )
    block_starts = jnp.moveaxis(block_starts, 0, 1)
    outputs = local_out + jnp.einsum(
        "hbtk,hbvk->hbtv", start_map, block_starts, precision=lax.Precision.HIGHEST
    )
    outputs = outputs.transpose(1, 2, 0, 3).reshape(length, heads, size)
    centered = outputs - jnp.mean(outputs, axis=-1, keepdims=True)
    variance = jnp.mean(centered * centered, axis=-1, keepdims=True)
    grouped = centered * lax.rsqrt(variance + GROUP_FLOOR) * group_gain.reshape(heads, size)
    state_out = (grouped.reshape(length, heads * size) * jax.nn.silu(gate_state)).astype(
        jnp.bfloat16
    )
    local_mix = jnp.concatenate([conv_out, state_out], axis=1)
    moved = lax.all_to_all(local_mix, "tp", split_axis=0, concat_axis=1, tiled=True)
    conv_rows, state_rows = (
        lax.all_gather(output_conv, "tp", axis=0, tiled=True),
        lax.all_gather(output_state, "tp", axis=0, tiled=True),
    )
    groups = lax.axis_size("tp")
    joined = jnp.concatenate(
        [conv_rows.reshape(groups, channels, -1), state_rows.reshape(groups, heads * size, -1)],
        axis=1,
    )
    joined = joined.reshape(groups * (channels + heads * size), -1)
    mixed = jnp.dot(
        moved,
        lax.all_gather(joined, ("sp", "fs"), axis=1, tiled=True),
        preferred_element_type=jnp.float32,
    )
    return mixed.astype(jnp.bfloat16).reshape(1, -1, width)


def halves(array):
    high = array.astype(jnp.bfloat16)
    low = (array - high.astype(jnp.float32)).astype(jnp.bfloat16)
    return (high, low)


def product(left, right, dims=((1,), (0,))):
    def one(a, b):
        return lax.dot_general(a, b, (dims, ((), ())), preferred_element_type=jnp.float32)

    return one(left[0], right[0]) + (one(left[0], right[1]) + one(left[1], right[0]))


STATES = 5


def layer_kernel(
    span,
    tokens_ref,
    query_ref,
    key_ref,
    value_ref,
    decay_ref,
    gate_ref,
    conv_value_ref,
    conv_admit_ref,
    conv_gate_ref,
    norm_gain_ref,
    base_ref,
    strength_ref,
    group_gain_ref,
    conv_gain_ref,
    pace_ref,
    begin_ref,
    taps_ref,
    point_ref,
    out_conv_ref,
    out_state_ref,
    out_ref,
    sequence,
    weights,
    packed,
    conv_pack,
    gate_pack,
    paces,
    gains,
    wout,
    proj,
    pace_col,
    local_ref,
    map_ref,
    carry_ref,
    add_ref,
    conv_ref,
    state_buf,
    side_buf,
    joined,
    sides,
    result,
    t_send,
    t_recv,
    x_send,
    x_recv,
    p_send,
    p_recv,
    w_send,
    w_recv,
    y_send,
    y_recv,
    c_send,
    c_recv,
    r_send,
    r_recv,
    g_send,
    g_recv,
    o_send,
    o_recv,
    oz_send,
    oz_recv,
    oy_send,
    oy_recv,
    on_send,
    on_recv,
    or_send,
    or_recv,
    es_send,
    es_recv,
    ec_send,
    ec_recv,
    xs_send,
    xs_recv,
    xc_send,
    xc_recv,
    f_send,
    f_recv,
    own_sem,
    tokens_in,
    point_in,
    fetched,
):
    f32 = jnp.float32
    bf16 = jnp.bfloat16
    along = paces.shape[0]
    place = lax.axis_index("sp")
    seat = lax.axis_index("fs")
    side = lax.axis_index("tp")
    other = 1 - side
    near = seat + 1 - 2 * lax.rem(seat, 2)
    far = lax.rem(seat + 2, 4)
    beyond = lax.rem(near + 2, 4)
    row_y = lax.div(seat, 2)
    mine = lax.rem(seat, 2) == side

    length, width = tokens_ref.shape[1:]
    half = length // 2
    total = along * length
    parts = next(n for n in (3, 2, 1) if half % (16 * n) == 0)
    chunk = half // parts
    depth = query_ref.shape[0]
    wide = query_ref.shape[1] // along
    channels = conv_value_ref.shape[1] // along
    size = begin_ref.shape[-1]
    heads = wide // size
    conv_rows = out_conv_ref.shape[0]
    state_rows = out_state_ref.shape[0]
    joint = conv_rows + state_rows
    columns = out_conv_ref.shape[1]
    conv_at = STATES * wide

    pending = []

    def ahead(steps):
        return lax.rem(place + steps, along)

    def behind(steps):
        return lax.rem(place + along - steps, along)

    def aligned(value, size_of):
        return pl.multiple_of(value * size_of, size_of)

    def remote(source, target, send_sem, recv_sem, where):
        return pltpu.make_async_remote_copy(
            src_ref=source,
            dst_ref=target,
            send_sem=send_sem,
            recv_sem=recv_sem,
            device_id=where,
            device_id_type=pl.DeviceIdType.MESH,
        )

    def guarded(valid, action):
        if valid is None:
            action()
        else:
            pl.when(valid)(action)

    def send(source, target, send_sem, recv_sem, where, valid=None, lone=False):
        copy = remote(source, target, send_sem, recv_sem, where)
        guarded(valid, copy.start)
        if lone:
            pending.append((valid, copy))

    def sent(whole, send_sem, where, valid=None):
        pending.append((valid, remote(whole, whole, send_sem, send_sem, where)))

    def arrive(target, send_sem, recv_sem, where, valid=None):
        guarded(valid, remote(target, target, send_sem, recv_sem, where).wait_recv)

    barrier = pltpu.get_barrier_semaphore()
    partners = [{"sp": ahead(s)} for s in range(1, along)]
    partners += [{"fs": near}, {"fs": far}, {"tp": other}]
    for partner in partners:
        pl.semaphore_signal(
            barrier, inc=1, device_id=partner, device_id_type=pl.DeviceIdType.MESH
        )

    state_refs = (query_ref, key_ref, value_ref, decay_ref, gate_ref)

    def rows_of(sp_at, fs_at):
        return pl.ds(aligned(sp_at * 4 + fs_at, depth), depth)

    def packed_of(sp_at, fs_at):
        return pl.ds(aligned(sp_at * 4 + fs_at, depth // 2), depth // 2)

    def fetch(source, target, at):
        pltpu.make_async_copy(source, target, fetched.at[at]).start()

    def fetched_all(target, at):
        pltpu.make_async_copy(target, target, fetched.at[at]).wait()

    own_rows = rows_of(place, seat)
    fetch(tokens_ref.at[0], tokens_in, 0)
    for at, ref in enumerate(state_refs):
        fetch(
            ref.at[:, pl.ds(aligned(place, wide), wide)],
            weights.at[own_rows, pl.ds(at * wide, wide)],
            1,
        )
    fetch(point_ref, point_in, 2)

    for at in range(along):
        cut = slice(at * channels, (at + 1) * channels)
        conv_pack[at] = jnp.concatenate(
            [conv_value_ref[:, cut].astype(f32), conv_admit_ref[:, cut].astype(f32)], axis=1
        ).astype(bf16)
        gate_pack[at] = jnp.concatenate(
            [
                conv_gate_ref[: depth // 2, cut].astype(f32),
                conv_gate_ref[depth // 2 :, cut].astype(f32),
            ],
            axis=1,
        ).astype(bf16)
    weights[own_rows, conv_at : conv_at + 2 * channels] = conv_pack[place]
    packed[packed_of(place, seat), :] = gate_pack[place]
    paces[place] = pace_ref[...]
    gains[side] = conv_gain_ref[...]

    tile = 32

    def normalise(turn, _):
        floats = tokens_in[pl.ds(aligned(turn, tile), tile), :].astype(f32)
        inverse = lax.rsqrt(jnp.mean(floats * floats, axis=1, keepdims=True) + NORM_FLOOR)
        at = pl.ds(pl.multiple_of(place * length + turn * tile, tile), tile)
        sequence[at, :] = (floats * inverse * norm_gain_ref[...]).astype(bf16)
        return 0

    def own_block(at):
        return wout.at[:, pl.ds(aligned(at, columns), columns)]

    pl.semaphore_wait(barrier, len(partners))

    def tokens_at(sp_at, side_at, part):
        first = sp_at * length + side_at * half + part * chunk
        return sequence.at[pl.ds(pl.multiple_of(first, 16), chunk)]

    hops = (
        ({"sp": ahead(1)}, lambda d: place >= d, lambda d: behind(d), place < along - 1),
        ({"sp": behind(1)}, lambda d: place + d < along, lambda d: ahead(d), place > 0),
    )

    def half_of(sp_at, side_at):
        first = sp_at * length + side_at * half
        return sequence.at[pl.ds(pl.multiple_of(first, 16), half)]

    own_slot = (place, along)
    def out_piece(side_at, at):
        cut = pl.ds(aligned(at, columns), columns)
        return (
            wout.at[pl.ds(aligned(side_at, joint), conv_rows), cut],
            wout.at[pl.ds(pl.multiple_of(side_at * joint + conv_rows, 16), state_rows), cut],
        )

    own_at = place * 2 + row_y
    theirs = jnp.logical_not(mine)
    def out_half(side_at):
        return wout.at[pl.ds(aligned(side_at, joint), joint), pl.ds(aligned(own_at, columns), columns)]

    sent(out_half(side), o_send.at[0], {"tp": other}, theirs)
    def piece(sp_at, fs_at, at):
        rows = rows_of(sp_at, fs_at)
        if at < STATES:
            return weights.at[rows, pl.ds(at * wide, wide)]
        if at == STATES:
            return weights.at[rows, pl.ds(conv_at, 2 * channels)]
        return packed.at[packed_of(sp_at, fs_at)]

    groups = ((0, 1, 2, 3, 4, 5), (6,))
    kinds = range(len(groups))
    gate_at = conv_at + 2 * channels

    def grouped(sp_at, fs_at, which):
        rows = rows_of(sp_at, fs_at)
        if which == 0:
            return weights.at[rows, pl.ds(0, gate_at)]
        return packed.at[packed_of(sp_at, fs_at)]

    for way, (onward, _, _, open_end) in enumerate(hops):
        sent(half_of(place, side), t_send.at[own_slot[way]], onward, open_end)

    edge = (place == 0) | (place == along - 1)
    inside = jnp.logical_not(edge)

    def tokens_on(d, chosen, here_if):
        for part in chosen:
            for onward, valid, source, open_end in hops:
                at = source(d)
                ready = valid(d) & here_if
                here = tokens_at(at, side, part)
                arrive(here, t_send.at[at], t_recv.at[at, part], onward, ready)
                if d < along - 1:
                    send(here, here, t_send.at[at], t_recv.at[at, part], onward, ready & open_end)
                send(here, here, x_send.at[0], x_recv.at[at], {"tp": other}, ready)

    for d in range(1, along - 1):
        for onward, valid, source, open_end in hops:
            at = source(d)
            sent(half_of(at, side), t_send.at[at], onward, valid(d) & open_end)
    sent(sequence.at[pl.ds(0, (along - 1) * half)], x_send.at[0], {"tp": other})

    def pass_on(at, which, ready=None):
        here = grouped(at, seat, which)
        send(here, here, y_send.at[which], y_recv.at[at, which], {"fs": far}, ready)
        send(here, here, c_send.at[which], c_recv.at[which], {"fs": near}, ready)

    def spread(d, which):
        for onward, valid, source, _ in hops:
            at = source(d)
            here = grouped(at, seat, which)
            arrive(here, w_send.at[which], w_recv.at[at, which], onward, valid(d))
            pass_on(at, which, valid(d))

    def relay(d, which):
        for _, valid, source, _ in hops if d else hops[:1]:
            at = source(d) if d else place
            ready = valid(d) if d else None
            here = grouped(at, far, which)
            arrive(here, y_send.at[which], y_recv.at[at, which], {"fs": far}, ready)
            send(here, here, r_send.at[which], r_recv.at[which], {"fs": near}, ready)

    def several(count, which):
        if which == 0:
            return weights.at[pl.ds(0, count * depth), pl.ds(0, gate_at)]
        return packed.at[pl.ds(0, count * depth // 2)]

    def hand_out(way, d, which):
        target = (ahead, behind)[way](d)
        reach_of = (place + d < along, place >= d)[way]
        for at in groups[which]:
            if at < STATES:
                source = state_refs[at].at[:, pl.ds(aligned(target, wide), wide)]
            elif at == STATES:
                source = conv_pack.at[target]
            else:
                source = gate_pack.at[target]
            send(
                source,
                piece(place, seat, at),
                w_send.at[which],
                w_recv.at[place, which],
                {"sp": target},
                reach_of,
            )

    for d in range(1, along):
        for which in kinds:
            for way in range(2):
                hand_out(way, d, which)
    fetched_all(tokens_in, 0)
    lax.fori_loop(0, length // tile, normalise, 0)
    fetched_all(weights.at[own_rows, pl.ds(0, conv_at)], 1)
    for which in kinds:
        pass_on(place, which)
    for part in range(parts):
        for way, (onward, _, _, open_end) in enumerate(hops):
            here = tokens_at(place, side, part)
            send(here, here, t_send.at[own_slot[way]], t_recv.at[place, part], onward, open_end)
    for source, target in zip((out_conv_ref, out_state_ref), out_piece(side, own_at)):
        send(source, target, o_send.at[0], o_recv.at[0], {"tp": other}, theirs)
    for source, target in zip((out_conv_ref, out_state_ref), out_piece(side, own_at)):
        pl.when(mine)(pltpu.make_async_copy(source, target, fetched.at[3]).start)
    own_gain = gains.at[side]
    send(
        conv_gain_ref,
        own_gain,
        g_send.at[0],
        g_recv.at[0],
        {"tp": other},
        lone=True,
    )
    for which in kinds:
        sent(several(along - 1, which), w_send.at[which], {"sp": ahead(1)})
        sent(several(along, which), y_send.at[which], {"fs": far})
        sent(several(along, which), c_send.at[which], {"fs": near})
        sent(several(along, which), r_send.at[which], {"fs": near})
    order = sorted(range(1, along), key=lambda s: min(s, along - s))
    for s in order:
        send(pace_ref, paces.at[place], p_send.at[s], p_recv.at[s], {"sp": ahead(s)}, lone=True)

    every_part = range(parts)

    def spread_all(d):
        for which in kinds:
            spread(d, which)

    def relay_all(d):
        for which in kinds:
            relay(d, which)

    spread_all(1)
    relay_all(0)
    tokens_on(1, every_part[:2], edge)
    spread_all(2)
    relay_all(1)
    tokens_on(1, every_part[2:], edge)
    for d in range(3, along):
        spread_all(d)
    for d in range(2, along - 1):
        relay_all(d)
    tokens_on(1, every_part[:1], inside)
    tokens_on(2, every_part[:1], edge)
    relay_all(along - 1)
    tokens_on(1, every_part[1:], inside)

    def out_off():
        arrive(out_half(other), o_send.at[0], o_recv.at[0], {"tp": other}, mine)
        pl.when(mine)(
            pltpu.make_async_copy(out_half(side), out_half(side), fetched.at[3]).wait
        )
        here = own_block(own_at)
        for d in range(1, along):
            for way in range(2):
                target = (ahead, behind)[way](d)
                reach_of = (place + d < along, place >= d)[way]
                send(here, here, oz_send.at[0], oz_recv.at[place], {"sp": target}, mine & reach_of)

    def out_near(at, ready):
        here = own_block(at * 2 + row_y)
        send(here, here, oy_send.at[0], oy_recv.at[at], {"fs": far}, ready)
        send(here, here, on_send.at[0], on_recv.at[at], {"fs": near}, ready)

    def out_on(d):
        for onward, valid, source, _ in hops:
            at = source(d)
            ready = mine & valid(d)
            arrive(own_block(at * 2 + row_y), oz_send.at[0], oz_recv.at[at], onward, ready)
            out_near(at, ready)

    def out_over(d):
        for _, valid, source, _ in hops if d else hops[:1]:
            at = source(d) if d else place
            ready = mine & valid(d) if d else mine
            here = own_block(at * 2 + 1 - row_y)
            arrive(here, oy_send.at[0], oy_recv.at[at], {"fs": far}, ready)
            send(here, here, or_send.at[0], or_recv.at[at], {"fs": near}, ready)

    every = wout.at[:, pl.ds(0, along * columns)]

    def settled(which):
        arrive(several(along, which), c_send.at[which], c_recv.at[which], {"fs": near})
        arrive(several(along, which), r_send.at[which], r_recv.at[which], {"fs": near})

    for s in order:
        arrive(paces.at[behind(s)], p_send.at[s], p_recv.at[s], {"sp": ahead(s)})
    blocks = total // span
    row = lax.broadcasted_iota(jnp.int32, (span, span), 0)
    col = lax.broadcasted_iota(jnp.int32, (span, span), 1)
    eye = (row == col).astype(f32)
    for at in range(along):
        for part in range(length // span):
            line = paces[at][:, part * span : (part + 1) * span]
            first = at * length + part * span
            pace_col[first : first + span, :] = jnp.sum(eye * line, axis=1, keepdims=True)
    for which in kinds:
        settled(which)

    def unpack(turn, _):
        both = packed[pl.ds(aligned(turn, depth // 2), depth // 2), :].astype(f32)
        at = pl.ds(aligned(turn, depth), depth // 2)
        weights[at, gate_at : gate_at + channels] = both[:, :channels].astype(bf16)
        at = pl.ds(pl.multiple_of(turn * depth + depth // 2, depth // 2), depth // 2)
        weights[at, gate_at : gate_at + channels] = both[:, channels:].astype(bf16)
        return 0

    lax.fori_loop(0, along * 4, unpack, 0)


    begins = [begin_ref[0, place * heads + head] for head in range(heads)]
    own_cut = pl.ds(aligned(place, wide), wide)
    base = base_ref[:, own_cut]
    strength = strength_ref[:, own_cut]
    gain = group_gain_ref[:, own_cut]

    strict = (row > col).astype(f32)
    weak = (row >= col).astype(f32)
    masks = jnp.concatenate(
        [jnp.concatenate([strict, strict], axis=1), jnp.concatenate([weak, weak], axis=1)], axis=0
    )
    square = (
        lax.broadcasted_iota(jnp.int32, (size, size), 0)
        == lax.broadcasted_iota(jnp.int32, (size, size), 1)
    ).astype(f32)
    least = min(8, span)
    same = (lax.div(row, least) == lax.div(col, least)).astype(f32)
    merges = []
    reach = least
    while reach < span:
        merges.append(
            (
                (lax.div(row, 2 * reach) == lax.div(col, 2 * reach))
                & (lax.div(row, reach) != lax.div(col, reach))
            ).astype(f32)
        )
        reach = 2 * reach
    weak_bf = weak.astype(bf16)

    def step(turn):
        items = []
        for part in range(length // span):
            block = turn * (length // span) + part
            rows = pl.ds(pl.multiple_of(block * span, span), span)
            query = proj[rows, 0:wide].astype(f32)
            keys = proj[rows, wide : 2 * wide].astype(f32)
            values = proj[rows, 2 * wide : 3 * wide].astype(f32)
            decay_in = proj[rows, 3 * wide : 4 * wide].astype(f32)
            log_keep = -jnp.exp(base + jnp.tanh(decay_in)) * pace_col[rows, :]
            high = log_keep.astype(bf16)
            rest = log_keep - high.astype(f32)
            mid = rest.astype(bf16)
            low = (rest - mid.astype(f32)).astype(bf16)
            summed = (
                jnp.dot(weak_bf, high, preferred_element_type=f32)
                + jnp.dot(weak_bf, mid, preferred_element_type=f32)
                + jnp.dot(weak_bf, low, preferred_element_type=f32)
            )
            last = summed[span - 1 : span, :]
            lead = jnp.exp(summed - log_keep)
            grown = jnp.exp(summed)
            back = jnp.exp(-summed)
            tail = jnp.exp(last - summed)
            ended = jnp.exp(last)
            for head in range(heads):
                at = slice(head * size, (head + 1) * size)
                key = keys[:, at]
                unit = key * lax.rsqrt(
                    jnp.maximum(jnp.sum(key * key, axis=1, keepdims=True), 1.0)
                )
                write = unit * strength[:, at]
                lead_remove = -unit * lead[:, at]
                lead_query = query[:, at] * grown[:, at]
                items.append(
                    dict(
                        at=(block, head),
                        value=values[:, at],
                        lead_remove=lead_remove,
                        lead_query=lead_query,
                        left=jnp.concatenate([lead_remove, lead_query], axis=0),
                        right=jnp.concatenate([write * back[:, at], key * back[:, at]], axis=0),
                        tail_write=write * tail[:, at],
                        tail_key=key * tail[:, at],
                        ended=ended[:, at],
                    )
                )
        for item in items:
            item["pair"] = (
                product(halves(item["left"]), halves(item["right"]), ((1,), (1,))) * masks
            )
        for item in items:
            item["system"] = item["pair"][:span, :span]
            item["power"] = halves(item["system"] * same)
            item["inverse"] = eye + item["system"] * same
        reach = 2
        while reach < least:
            for item in items:
                item["power"] = halves(product(item["power"], item["power"]))
            for item in items:
                item["inverse"] = item["inverse"] + product(
                    halves(item["inverse"]), item["power"]
                )
            reach = 2 * reach
        for item in items:
            padded = jnp.concatenate([jnp.zeros_like(item["value"]), item["value"]], axis=0)
            item["mixed"] = product(halves(item["pair"]), halves(padded))
        for merge in merges:
            for item in items:
                item["inside"] = halves(item["inverse"])
                item["next"] = halves(product(halves(item["system"] * merge), item["inside"]))
            for item in items:
                item["inverse"] = item["inverse"] + product(item["inside"], item["next"])
        for item in items:
            right_side = jnp.concatenate([item["mixed"][:span], item["lead_remove"]], axis=1)
            item["solved"] = halves(product(halves(item["inverse"]), halves(right_side)))
        for item in items:
            block, head = item["at"]
            seen = product(halves(item["pair"][span:, :span]), item["solved"])
            local_ref[head, block] = seen[:, :size] + item["mixed"][span:]
            map_ref[head, block] = item["lead_query"] + seen[:, size:]
            carried = product(item["solved"], halves(item["tail_write"]), ((0,), (0,)))
            carry_ref[head, block] = carried[size:] + square * item["ended"]
            add_ref[head, block] = carried[:size] + product(
                halves(item["value"]), halves(item["tail_key"]), ((0,), (0,))
            )

    def rows_for(at):
        return pl.ds(at * length, length)

    def convolve():
        kernel = taps_ref.shape[0]
        lead_rows = conv_ref.shape[0] - total
        pair = pl.ds(aligned(lax.div(place * channels, 128), 128), 128)
        both_taps = taps_ref[:, pair]
        taps = jnp.where(
            lax.rem(place * channels, 128) == 0, both_taps[:, :channels], both_taps[:, 128 - channels :]
        )
        conv_ref[0:lead_rows, :] = jnp.zeros((lead_rows, channels), f32)
        for block in range(blocks):
            rows = pl.ds(block * span, span)
            value = proj[rows, conv_at : conv_at + channels].astype(f32)
            admit = proj[rows, conv_at + channels : conv_at + 2 * channels].astype(f32)
            conv_ref[pl.ds(lead_rows + block * span, span), :] = (
                (value * jax.nn.sigmoid(admit)).astype(bf16).astype(f32)
            )
        for block in range(blocks):
            summed = jnp.zeros((span, channels), f32)
            for tap in range(kernel):
                first = lead_rows - (kernel - 1) + block * span + tap
                summed = summed + taps[tap : tap + 1, :] * conv_ref[pl.ds(first, span), :]
            rows = pl.ds(block * span, span)
            gate = proj[rows, gate_at : gate_at + channels].astype(f32)
            side_buf[rows, :] = jnp.concatenate([summed, gate], axis=1).astype(bf16)

        for at in range(along):
            target = sides.at[side, place]

            @pl.when(place == at)
            def _():
                sides[side, place] = side_buf[rows_for(at), :]

            away = place != at
            send(
                side_buf.at[rows_for(at)], target, ec_send.at[0], ec_recv.at[place], {"sp": at}, away
            )
            send(
                side_buf.at[rows_for(at)],
                target,
                xc_send.at[0],
                xc_recv.at[0],
                {"tp": other},
                place == at,
            )

    tables = [sorted(range(along), key=lambda q: abs(q - p)) for p in range(along)]

    def turn_of(k):
        found = tables[0][k]
        for p in range(1, along):
            found = jnp.where(place == p, tables[p][k], found)
        return found

    def mix(k):
        at = turn_of(k)
        if k:
            arrive(half_of(at, other), x_send.at[0], x_recv.at[at], {"tp": other})
        rows = pl.ds(aligned(at, length), length)
        proj[rows, :] = jnp.dot(
            sequence[rows, :], weights[...], preferred_element_type=f32
        ).astype(bf16)
        step(at)

    tokens_on(2, every_part[1:2], edge)
    tokens_on(2, every_part[:1], inside)
    mix(0)
    tokens_on(2, every_part[2:], edge)
    tokens_on(2, every_part[1:], inside)
    out_off()
    mix(1)
    for d in range(3, along):
        tokens_on(d, every_part[:2], edge)
    for k in range(2, along - 1):
        mix(k)
    for d in range(3, along):
        tokens_on(d, every_part[2:], edge)
    out_near(place, mine)
    mix(along - 1)
    convolve()
    out_over(0)
    out_on(1)

    def joined_at(side_at, sp_at):
        first = side_at * joint + conv_rows + sp_at * wide
        return joined.at[:, pl.ds(pl.multiple_of(first, 128), wide)]

    states = list(begins)
    for block in range(blocks):
        rows = pl.ds(block * span, span)
        gate = proj[rows, 4 * wide : 5 * wide].astype(f32)
        pieces = []
        for head in range(heads):
            state = halves(states[head])
            out = local_ref[head, block] + product(
                halves(map_ref[head, block]), state, ((1,), (1,))
            )
            states[head] = product(state, halves(carry_ref[head, block])) + add_ref[head, block]
            centered = out - jnp.mean(out, axis=1, keepdims=True)
            variance = jnp.mean(centered * centered, axis=1, keepdims=True)
            pieces.append(centered * lax.rsqrt(variance + GROUP_FLOOR))
        scaled = jnp.concatenate(pieces, axis=1) * gain
        state_buf[rows, :] = (scaled * gate * jax.nn.sigmoid(gate)).astype(bf16)
        if (block + 1) * span % length == 0:
            at = (block + 1) * span // length - 1
            target = joined_at(side, place)

            @pl.when(place == at)
            def _():
                joined[:, pl.ds(
                    pl.multiple_of(side * joint + conv_rows + place * wide, 128), wide
                )] = state_buf[rows_for(at), :]

            source = state_buf.at[rows_for(at)]
            send(source, target, es_send.at[0], es_recv.at[place], {"sp": at}, place != at)
            send(
                source,
                target,
                xs_send.at[0],
                xs_recv.at[0],
                {"tp": other},
                place == at,
            )

    for d in range(2, along - 1):
        out_on(d)
    for s in order:
        here = sides.at[side, behind(s)]
        arrive(here, ec_send.at[0], ec_recv.at[behind(s)], {"sp": ahead(s)})
        send(here, here, xc_send.at[0], xc_recv.at[0], {"tp": other})

    for s in order:
        here = joined_at(side, behind(s))
        arrive(here, es_send.at[0], es_recv.at[behind(s)], {"sp": ahead(s)})
        send(here, here, xs_send.at[0], xs_recv.at[0], {"tp": other})
    out_on(along - 1)
    arrive(sides.at[other], xc_send.at[0], xc_recv.at[0], {"tp": other})
    arrive(gains.at[other], g_send.at[0], g_recv.at[0], {"tp": other})
    whole_gain = jnp.concatenate([gains[0], gains[1]], axis=1)
    piece_rows = next(n for n in (64, 48, 32, 16) if length % n == 0)

    def convolved(turn, _):
        at = pl.ds(aligned(turn, piece_rows), piece_rows)
        sums = jnp.concatenate(
            [
                sides[s, p, at, 0:channels].astype(f32)
                for s in range(2)
                for p in range(along)
            ],
            axis=1,
        )
        gates = jnp.concatenate(
            [
                sides[s, p, at, channels : 2 * channels].astype(f32)
                for s in range(2)
                for p in range(along)
            ],
            axis=1,
        )
        mean = jnp.mean(sums, axis=1, keepdims=True)
        spread_of = jnp.mean(sums * sums, axis=1, keepdims=True) - mean * mean
        shaped = jax.nn.silu(
            (sums - mean) * lax.rsqrt(spread_of + CHANNEL_FLOOR) * whole_gain
        ).astype(bf16)
        pointwise = jnp.dot(shaped, point_in[...], preferred_element_type=f32)
        conv_out = (pointwise * jax.nn.silu(gates)).astype(bf16)
        joined[at, 0:conv_rows] = conv_out[:, :conv_rows]
        joined[at, joint : joint + conv_rows] = conv_out[:, conv_rows:]
        return 0

    fetched_all(point_in, 2)
    lax.fori_loop(0, length // piece_rows, convolved, 0)

    for d in range(1, along):
        out_over(d)
    arrive(state_buf, xs_send.at[0], xs_recv.at[0], {"tp": other})

    ours = pl.ds(pl.multiple_of(side * half, 16), half)
    others = pl.ds(pl.multiple_of(other * half, 16), half)

    def out_cut(at, side_at):
        return pl.ds(aligned(2 * at + side_at, columns), columns)

    for k in range(along):
        zone = turn_of(k)
        arrive(
            own_block(zone * 2 + row_y), on_send.at[0], on_recv.at[zone], {"fs": near}, theirs
        )
        arrive(
            own_block(zone * 2 + 1 - row_y), or_send.at[0], or_recv.at[zone], {"fs": near}, theirs
        )
        cut = pl.ds(aligned(zone, 2 * columns), 2 * columns)
        result[:, cut] = jnp.dot(joined[...], wout[:, cut], preferred_element_type=f32).astype(bf16)
        for at in (zone * 2, zone * 2 + 1):
            piece_cut = pl.ds(aligned(at, columns), columns)
            send(
                result.at[others, piece_cut],
                out_ref.at[:, out_cut(at, side)],
                f_send.at[0],
                f_recv.at[0],
                {"tp": other},
            )
            pltpu.make_async_copy(
                result.at[ours, piece_cut], out_ref.at[:, out_cut(at, side)], own_sem.at[0]
            ).start()
    halfway = result.at[pl.ds(0, half)]
    arrive(halfway, f_send.at[0], f_recv.at[0], {"tp": other})
    pltpu.make_async_copy(halfway, halfway, own_sem.at[0]).wait()
    away_rows = pl.ds(0, (along - 1) * length)
    sent(side_buf.at[away_rows], ec_send.at[0], {"sp": ahead(1)})
    sent(state_buf.at[away_rows], es_send.at[0], {"sp": ahead(1)})
    sent(side_buf, xc_send.at[0], {"tp": other})
    sent(state_buf, xs_send.at[0], {"tp": other})
    sent(wout.at[:, pl.ds(0, (along - 1) * columns)], oz_send.at[0], {"sp": ahead(1)}, mine)
    sent(every, oy_send.at[0], {"fs": far}, mine)
    sent(every, on_send.at[0], {"fs": near}, mine)
    sent(every, or_send.at[0], {"fs": near}, mine)
    sent(halfway, f_send.at[0], {"tp": other})
    for valid, copy in pending:
        guarded(valid, copy.wait_send)


def fused_body(
    tokens,
    decay_pace,
    start_state,
    norm_gain,
    conv_value,
    conv_admit,
    conv_gate,
    state_query,
    state_key,
    state_value,
    state_decay,
    state_gate,
    conv_taps,
    conv_gain,
    point_weight,
    decay_base,
    correction,
    group_gain,
    output_conv,
    output_state,
):
    along = lax.axis_size("sp")
    _, length, width = tokens.shape
    depth, wide = state_query.shape[0], state_query.shape[1] // along
    channels = conv_value.shape[1] // along
    size = start_state.shape[-1]
    heads = wide // size
    total = along * length
    span = 64
    blocks = total // span
    kernel = conv_taps.shape[0]
    joint = output_conv.shape[0] + output_state.shape[0]
    columns = output_conv.shape[1]
    gain_lanes = conv_gain.shape[0]
    f32, bf16 = jnp.float32, jnp.bfloat16
    half = length // 2
    parts = next(n for n in (3, 2, 1) if half % (16 * n) == 0)
    lead_rows = -(-(kernel - 1) // 8) * 8
    dma = pltpu.SemaphoreType.DMA
    maps = pltpu.VMEM((heads, blocks, size, size), f32)
    wout_blocks = along * 2

    def both(*shape):
        return [dma(shape), dma(shape)]

    mixed = pl.pallas_call(
        functools.partial(layer_kernel, span),
        out_shape=jax.ShapeDtypeStruct((half, width), bf16),
        in_specs=[pl.BlockSpec(memory_space=pl.ANY)] * 6
        + [pl.BlockSpec(memory_space=pltpu.VMEM)] * 11
        + [pl.BlockSpec(memory_space=pl.ANY)] * 3,
        out_specs=pl.BlockSpec(memory_space=pl.ANY),
        scratch_shapes=[
            pltpu.VMEM((total, width), bf16),
            pltpu.VMEM((width, 5 * wide + 3 * channels), bf16),
            pltpu.VMEM((width // 2, 2 * channels), bf16),
            pltpu.VMEM((along, depth, 2 * channels), bf16),
            pltpu.VMEM((along, depth // 2, 2 * channels), bf16),
            pltpu.VMEM((along, 1, length), f32),
            pltpu.VMEM((2, 1, gain_lanes), f32),
            pltpu.VMEM((2 * joint, wout_blocks * columns), bf16),
            pltpu.VMEM((total, 5 * wide + 3 * channels), bf16),
            pltpu.VMEM((total, 1), f32),
            pltpu.VMEM((heads, blocks, span, size), f32),
            pltpu.VMEM((heads, blocks, span, size), f32),
            maps,
            maps,
            pltpu.VMEM((lead_rows + total, channels), f32),
            pltpu.VMEM((total, wide), bf16),
            pltpu.VMEM((total, 2 * channels), bf16),
            pltpu.VMEM((length, 2 * joint), bf16),
            pltpu.VMEM((2, along, length, 2 * channels), bf16),
            pltpu.VMEM((length, wout_blocks * columns), bf16),
        ]
        + [dma((along + 1,)), dma((along, parts))]
        + [dma((1,)), dma((along,))]
        + both(along)
        + [dma((2,)), dma((along, 2))]
        + [dma((2,)), dma((along, 2))]
        + both(2)
        + both(2)
        + both(1)
        + both(1)
        + [dma((1,)), dma((along,))]
        + [dma((1,)), dma((along,))]
        + [dma((1,)), dma((along,))]
        + [dma((1,)), dma((along,))]
        + [dma((1,)), dma((along,))]
        + [dma((1,)), dma((along,))]
        + both(1)
        + both(1)
        + both(1)
        + [dma((1,))]
        + [
            pltpu.VMEM((length, width), bf16),
            pltpu.VMEM(point_weight.shape, bf16),
            dma((4,)),
        ],
        compiler_params=pltpu.CompilerParams(
            collective_id=0, has_side_effects=True, vmem_limit_bytes=56 * 1024 * 1024
        ),
        cost_estimate=pl.CostEstimate(
            flops=60_000_000_000, bytes_accessed=8_000_000, transcendentals=0
        ),
        name="layer",
    )(
        tokens,
        state_query,
        state_key,
        state_value,
        state_decay,
        state_gate,
        conv_value,
        conv_admit,
        conv_gate,
        norm_gain[None],
        decay_base[None],
        correction[None],
        group_gain[None],
        conv_gain[None],
        decay_pace,
        start_state,
        conv_taps,
        point_weight,
        output_conv,
        output_state,
    )
    return mixed.reshape(1, half, width)


def dispatch(*arrays):
    along = lax.axis_size("sp")
    tokens, start_state, conv_value, query, output_conv, output_state = (
        arrays[0],
        arrays[2],
        arrays[4],
        arrays[7],
        arrays[18],
        arrays[19],
    )
    depth, width = query.shape[0], tokens.shape[2]
    size = start_state.shape[-1]
    fits = (
        along > 2
        and lax.axis_size("fs") == 4
        and lax.axis_size("tp") == 2
        and tokens.shape[1] % 64 == 0
        and tokens.shape[0] == 1
        and start_state.shape[1] % along == 0
        and size == 64
        and query.shape[1] == along * 128
        and conv_value.shape[1] == along * 64
        and depth % 32 == 0
        and depth * along * 4 == width
        and output_conv.shape[0] == along * 64
        and output_state.shape[0] == along * 128
        and output_conv.shape[1] == 128
        and width == along * 4 * 128
    )
    return (fused_body if fits else body)(*arrays)


def solution(mesh):
    return jax.shard_map(
        dispatch,
        mesh=mesh,
        in_specs=(
            P("fs", "sp", None),
            P("fs", "sp"),
            P("fs", "tp", None, None),
            P(),
            P(("sp", "fs"), "tp"),
            P(("sp", "fs"), "tp"),
            P(("sp", "fs"), "tp"),
            P(("sp", "fs"), "tp"),
            P(("sp", "fs"), "tp"),
            P(("sp", "fs"), "tp"),
            P(("sp", "fs"), "tp"),
            P(("sp", "fs"), "tp"),
            P(None, "tp"),
            P("tp"),
            P(),
            P("tp"),
            P("tp"),
            P("tp"),
            P("tp", ("sp", "fs")),
            P("tp", ("sp", "fs")),
        ),
        out_specs=P("fs", ("sp", "tp"), None),
        check_vma=False,
    )
```

```python
import functools

import jax
import jax.numpy as jnp
from jax import lax
from jax.experimental import pallas as pl
from jax.experimental.pallas import tpu as pltpu
from jax.sharding import PartitionSpec as P

NORM_FLOOR = 0.1
CHANNEL_FLOOR = 0.1
GROUP_FLOOR = 1.0


def passed_along(value, axis, steps):
    count = lax.axis_size(axis)
    leading, last = (max(0, -steps), min(count, count - steps))
    return lax.ppermute(value, axis, [(source, source + steps) for source in range(leading, last)])


def entering_2(value, axis, join, neutral):
    place = lax.axis_index(axis)
    gathered = jax.tree.map(
        lambda a, kind: lax.all_gather(a.astype(kind), axis),
        value,
        jax.tree.map(lambda a: jnp.bfloat16 if a.dtype == jnp.float32 else a.dtype, value),
    )
    state = jax.tree.map(lambda a, e: jnp.zeros_like(a) + jnp.asarray(e, a.dtype), value, neutral)

    def one(lap, state):
        return join(
            state,
            jax.tree.map(
                lambda a, own: lax.dynamic_index_in_dim(a, lap, 0, False).astype(own.dtype),
                gathered,
                value,
            ),
        )

    return lax.fori_loop(0, place, one, state)


def apply_map(matrix, right):
    return jnp.einsum("hbti,hbic->hbtc", matrix, right, precision=lax.Precision.HIGHEST)


def pair_terms(left, right, mask):
    return jnp.einsum("hbtc,hbic->hbti", left, right, precision=lax.Precision.HIGHEST) * mask


def compose(earlier, later):
    first = jnp.matmul(earlier[0], later[0], precision=lax.Precision.HIGHEST)
    second = jnp.matmul(earlier[1], later[0], precision=lax.Precision.HIGHEST) + later[1]
    return (first, second)


def block_terms(query, keys, values, unit, write, log_keep):
    size = query.shape[-1]
    span = query.shape[2]
    total_log = jnp.cumsum(log_keep, axis=2)
    before_log = total_log - log_keep
    last_log = total_log[:, :, span - 1 :, :]
    lead_remove = -unit * jnp.exp(before_log)
    lead_query = query * jnp.exp(total_log)
    back_write = write * jnp.exp(-total_log)
    back_key = keys * jnp.exp(-total_log)
    places = jnp.arange(span)
    strict = (places[:, None] > places[None, :]).astype(jnp.float32)
    weak = (places[:, None] >= places[None, :]).astype(jnp.float32)
    remove_write = pair_terms(lead_remove, back_write, strict)
    remove_key = pair_terms(lead_remove, back_key, strict)
    query_write = pair_terms(lead_query, back_write, weak)
    query_key = pair_terms(lead_query, back_key, weak)
    right_side = jnp.concatenate([apply_map(remove_key, values), lead_remove], axis=-1)
    system = jnp.eye(span, dtype=jnp.float32) - remove_write
    solved = jax.scipy.linalg.solve_triangular(system, right_side, lower=True, unit_diagonal=True)
    own_part = solved[..., :size]
    start_part = solved[..., size:]
    local_out = apply_map(query_write, own_part) + apply_map(query_key, values)
    start_map = lead_query + apply_map(query_write, start_part)
    tail_write = write * jnp.exp(last_log - total_log)
    tail_key = keys * jnp.exp(last_log - total_log)
    carry_map = jnp.einsum(
        "hbtk,hbtj->hbkj", start_part, tail_write, precision=lax.Precision.HIGHEST
    ) + jnp.eye(size, dtype=jnp.float32) * jnp.exp(last_log)
    carry_add = jnp.einsum(
        "hbtv,hbtj->hbvj", own_part, tail_write, precision=lax.Precision.HIGHEST
    ) + jnp.einsum("hbtv,hbtj->hbvj", values, tail_key, precision=lax.Precision.HIGHEST)
    return (local_out, start_map, carry_map, carry_add)


def body(
    tokens,
    decay_pace,
    start_state,
    norm_gain,
    conv_value,
    conv_admit,
    conv_gate,
    state_query,
    state_key,
    state_value,
    state_decay,
    state_gate,
    conv_taps,
    conv_gain,
    point_weight,
    decay_base,
    correction,
    group_gain,
    output_conv,
    output_state,
):
    width = tokens.shape[-1]
    rows = tokens.reshape(-1, width)
    length = rows.shape[0]
    floats = rows.astype(jnp.float32)
    inverse = lax.rsqrt(jnp.mean(floats * floats, axis=1, keepdims=True) + NORM_FLOOR)
    normed = (floats * inverse * norm_gain).astype(jnp.bfloat16)
    shards = (
        conv_value,
        conv_admit,
        conv_gate,
        state_query,
        state_key,
        state_value,
        state_decay,
        state_gate,
    )
    stacked = jnp.concatenate(shards, axis=1)
    projected = jnp.dot(
        normed,
        lax.all_gather(stacked, ("sp", "fs"), axis=0, tiled=True),
        preferred_element_type=jnp.float32,
    ).astype(jnp.bfloat16)
    pieces = []
    offset = 0
    for shard in shards:
        pieces.append(projected[:, offset : offset + shard.shape[1]].astype(jnp.float32))
        offset = offset + shard.shape[1]
    value, admit, gate_conv, query, keys, values, decay_in, gate_state = pieces
    channels = value.shape[1]
    kernel = conv_taps.shape[0]
    conv_input = (value * jax.nn.sigmoid(admit)).astype(jnp.bfloat16)
    earlier = passed_along(conv_input[length - (kernel - 1) :], "sp", 1)
    padded = jnp.concatenate([earlier, conv_input], axis=0).astype(jnp.float32)
    conv_sum = jnp.zeros((length, channels), jnp.float32)
    for place in range(kernel):
        conv_sum = conv_sum + conv_taps[place] * padded[place : place + length]
    local_point = lax.dynamic_slice_in_dim(
        point_weight, lax.axis_index("tp") * channels, channels, 1
    )
    whole_sum, whole_gain = (
        lax.all_gather(conv_sum.astype(jnp.bfloat16), "tp", axis=1, tiled=True).astype(
            conv_sum.dtype
        ),
        lax.all_gather(conv_gain.astype(jnp.bfloat16), "tp", axis=0, tiled=True).astype(
            conv_gain.dtype
        ),
    )
    mean = jnp.mean(whole_sum, axis=1, keepdims=True)
    spread = jnp.mean(whole_sum * whole_sum, axis=1, keepdims=True) - mean * mean
    shaped = jax.nn.silu(
        (whole_sum - mean) * lax.rsqrt(spread + CHANNEL_FLOOR) * whole_gain
    ).astype(jnp.bfloat16)
    pointwise = jnp.dot(shaped, local_point, preferred_element_type=jnp.float32)
    conv_out = (pointwise * jax.nn.silu(gate_conv)).astype(jnp.bfloat16)
    size = start_state.shape[-1]
    heads = query.shape[1] // size
    span = min(64, length)
    blocks = length // span
    log_keep = -jnp.exp(decay_base + jnp.tanh(decay_in)) * decay_pace.reshape(-1)[:, None]
    key_heads = keys.reshape(length, heads, size)
    unit = key_heads * lax.rsqrt(
        jnp.maximum(jnp.sum(key_heads * key_heads, axis=-1, keepdims=True), 1.0)
    )
    write = unit * correction.reshape(heads, size)

    def arrange(array):
        return array.reshape(blocks, span, heads, size).transpose(2, 0, 1, 3)

    local_out, start_map, carry_map, carry_add = block_terms(
        arrange(query),
        arrange(keys),
        arrange(values),
        arrange(unit),
        arrange(write),
        arrange(log_keep),
    )
    identity = (
        jnp.broadcast_to(jnp.eye(size, dtype=jnp.float32), (heads, size, size)),
        jnp.zeros((heads, size, size), jnp.float32),
    )

    def along(carried, block_pair):
        return (compose(carried, block_pair), carried)

    device_pair, prefixes = lax.scan(
        along, identity, (jnp.moveaxis(carry_map, 1, 0), jnp.moveaxis(carry_add, 1, 0))
    )
    prior_map, prior_add = entering_2(device_pair, "sp", compose, identity)
    begin = start_state.reshape(heads, size, size)
    entering = jnp.matmul(begin, prior_map, precision=lax.Precision.HIGHEST) + prior_add
    block_starts = (
        jnp.matmul(entering[None], prefixes[0], precision=lax.Precision.HIGHEST) + prefixes[1]
    )
    block_starts = jnp.moveaxis(block_starts, 0, 1)
    outputs = local_out + jnp.einsum(
        "hbtk,hbvk->hbtv", start_map, block_starts, precision=lax.Precision.HIGHEST
    )
    outputs = outputs.transpose(1, 2, 0, 3).reshape(length, heads, size)
    centered = outputs - jnp.mean(outputs, axis=-1, keepdims=True)
    variance = jnp.mean(centered * centered, axis=-1, keepdims=True)
    grouped = centered * lax.rsqrt(variance + GROUP_FLOOR) * group_gain.reshape(heads, size)
    state_out = (grouped.reshape(length, heads * size) * jax.nn.silu(gate_state)).astype(
        jnp.bfloat16
    )
    local_mix = jnp.concatenate([conv_out, state_out], axis=1)
    moved = lax.all_to_all(local_mix, "tp", split_axis=0, concat_axis=1, tiled=True)
    conv_rows, state_rows = (
        lax.all_gather(output_conv, "tp", axis=0, tiled=True),
        lax.all_gather(output_state, "tp", axis=0, tiled=True),
    )
    groups = lax.axis_size("tp")
    joined = jnp.concatenate(
        [conv_rows.reshape(groups, channels, -1), state_rows.reshape(groups, heads * size, -1)],
        axis=1,
    )
    joined = joined.reshape(groups * (channels + heads * size), -1)
    mixed = jnp.dot(
        moved,
        lax.all_gather(joined, ("sp", "fs"), axis=1, tiled=True),
        preferred_element_type=jnp.float32,
    )
    return mixed.astype(jnp.bfloat16).reshape(1, -1, width)


def halves(array):
    high = array.astype(jnp.bfloat16)
    low = (array - high.astype(jnp.float32)).astype(jnp.bfloat16)
    return (high, low)


def product(left, right, dims=((1,), (0,))):
    def one(a, b):
        return lax.dot_general(a, b, (dims, ((), ())), preferred_element_type=jnp.float32)

    return one(left[0], right[0]) + (one(left[0], right[1]) + one(left[1], right[0]))


STATES = 5


def layer_kernel(
    span,
    tokens_ref,
    query_ref,
    key_ref,
    value_ref,
    decay_ref,
    gate_ref,
    conv_value_hbm,
    conv_admit_hbm,
    conv_gate_hbm,
    norm_gain_hbm,
    base_hbm,
    strength_hbm,
    group_gain_hbm,
    conv_gain_hbm,
    pace_hbm,
    begin_hbm,
    taps_hbm,
    point_ref,
    out_conv_ref,
    out_state_ref,
    out_ref,
    sequence,
    weights,
    packed,
    conv_pack,
    gate_pack,
    paces,
    gains,
    wout,
    proj,
    pace_col,
    local_ref,
    map_ref,
    carry_ref,
    add_ref,
    conv_ref,
    state_buf,
    side_buf,
    joined,
    sides,
    result,
    t_send,
    t_recv,
    x_send,
    x_recv,
    p_send,
    p_recv,
    w_send,
    w_recv,
    y_send,
    y_recv,
    c_send,
    c_recv,
    r_send,
    r_recv,
    g_send,
    g_recv,
    o_send,
    o_recv,
    oz_send,
    oz_recv,
    oy_send,
    oy_recv,
    on_send,
    on_recv,
    or_send,
    or_recv,
    es_send,
    es_recv,
    ec_send,
    ec_recv,
    xs_send,
    xs_recv,
    xc_send,
    xc_recv,
    f_send,
    f_recv,
    own_sem,
    tokens_in,
    point_in,
    fetched,
    conv_value_ref,
    conv_admit_ref,
    conv_gate_ref,
    norm_gain_ref,
    base_ref,
    strength_ref,
    group_gain_ref,
    conv_gain_ref,
    pace_ref,
    begin_ref,
    taps_ref,
):
    f32 = jnp.float32
    bf16 = jnp.bfloat16
    along = paces.shape[0]
    place = lax.axis_index("sp")
    seat = lax.axis_index("fs")
    side = lax.axis_index("tp")
    other = 1 - side
    near = seat + 1 - 2 * lax.rem(seat, 2)
    far = lax.rem(seat + 2, 4)
    beyond = lax.rem(near + 2, 4)
    row_y = lax.div(seat, 2)
    mine = lax.rem(seat, 2) == side

    length, width = tokens_ref.shape[1:]
    half = length // 2
    total = along * length
    parts = next(n for n in (6, 3, 2, 1) if half % (16 * n) == 0)
    chunk = half // parts
    depth = query_ref.shape[0]
    wide = query_ref.shape[1] // along
    channels = conv_value_ref.shape[1] // along
    size = begin_ref.shape[-1]
    heads = wide // size
    conv_rows = out_conv_ref.shape[0]
    state_rows = out_state_ref.shape[0]
    joint = conv_rows + state_rows
    columns = out_conv_ref.shape[1]
    conv_at = STATES * wide

    pending = []

    def ahead(steps):
        return lax.rem(place + steps, along)

    def behind(steps):
        return lax.rem(place + along - steps, along)

    def aligned(value, size_of):
        return pl.multiple_of(value * size_of, size_of)

    def remote(source, target, send_sem, recv_sem, where):
        return pltpu.make_async_remote_copy(
            src_ref=source,
            dst_ref=target,
            send_sem=send_sem,
            recv_sem=recv_sem,
            device_id=where,
            device_id_type=pl.DeviceIdType.MESH,
        )

    def guarded(valid, action):
        if valid is None:
            action()
        else:
            pl.when(valid)(action)

    def send(source, target, send_sem, recv_sem, where, valid=None, lone=False):
        copy = remote(source, target, send_sem, recv_sem, where)
        guarded(valid, copy.start)
        if lone:
            pending.append((valid, copy))

    def sent(whole, send_sem, where, valid=None):
        pending.append((valid, remote(whole, whole, send_sem, send_sem, where)))

    def arrive(target, send_sem, recv_sem, where, valid=None):
        guarded(valid, remote(target, target, send_sem, recv_sem, where).wait_recv)

    barrier = pltpu.get_barrier_semaphore()
    partners = [{"sp": ahead(s)} for s in range(1, along)]
    partners += [{"fs": near}, {"fs": far}, {"tp": other}]
    for partner in partners:
        pl.semaphore_signal(
            barrier, inc=1, device_id=partner, device_id_type=pl.DeviceIdType.MESH
        )

    state_refs = (query_ref, key_ref, value_ref, decay_ref, gate_ref)

    def rows_of(sp_at, fs_at):
        return pl.ds(aligned(sp_at * 4 + fs_at, depth), depth)

    def packed_of(sp_at, fs_at):
        return pl.ds(aligned(sp_at * 4 + fs_at, depth // 2), depth // 2)

    def fetch(source, target, at):
        pltpu.make_async_copy(source, target, fetched.at[at]).start()

    def fetched_all(target, at):
        pltpu.make_async_copy(target, target, fetched.at[at]).wait()

    own_rows = rows_of(place, seat)
    fetch(tokens_ref.at[0], tokens_in, 0)
    for at, ref in enumerate(state_refs):
        fetch(
            ref.at[:, pl.ds(aligned(place, wide), wide)],
            weights.at[own_rows, pl.ds(at * wide, wide)],
            1,
        )
    fetch(point_ref, point_in, 2)
    small = (
        (conv_value_hbm, conv_value_ref),
        (conv_admit_hbm, conv_admit_ref),
        (conv_gate_hbm, conv_gate_ref),
        (norm_gain_hbm, norm_gain_ref),
        (base_hbm, base_ref),
        (strength_hbm, strength_ref),
        (group_gain_hbm, group_gain_ref),
        (conv_gain_hbm, conv_gain_ref),
        (pace_hbm, pace_ref),
        (begin_hbm, begin_ref),
        (taps_hbm, taps_ref),
    )
    for at, (source, target) in enumerate(small):
        fetch(source, target, 4 + at)

    def small_in(first, last):
        for at in range(first, last):
            fetched_all(small[at][1], 4 + at)

    small_in(0, 3)
    for at in range(along):
        cut = slice(at * channels, (at + 1) * channels)
        conv_pack[at] = jnp.concatenate(
            [conv_value_ref[:, cut].astype(f32), conv_admit_ref[:, cut].astype(f32)], axis=1
        ).astype(bf16)
        gate_pack[at] = jnp.concatenate(
            [
                conv_gate_ref[: depth // 2, cut].astype(f32),
                conv_gate_ref[depth // 2 :, cut].astype(f32),
            ],
            axis=1,
        ).astype(bf16)
    weights[own_rows, conv_at : conv_at + 2 * channels] = conv_pack[place]
    packed[packed_of(place, seat), :] = gate_pack[place]

    tile = 32

    def normalise(turn, _):
        floats = tokens_in[pl.ds(aligned(turn, tile), tile), :].astype(f32)
        inverse = lax.rsqrt(jnp.mean(floats * floats, axis=1, keepdims=True) + NORM_FLOOR)
        at = pl.ds(pl.multiple_of(place * length + turn * tile, tile), tile)
        sequence[at, :] = (floats * inverse * norm_gain_ref[...]).astype(bf16)
        return 0

    def own_block(at):
        return wout.at[:, pl.ds(aligned(at, columns), columns)]

    pl.semaphore_wait(barrier, len(partners))

    def tokens_at(sp_at, side_at, part):
        first = sp_at * length + side_at * half + part * chunk
        return sequence.at[pl.ds(pl.multiple_of(first, 16), chunk)]

    hops = (
        ({"sp": ahead(1)}, lambda d: place >= d, lambda d: behind(d), place < along - 1),
        ({"sp": behind(1)}, lambda d: place + d < along, lambda d: ahead(d), place > 0),
    )

    def half_of(sp_at, side_at):
        first = sp_at * length + side_at * half
        return sequence.at[pl.ds(pl.multiple_of(first, 16), half)]

    own_slot = (place, along)
    def out_piece(side_at, at):
        cut = pl.ds(aligned(at, columns), columns)
        return (
            wout.at[pl.ds(aligned(side_at, joint), conv_rows), cut],
            wout.at[pl.ds(pl.multiple_of(side_at * joint + conv_rows, 16), state_rows), cut],
        )

    own_at = place * 2 + row_y
    theirs = jnp.logical_not(mine)
    def out_half(side_at):
        return wout.at[pl.ds(aligned(side_at, joint), joint), pl.ds(aligned(own_at, columns), columns)]

    sent(out_half(side), o_send.at[0], {"tp": other}, theirs)
    def piece(sp_at, fs_at, at):
        rows = rows_of(sp_at, fs_at)
        if at < STATES:
            return weights.at[rows, pl.ds(at * wide, wide)]
        if at == STATES:
            return weights.at[rows, pl.ds(conv_at, 2 * channels)]
        return packed.at[packed_of(sp_at, fs_at)]

    groups = ((0, 1, 2, 3, 4, 5), (6,))
    kinds = range(len(groups))
    gate_at = conv_at + 2 * channels

    def grouped(sp_at, fs_at, which):
        rows = rows_of(sp_at, fs_at)
        if which == 0:
            return weights.at[rows, pl.ds(0, gate_at)]
        return packed.at[packed_of(sp_at, fs_at)]

    for way, (onward, _, _, open_end) in enumerate(hops):
        sent(half_of(place, side), t_send.at[own_slot[way]], onward, open_end)

    edge = (place == 0) | (place == along - 1)
    inside = jnp.logical_not(edge)

    def tokens_on(d, chosen, here_if):
        for part in chosen:
            for onward, valid, source, open_end in hops:
                at = source(d)
                ready = valid(d) & here_if
                here = tokens_at(at, side, part)
                arrive(here, t_send.at[at], t_recv.at[at, part], onward, ready)
                if d < along - 1:
                    send(here, here, t_send.at[at], t_recv.at[at, part], onward, ready & open_end)
                send(here, here, x_send.at[0], x_recv.at[at], {"tp": other}, ready)

    for d in range(1, along - 1):
        for onward, valid, source, open_end in hops:
            at = source(d)
            sent(half_of(at, side), t_send.at[at], onward, valid(d) & open_end)
    sent(sequence.at[pl.ds(0, (along - 1) * half)], x_send.at[0], {"tp": other})

    def pass_on(at, which, ready=None):
        here = grouped(at, seat, which)
        send(here, here, y_send.at[which], y_recv.at[at, which], {"fs": far}, ready)
        send(here, here, c_send.at[which], c_recv.at[which], {"fs": near}, ready)

    def spread(d, which):
        for onward, valid, source, _ in hops:
            at = source(d)
            here = grouped(at, seat, which)
            arrive(here, w_send.at[which], w_recv.at[at, which], onward, valid(d))
            pass_on(at, which, valid(d))

    def relay(d, which):
        for _, valid, source, _ in hops if d else hops[:1]:
            at = source(d) if d else place
            ready = valid(d) if d else None
            here = grouped(at, far, which)
            arrive(here, y_send.at[which], y_recv.at[at, which], {"fs": far}, ready)
            send(here, here, r_send.at[which], r_recv.at[which], {"fs": near}, ready)

    def several(count, which):
        if which == 0:
            return weights.at[pl.ds(0, count * depth), pl.ds(0, gate_at)]
        return packed.at[pl.ds(0, count * depth // 2)]

    def hand_out(way, d, which):
        target = (ahead, behind)[way](d)
        reach_of = (place + d < along, place >= d)[way]
        for at in groups[which]:
            if at < STATES:
                source = state_refs[at].at[:, pl.ds(aligned(target, wide), wide)]
            elif at == STATES:
                source = conv_pack.at[target]
            else:
                source = gate_pack.at[target]
            send(
                source,
                piece(place, seat, at),
                w_send.at[which],
                w_recv.at[place, which],
                {"sp": target},
                reach_of,
            )

    for d in range(1, along):
        for which in kinds:
            for way in range(2):
                hand_out(way, d, which)
    small_in(3, len(small))
    paces[place] = pace_ref[...]
    gains[side] = conv_gain_ref[...]
    fetched_all(tokens_in, 0)
    lax.fori_loop(0, length // tile, normalise, 0)
    fetched_all(weights.at[own_rows, pl.ds(0, conv_at)], 1)
    for which in kinds:
        pass_on(place, which)
    outward = (inside & (place * 2 >= along), inside & (place * 2 < along))

    def tokens_off(late):
        for part in range(parts):
            for way, (onward, _, _, open_end) in enumerate(hops):
                here = tokens_at(place, side, part)
                wanted = outward[way] if late else jnp.logical_not(outward[way])
                send(
                    here,
                    here,
                    t_send.at[own_slot[way]],
                    t_recv.at[place, part],
                    onward,
                    open_end & wanted,
                )

    tokens_off(False)
    for source, target in zip((out_conv_ref, out_state_ref), out_piece(side, own_at)):
        send(source, target, o_send.at[0], o_recv.at[0], {"tp": other}, theirs)
    for source, target in zip((out_conv_ref, out_state_ref), out_piece(side, own_at)):
        pl.when(mine)(pltpu.make_async_copy(source, target, fetched.at[3]).start)
    own_gain = gains.at[side]
    send(
        conv_gain_ref,
        own_gain,
        g_send.at[0],
        g_recv.at[0],
        {"tp": other},
        lone=True,
    )
    for which in kinds:
        sent(several(along - 1, which), w_send.at[which], {"sp": ahead(1)})
        sent(several(along, which), y_send.at[which], {"fs": far})
        sent(several(along, which), c_send.at[which], {"fs": near})
        sent(several(along, which), r_send.at[which], {"fs": near})
    order = sorted(range(1, along), key=lambda s: min(s, along - s))
    for s in order:
        send(pace_ref, paces.at[place], p_send.at[s], p_recv.at[s], {"sp": ahead(s)}, lone=True)

    third = [range(parts * k // 3, parts * (k + 1) // 3) for k in range(3)]

    def thirds(first, last):
        return [part for k in range(first, last) for part in third[k]]

    def spread_all(d):
        for which in kinds:
            spread(d, which)

    def relay_all(d):
        for which in kinds:
            relay(d, which)

    relay_all(0)
    tokens_off(True)
    spread_all(1)
    spread_all(2)
    relay_all(1)
    tokens_on(1, thirds(0, 2), edge)
    for d in range(3, along):
        spread_all(d)
    for d in range(2, along - 1):
        relay_all(d)
    tokens_on(1, thirds(2, 3), edge)
    tokens_on(1, thirds(0, 1), inside)
    relay_all(along - 1)
    tokens_on(2, thirds(0, 1), edge)
    tokens_on(1, thirds(1, 3), inside)

    def out_off():
        arrive(out_half(other), o_send.at[0], o_recv.at[0], {"tp": other}, mine)
        pl.when(mine)(
            pltpu.make_async_copy(out_half(side), out_half(side), fetched.at[3]).wait
        )
        for d in range(1, along):
            for part in range(2):
                here = own_part(own_at, part)
                for way in range(2):
                    target = (ahead, behind)[way](d)
                    reach_of = (place + d < along, place >= d)[way]
                    send(
                        here,
                        here,
                        oz_send.at[0],
                        oz_recv.at[place, part],
                        {"sp": target},
                        mine & reach_of,
                    )

    def own_part(at, part):
        return wout.at[pl.ds(part * joint, joint), pl.ds(aligned(at, columns), columns)]

    def out_near(at, ready, part):
        here = own_part(at * 2 + row_y, part)
        send(here, here, oy_send.at[0], oy_recv.at[at, part], {"fs": far}, ready)
        send(here, here, on_send.at[0], on_recv.at[at], {"fs": near}, ready)

    def out_on(d, chosen=(0, 1)):
        for onward, valid, source, _ in hops:
            at = source(d)
            ready = mine & valid(d)
            for part in chosen:
                arrive(
                    own_part(at * 2 + row_y, part), oz_send.at[0], oz_recv.at[at, part], onward, ready
                )
                out_near(at, ready, part)

    def out_over(d, here_if=True):
        for _, valid, source, _ in hops if d else hops[:1]:
            at = source(d) if d else place
            ready = mine & valid(d) & here_if if d else mine
            for part in range(2):
                here = own_part(at * 2 + 1 - row_y, part)
                arrive(here, oy_send.at[0], oy_recv.at[at, part], {"fs": far}, ready)
                send(here, here, or_send.at[0], or_recv.at[at], {"fs": near}, ready)

    every = wout.at[:, pl.ds(0, along * columns)]

    def settled(which):
        arrive(several(along, which), c_send.at[which], c_recv.at[which], {"fs": near})
        arrive(several(along, which), r_send.at[which], r_recv.at[which], {"fs": near})

    for s in order:
        arrive(paces.at[behind(s)], p_send.at[s], p_recv.at[s], {"sp": ahead(s)})
    blocks = total // span
    row = lax.broadcasted_iota(jnp.int32, (span, span), 0)
    col = lax.broadcasted_iota(jnp.int32, (span, span), 1)
    eye = (row == col).astype(f32)
    for at in range(along):
        for part in range(length // span):
            line = paces[at][:, part * span : (part + 1) * span]
            first = at * length + part * span
            pace_col[first : first + span, :] = jnp.sum(eye * line, axis=1, keepdims=True)
    for which in kinds:
        settled(which)

    def unpack(turn, _):
        both = packed[pl.ds(aligned(turn, depth // 2), depth // 2), :].astype(f32)
        at = pl.ds(aligned(turn, depth), depth // 2)
        weights[at, gate_at : gate_at + channels] = both[:, :channels].astype(bf16)
        at = pl.ds(pl.multiple_of(turn * depth + depth // 2, depth // 2), depth // 2)
        weights[at, gate_at : gate_at + channels] = both[:, channels:].astype(bf16)
        return 0

    lax.fori_loop(0, along * 4, unpack, 0)


    begins = [begin_ref[0, place * heads + head] for head in range(heads)]
    own_cut = pl.ds(aligned(place, wide), wide)
    base = base_ref[:, own_cut]
    strength = strength_ref[:, own_cut]
    gain = group_gain_ref[:, own_cut]

    strict = (row > col).astype(f32)
    weak = (row >= col).astype(f32)
    masks = jnp.concatenate(
        [jnp.concatenate([strict, strict], axis=1), jnp.concatenate([weak, weak], axis=1)], axis=0
    )
    square = (
        lax.broadcasted_iota(jnp.int32, (size, size), 0)
        == lax.broadcasted_iota(jnp.int32, (size, size), 1)
    ).astype(f32)
    least = min(8, span)
    same = (lax.div(row, least) == lax.div(col, least)).astype(f32)
    merges = []
    reach = least
    while reach < span:
        merges.append(
            (
                (lax.div(row, 2 * reach) == lax.div(col, 2 * reach))
                & (lax.div(row, reach) != lax.div(col, reach))
            ).astype(f32)
        )
        reach = 2 * reach
    weak_bf = weak.astype(bf16)

    def step(turn):
        items = []
        for part in range(length // span):
            block = turn * (length // span) + part
            rows = pl.ds(pl.multiple_of(block * span, span), span)
            query = proj[rows, 0:wide].astype(f32)
            keys = proj[rows, wide : 2 * wide].astype(f32)
            values = proj[rows, 2 * wide : 3 * wide].astype(f32)
            decay_in = proj[rows, 3 * wide : 4 * wide].astype(f32)
            log_keep = -jnp.exp(base + jnp.tanh(decay_in)) * pace_col[rows, :]
            high = log_keep.astype(bf16)
            rest = log_keep - high.astype(f32)
            mid = rest.astype(bf16)
            low = (rest - mid.astype(f32)).astype(bf16)
            summed = (
                jnp.dot(weak_bf, high, preferred_element_type=f32)
                + jnp.dot(weak_bf, mid, preferred_element_type=f32)
                + jnp.dot(weak_bf, low, preferred_element_type=f32)
            )
            last = summed[span - 1 : span, :]
            lead = jnp.exp(summed - log_keep)
            grown = jnp.exp(summed)
            back = jnp.exp(-summed)
            tail = jnp.exp(last - summed)
            ended = jnp.exp(last)
            for head in range(heads):
                at = slice(head * size, (head + 1) * size)
                key = keys[:, at]
                unit = key * lax.rsqrt(
                    jnp.maximum(jnp.sum(key * key, axis=1, keepdims=True), 1.0)
                )
                write = unit * strength[:, at]
                lead_remove = -unit * lead[:, at]
                lead_query = query[:, at] * grown[:, at]
                items.append(
                    dict(
                        at=(block, head),
                        value=values[:, at],
                        lead_remove=lead_remove,
                        lead_query=lead_query,
                        left=jnp.concatenate([lead_remove, lead_query], axis=0),
                        right=jnp.concatenate([write * back[:, at], key * back[:, at]], axis=0),
                        tail_write=write * tail[:, at],
                        tail_key=key * tail[:, at],
                        ended=ended[:, at],
                    )
                )
        for item in items:
            item["pair"] = (
                product(halves(item["left"]), halves(item["right"]), ((1,), (1,))) * masks
            )
        for item in items:
            item["system"] = item["pair"][:span, :span]
            item["power"] = halves(item["system"] * same)
            item["inverse"] = eye + item["system"] * same
        reach = 2
        while reach < least:
            for item in items:
                item["power"] = halves(product(item["power"], item["power"]))
            for item in items:
                item["inverse"] = item["inverse"] + product(
                    halves(item["inverse"]), item["power"]
                )
            reach = 2 * reach
        for item in items:
            padded = jnp.concatenate([jnp.zeros_like(item["value"]), item["value"]], axis=0)
            item["mixed"] = product(halves(item["pair"]), halves(padded))
        for merge in merges:
            for item in items:
                item["inside"] = halves(item["inverse"])
                item["next"] = halves(product(halves(item["system"] * merge), item["inside"]))
            for item in items:
                item["inverse"] = item["inverse"] + product(item["inside"], item["next"])
        for item in items:
            right_side = jnp.concatenate([item["mixed"][:span], item["lead_remove"]], axis=1)
            item["solved"] = halves(product(halves(item["inverse"]), halves(right_side)))
        for item in items:
            block, head = item["at"]
            seen = product(halves(item["pair"][span:, :span]), item["solved"])
            local_ref[head, block] = seen[:, :size] + item["mixed"][span:]
            map_ref[head, block] = item["lead_query"] + seen[:, size:]
            carried = product(item["solved"], halves(item["tail_write"]), ((0,), (0,)))
            carry_ref[head, block] = carried[size:] + square * item["ended"]
            add_ref[head, block] = carried[:size] + product(
                halves(item["value"]), halves(item["tail_key"]), ((0,), (0,))
            )

    def rows_for(at):
        return pl.ds(at * length, length)

    def convolve():
        kernel = taps_ref.shape[0]
        lead_rows = conv_ref.shape[0] - total
        pair = pl.ds(aligned(lax.div(place * channels, 128), 128), 128)
        both_taps = taps_ref[:, pair]
        taps = jnp.where(
            lax.rem(place * channels, 128) == 0, both_taps[:, :channels], both_taps[:, 128 - channels :]
        )
        conv_ref[0:lead_rows, :] = jnp.zeros((lead_rows, channels), f32)
        for block in range(blocks):
            rows = pl.ds(block * span, span)
            value = proj[rows, conv_at : conv_at + channels].astype(f32)
            admit = proj[rows, conv_at + channels : conv_at + 2 * channels].astype(f32)
            conv_ref[pl.ds(lead_rows + block * span, span), :] = (
                (value * jax.nn.sigmoid(admit)).astype(bf16).astype(f32)
            )
        for block in range(blocks):
            summed = jnp.zeros((span, channels), f32)
            for tap in range(kernel):
                first = lead_rows - (kernel - 1) + block * span + tap
                summed = summed + taps[tap : tap + 1, :] * conv_ref[pl.ds(first, span), :]
            rows = pl.ds(block * span, span)
            gate = proj[rows, gate_at : gate_at + channels].astype(f32)
            side_buf[rows, :] = jnp.concatenate([summed, gate], axis=1).astype(bf16)

        for at in range(along):
            target = sides.at[side, place]

            @pl.when(place == at)
            def _():
                sides[side, place] = side_buf[rows_for(at), :]

            away = place != at
            send(
                side_buf.at[rows_for(at)], target, ec_send.at[0], ec_recv.at[place], {"sp": at}, away
            )
            send(
                side_buf.at[rows_for(at)],
                target,
                xc_send.at[0],
                xc_recv.at[0],
                {"tp": other},
                place == at,
            )

    tables = [sorted(range(along), key=lambda q: abs(q - p)) for p in range(along)]

    def turn_of(k):
        found = tables[0][k]
        for p in range(1, along):
            found = jnp.where(place == p, tables[p][k], found)
        return found

    def mix(k, between=None):
        at = turn_of(k)
        if k:
            arrive(half_of(at, other), x_send.at[0], x_recv.at[at], {"tp": other})
        rows = pl.ds(aligned(at, length), length)
        proj[rows, :] = jnp.dot(
            sequence[rows, :], weights[...], preferred_element_type=f32
        ).astype(bf16)
        if between is not None:
            between()
        step(at)

    tokens_on(2, thirds(1, 2), edge)
    tokens_on(2, thirds(0, 1), inside)
    mix(0)
    tokens_on(2, thirds(2, 3), edge)
    tokens_on(2, thirds(1, 3), inside)
    out_off()
    for part in range(2):
        out_near(place, mine, part)
    def first_far():
        for d in range(3, along):
            tokens_on(d, thirds(0, 1), edge)

    mix(1, first_far)
    for d in range(3, along):
        tokens_on(d, thirds(1, 2), edge)
    for k in range(2, along - 1):
        mix(k)
    for d in range(3, along):
        tokens_on(d, thirds(2, 3), edge)
    out_over(0)
    out_on(1)
    mix(along - 1)
    convolve()

    def joined_at(side_at, sp_at):
        first = side_at * joint + conv_rows + sp_at * wide
        return joined.at[:, pl.ds(pl.multiple_of(first, 128), wide)]

    states = list(begins)
    for block in range(blocks):
        rows = pl.ds(block * span, span)
        gate = proj[rows, 4 * wide : 5 * wide].astype(f32)
        pieces = []
        for head in range(heads):
            state = halves(states[head])
            out = local_ref[head, block] + product(
                halves(map_ref[head, block]), state, ((1,), (1,))
            )
            states[head] = product(state, halves(carry_ref[head, block])) + add_ref[head, block]
            centered = out - jnp.mean(out, axis=1, keepdims=True)
            variance = jnp.mean(centered * centered, axis=1, keepdims=True)
            pieces.append(centered * lax.rsqrt(variance + GROUP_FLOOR))
        scaled = jnp.concatenate(pieces, axis=1) * gain
        state_buf[rows, :] = (scaled * gate * jax.nn.sigmoid(gate)).astype(bf16)
        if (block + 1) * span % length == 0:
            at = (block + 1) * span // length - 1
            target = joined_at(side, place)

            @pl.when(place == at)
            def _():
                joined[:, pl.ds(
                    pl.multiple_of(side * joint + conv_rows + place * wide, 128), wide
                )] = state_buf[rows_for(at), :]

            source = state_buf.at[rows_for(at)]
            send(source, target, es_send.at[0], es_recv.at[place], {"sp": at}, place != at)
            send(
                source,
                target,
                xs_send.at[0],
                xs_recv.at[0],
                {"tp": other},
                place == at,
            )

    for d in range(2, along - 1):
        out_on(d)
    for s in order:
        here = sides.at[side, behind(s)]
        arrive(here, ec_send.at[0], ec_recv.at[behind(s)], {"sp": ahead(s)})
        send(here, here, xc_send.at[0], xc_recv.at[0], {"tp": other})

    out_on(along - 1)
    out_over(1)
    for s in order:
        here = joined_at(side, behind(s))
        arrive(here, es_send.at[0], es_recv.at[behind(s)], {"sp": ahead(s)})
        send(here, here, xs_send.at[0], xs_recv.at[0], {"tp": other})
    arrive(sides.at[other], xc_send.at[0], xc_recv.at[0], {"tp": other})
    arrive(gains.at[other], g_send.at[0], g_recv.at[0], {"tp": other})
    whole_gain = jnp.concatenate([gains[0], gains[1]], axis=1)
    piece_rows = next(n for n in (64, 48, 32, 16) if length % n == 0)

    def convolved(turn, _):
        at = pl.ds(aligned(turn, piece_rows), piece_rows)
        sums = jnp.concatenate(
            [
                sides[s, p, at, 0:channels].astype(f32)
                for s in range(2)
                for p in range(along)
            ],
            axis=1,
        )
        gates = jnp.concatenate(
            [
                sides[s, p, at, channels : 2 * channels].astype(f32)
                for s in range(2)
                for p in range(along)
            ],
            axis=1,
        )
        mean = jnp.mean(sums, axis=1, keepdims=True)
        spread_of = jnp.mean(sums * sums, axis=1, keepdims=True) - mean * mean
        shaped = jax.nn.silu(
            (sums - mean) * lax.rsqrt(spread_of + CHANNEL_FLOOR) * whole_gain
        ).astype(bf16)
        pointwise = jnp.dot(shaped, point_in[...], preferred_element_type=f32)
        conv_out = (pointwise * jax.nn.silu(gates)).astype(bf16)
        joined[at, 0:conv_rows] = conv_out[:, :conv_rows]
        joined[at, joint : joint + conv_rows] = conv_out[:, conv_rows:]
        return 0

    fetched_all(point_in, 2)
    lax.fori_loop(0, length // piece_rows, convolved, 0)

    arrive(state_buf, xs_send.at[0], xs_recv.at[0], {"tp": other})

    ours = pl.ds(pl.multiple_of(side * half, 16), half)
    others = pl.ds(pl.multiple_of(other * half, 16), half)

    def out_cut(at, side_at):
        return pl.ds(aligned(2 * at + side_at, columns), columns)

    for k in range(along):
        zone = turn_of(k)
        if 1 < k < along - 1:
            out_over(k, edge)
        if k == along - 1:
            for d in range(2, k):
                out_over(d, inside)
            out_over(k)
        arrive(
            own_block(zone * 2 + row_y), on_send.at[0], on_recv.at[zone], {"fs": near}, theirs
        )
        arrive(
            own_block(zone * 2 + 1 - row_y), or_send.at[0], or_recv.at[zone], {"fs": near}, theirs
        )
        cut = pl.ds(aligned(zone, 2 * columns), 2 * columns)
        result[:, cut] = jnp.dot(joined[...], wout[:, cut], preferred_element_type=f32).astype(bf16)
        for at in (zone * 2, zone * 2 + 1):
            piece_cut = pl.ds(aligned(at, columns), columns)
            send(
                result.at[others, piece_cut],
                out_ref.at[:, out_cut(at, side)],
                f_send.at[0],
                f_recv.at[0],
                {"tp": other},
            )
            pltpu.make_async_copy(
                result.at[ours, piece_cut], out_ref.at[:, out_cut(at, side)], own_sem.at[0]
            ).start()
    halfway = result.at[pl.ds(0, half)]
    arrive(halfway, f_send.at[0], f_recv.at[0], {"tp": other})
    pltpu.make_async_copy(halfway, halfway, own_sem.at[0]).wait()
    away_rows = pl.ds(0, (along - 1) * length)
    sent(side_buf.at[away_rows], ec_send.at[0], {"sp": ahead(1)})
    sent(state_buf.at[away_rows], es_send.at[0], {"sp": ahead(1)})
    sent(side_buf, xc_send.at[0], {"tp": other})
    sent(state_buf, xs_send.at[0], {"tp": other})
    sent(wout.at[:, pl.ds(0, (along - 1) * columns)], oz_send.at[0], {"sp": ahead(1)}, mine)
    sent(every, oy_send.at[0], {"fs": far}, mine)
    sent(every, on_send.at[0], {"fs": near}, mine)
    sent(every, or_send.at[0], {"fs": near}, mine)
    sent(halfway, f_send.at[0], {"tp": other})
    for valid, copy in pending:
        guarded(valid, copy.wait_send)


def fused_body(
    tokens,
    decay_pace,
    start_state,
    norm_gain,
    conv_value,
    conv_admit,
    conv_gate,
    state_query,
    state_key,
    state_value,
    state_decay,
    state_gate,
    conv_taps,
    conv_gain,
    point_weight,
    decay_base,
    correction,
    group_gain,
    output_conv,
    output_state,
):
    along = lax.axis_size("sp")
    _, length, width = tokens.shape
    depth, wide = state_query.shape[0], state_query.shape[1] // along
    channels = conv_value.shape[1] // along
    size = start_state.shape[-1]
    heads = wide // size
    total = along * length
    span = 64
    blocks = total // span
    kernel = conv_taps.shape[0]
    joint = output_conv.shape[0] + output_state.shape[0]
    columns = output_conv.shape[1]
    gain_lanes = conv_gain.shape[0]
    f32, bf16 = jnp.float32, jnp.bfloat16
    half = length // 2
    parts = next(n for n in (6, 3, 2, 1) if half % (16 * n) == 0)
    lead_rows = -(-(kernel - 1) // 8) * 8
    dma = pltpu.SemaphoreType.DMA
    maps = pltpu.VMEM((heads, blocks, size, size), f32)
    wout_blocks = along * 2

    def both(*shape):
        return [dma(shape), dma(shape)]

    mixed = pl.pallas_call(
        functools.partial(layer_kernel, span),
        out_shape=jax.ShapeDtypeStruct((half, width), bf16),
        in_specs=[pl.BlockSpec(memory_space=pl.ANY)] * 20,
        out_specs=pl.BlockSpec(memory_space=pl.ANY),
        scratch_shapes=[
            pltpu.VMEM((total, width), bf16),
            pltpu.VMEM((width, 5 * wide + 3 * channels), bf16),
            pltpu.VMEM((width // 2, 2 * channels), bf16),
            pltpu.VMEM((along, depth, 2 * channels), bf16),
            pltpu.VMEM((along, depth // 2, 2 * channels), bf16),
            pltpu.VMEM((along, 1, length), f32),
            pltpu.VMEM((2, 1, gain_lanes), f32),
            pltpu.VMEM((2 * joint, wout_blocks * columns), bf16),
            pltpu.VMEM((total, 5 * wide + 3 * channels), bf16),
            pltpu.VMEM((total, 1), f32),
            pltpu.VMEM((heads, blocks, span, size), f32),
            pltpu.VMEM((heads, blocks, span, size), f32),
            maps,
            maps,
            pltpu.VMEM((lead_rows + total, channels), f32),
            pltpu.VMEM((total, wide), bf16),
            pltpu.VMEM((total, 2 * channels), bf16),
            pltpu.VMEM((length, 2 * joint), bf16),
            pltpu.VMEM((2, along, length, 2 * channels), bf16),
            pltpu.VMEM((length, wout_blocks * columns), bf16),
        ]
        + [dma((along + 1,)), dma((along, parts))]
        + [dma((1,)), dma((along,))]
        + both(along)
        + [dma((2,)), dma((along, 2))]
        + [dma((2,)), dma((along, 2))]
        + both(2)
        + both(2)
        + both(1)
        + both(1)
        + [dma((1,)), dma((along, 2))]
        + [dma((1,)), dma((along, 2))]
        + [dma((1,)), dma((along,))]
        + [dma((1,)), dma((along,))]
        + [dma((1,)), dma((along,))]
        + [dma((1,)), dma((along,))]
        + both(1)
        + both(1)
        + both(1)
        + [dma((1,))]
        + [
            pltpu.VMEM((length, width), bf16),
            pltpu.VMEM(point_weight.shape, bf16),
            dma((15,)),
            pltpu.VMEM(conv_value.shape, bf16),
            pltpu.VMEM(conv_admit.shape, bf16),
            pltpu.VMEM(conv_gate.shape, bf16),
            pltpu.VMEM((1, width), f32),
            pltpu.VMEM((1, decay_base.shape[0]), f32),
            pltpu.VMEM((1, correction.shape[0]), f32),
            pltpu.VMEM((1, group_gain.shape[0]), f32),
            pltpu.VMEM((1, gain_lanes), f32),
            pltpu.VMEM(decay_pace.shape, f32),
            pltpu.VMEM(start_state.shape, f32),
            pltpu.VMEM(conv_taps.shape, f32),
        ],
        compiler_params=pltpu.CompilerParams(
            collective_id=0, has_side_effects=True, vmem_limit_bytes=56 * 1024 * 1024
        ),
        cost_estimate=pl.CostEstimate(
            flops=60_000_000_000, bytes_accessed=8_000_000, transcendentals=0
        ),
        name="layer",
    )(
        tokens,
        state_query,
        state_key,
        state_value,
        state_decay,
        state_gate,
        conv_value,
        conv_admit,
        conv_gate,
        norm_gain[None],
        decay_base[None],
        correction[None],
        group_gain[None],
        conv_gain[None],
        decay_pace,
        start_state,
        conv_taps,
        point_weight,
        output_conv,
        output_state,
    )
    return mixed.reshape(1, half, width)


def dispatch(*arrays):
    along = lax.axis_size("sp")
    tokens, start_state, conv_value, query, output_conv, output_state = (
        arrays[0],
        arrays[2],
        arrays[4],
        arrays[7],
        arrays[18],
        arrays[19],
    )
    depth, width = query.shape[0], tokens.shape[2]
    size = start_state.shape[-1]
    fits = (
        along == 4
        and lax.axis_size("fs") == 4
        and lax.axis_size("tp") == 2
        and tokens.shape[1] % 64 == 0
        and tokens.shape[0] == 1
        and start_state.shape[1] % along == 0
        and size == 64
        and query.shape[1] == along * 128
        and conv_value.shape[1] == along * 64
        and depth % 32 == 0
        and depth * along * 4 == width
        and output_conv.shape[0] == along * 64
        and output_state.shape[0] == along * 128
        and output_conv.shape[1] == 128
        and width == along * 4 * 128
    )
    return (fused_body if fits else body)(*arrays)


def solution(mesh):
    return jax.shard_map(
        dispatch,
        mesh=mesh,
        in_specs=(
            P("fs", "sp", None),
            P("fs", "sp"),
            P("fs", "tp", None, None),
            P(),
            P(("sp", "fs"), "tp"),
            P(("sp", "fs"), "tp"),
            P(("sp", "fs"), "tp"),
            P(("sp", "fs"), "tp"),
            P(("sp", "fs"), "tp"),
            P(("sp", "fs"), "tp"),
            P(("sp", "fs"), "tp"),
            P(("sp", "fs"), "tp"),
            P(None, "tp"),
            P("tp"),
            P(),
            P("tp"),
            P("tp"),
            P("tp"),
            P("tp", ("sp", "fs")),
            P("tp", ("sp", "fs")),
        ),
        out_specs=P("fs", ("sp", "tp"), None),
        check_vma=False,
    )
```

```python
import functools

import jax
import jax.numpy as jnp
from jax import lax
from jax.experimental import pallas as pl
from jax.experimental.pallas import tpu as pltpu
from jax.sharding import PartitionSpec as P

NORM_FLOOR = 0.1
CHANNEL_FLOOR = 0.1
GROUP_FLOOR = 1.0


def passed_along(value, axis, steps):
    count = lax.axis_size(axis)
    leading, last = (max(0, -steps), min(count, count - steps))
    return lax.ppermute(value, axis, [(source, source + steps) for source in range(leading, last)])


def entering_2(value, axis, join, neutral):
    place = lax.axis_index(axis)
    gathered = jax.tree.map(
        lambda a, kind: lax.all_gather(a.astype(kind), axis),
        value,
        jax.tree.map(lambda a: jnp.bfloat16 if a.dtype == jnp.float32 else a.dtype, value),
    )
    state = jax.tree.map(lambda a, e: jnp.zeros_like(a) + jnp.asarray(e, a.dtype), value, neutral)

    def one(lap, state):
        return join(
            state,
            jax.tree.map(
                lambda a, own: lax.dynamic_index_in_dim(a, lap, 0, False).astype(own.dtype),
                gathered,
                value,
            ),
        )

    return lax.fori_loop(0, place, one, state)


def apply_map(matrix, right):
    return jnp.einsum("hbti,hbic->hbtc", matrix, right, precision=lax.Precision.HIGHEST)


def pair_terms(left, right, mask):
    return jnp.einsum("hbtc,hbic->hbti", left, right, precision=lax.Precision.HIGHEST) * mask


def compose(earlier, later):
    first = jnp.matmul(earlier[0], later[0], precision=lax.Precision.HIGHEST)
    second = jnp.matmul(earlier[1], later[0], precision=lax.Precision.HIGHEST) + later[1]
    return (first, second)


def block_terms(query, keys, values, unit, write, log_keep):
    size = query.shape[-1]
    span = query.shape[2]
    total_log = jnp.cumsum(log_keep, axis=2)
    before_log = total_log - log_keep
    last_log = total_log[:, :, span - 1 :, :]
    lead_remove = -unit * jnp.exp(before_log)
    lead_query = query * jnp.exp(total_log)
    back_write = write * jnp.exp(-total_log)
    back_key = keys * jnp.exp(-total_log)
    places = jnp.arange(span)
    strict = (places[:, None] > places[None, :]).astype(jnp.float32)
    weak = (places[:, None] >= places[None, :]).astype(jnp.float32)
    remove_write = pair_terms(lead_remove, back_write, strict)
    remove_key = pair_terms(lead_remove, back_key, strict)
    query_write = pair_terms(lead_query, back_write, weak)
    query_key = pair_terms(lead_query, back_key, weak)
    right_side = jnp.concatenate([apply_map(remove_key, values), lead_remove], axis=-1)
    system = jnp.eye(span, dtype=jnp.float32) - remove_write
    solved = jax.scipy.linalg.solve_triangular(system, right_side, lower=True, unit_diagonal=True)
    own_part = solved[..., :size]
    start_part = solved[..., size:]
    local_out = apply_map(query_write, own_part) + apply_map(query_key, values)
    start_map = lead_query + apply_map(query_write, start_part)
    tail_write = write * jnp.exp(last_log - total_log)
    tail_key = keys * jnp.exp(last_log - total_log)
    carry_map = jnp.einsum(
        "hbtk,hbtj->hbkj", start_part, tail_write, precision=lax.Precision.HIGHEST
    ) + jnp.eye(size, dtype=jnp.float32) * jnp.exp(last_log)
    carry_add = jnp.einsum(
        "hbtv,hbtj->hbvj", own_part, tail_write, precision=lax.Precision.HIGHEST
    ) + jnp.einsum("hbtv,hbtj->hbvj", values, tail_key, precision=lax.Precision.HIGHEST)
    return (local_out, start_map, carry_map, carry_add)


def body(
    tokens,
    decay_pace,
    start_state,
    norm_gain,
    conv_value,
    conv_admit,
    conv_gate,
    state_query,
    state_key,
    state_value,
    state_decay,
    state_gate,
    conv_taps,
    conv_gain,
    point_weight,
    decay_base,
    correction,
    group_gain,
    output_conv,
    output_state,
):
    width = tokens.shape[-1]
    rows = tokens.reshape(-1, width)
    length = rows.shape[0]
    floats = rows.astype(jnp.float32)
    inverse = lax.rsqrt(jnp.mean(floats * floats, axis=1, keepdims=True) + NORM_FLOOR)
    normed = (floats * inverse * norm_gain).astype(jnp.bfloat16)
    shards = (
        conv_value,
        conv_admit,
        conv_gate,
        state_query,
        state_key,
        state_value,
        state_decay,
        state_gate,
    )
    stacked = jnp.concatenate(shards, axis=1)
    projected = jnp.dot(
        normed,
        lax.all_gather(stacked, ("sp", "fs"), axis=0, tiled=True),
        preferred_element_type=jnp.float32,
    ).astype(jnp.bfloat16)
    pieces = []
    offset = 0
    for shard in shards:
        pieces.append(projected[:, offset : offset + shard.shape[1]].astype(jnp.float32))
        offset = offset + shard.shape[1]
    value, admit, gate_conv, query, keys, values, decay_in, gate_state = pieces
    channels = value.shape[1]
    kernel = conv_taps.shape[0]
    conv_input = (value * jax.nn.sigmoid(admit)).astype(jnp.bfloat16)
    earlier = passed_along(conv_input[length - (kernel - 1) :], "sp", 1)
    padded = jnp.concatenate([earlier, conv_input], axis=0).astype(jnp.float32)
    conv_sum = jnp.zeros((length, channels), jnp.float32)
    for place in range(kernel):
        conv_sum = conv_sum + conv_taps[place] * padded[place : place + length]
    local_point = lax.dynamic_slice_in_dim(
        point_weight, lax.axis_index("tp") * channels, channels, 1
    )
    whole_sum, whole_gain = (
        lax.all_gather(conv_sum.astype(jnp.bfloat16), "tp", axis=1, tiled=True).astype(
            conv_sum.dtype
        ),
        lax.all_gather(conv_gain.astype(jnp.bfloat16), "tp", axis=0, tiled=True).astype(
            conv_gain.dtype
        ),
    )
    mean = jnp.mean(whole_sum, axis=1, keepdims=True)
    spread = jnp.mean(whole_sum * whole_sum, axis=1, keepdims=True) - mean * mean
    shaped = jax.nn.silu(
        (whole_sum - mean) * lax.rsqrt(spread + CHANNEL_FLOOR) * whole_gain
    ).astype(jnp.bfloat16)
    pointwise = jnp.dot(shaped, local_point, preferred_element_type=jnp.float32)
    conv_out = (pointwise * jax.nn.silu(gate_conv)).astype(jnp.bfloat16)
    size = start_state.shape[-1]
    heads = query.shape[1] // size
    span = min(64, length)
    blocks = length // span
    log_keep = -jnp.exp(decay_base + jnp.tanh(decay_in)) * decay_pace.reshape(-1)[:, None]
    key_heads = keys.reshape(length, heads, size)
    unit = key_heads * lax.rsqrt(
        jnp.maximum(jnp.sum(key_heads * key_heads, axis=-1, keepdims=True), 1.0)
    )
    write = unit * correction.reshape(heads, size)

    def arrange(array):
        return array.reshape(blocks, span, heads, size).transpose(2, 0, 1, 3)

    local_out, start_map, carry_map, carry_add = block_terms(
        arrange(query),
        arrange(keys),
        arrange(values),
        arrange(unit),
        arrange(write),
        arrange(log_keep),
    )
    identity = (
        jnp.broadcast_to(jnp.eye(size, dtype=jnp.float32), (heads, size, size)),
        jnp.zeros((heads, size, size), jnp.float32),
    )

    def along(carried, block_pair):
        return (compose(carried, block_pair), carried)

    device_pair, prefixes = lax.scan(
        along, identity, (jnp.moveaxis(carry_map, 1, 0), jnp.moveaxis(carry_add, 1, 0))
    )
    prior_map, prior_add = entering_2(device_pair, "sp", compose, identity)
    begin = start_state.reshape(heads, size, size)
    entering = jnp.matmul(begin, prior_map, precision=lax.Precision.HIGHEST) + prior_add
    block_starts = (
        jnp.matmul(entering[None], prefixes[0], precision=lax.Precision.HIGHEST) + prefixes[1]
    )
    block_starts = jnp.moveaxis(block_starts, 0, 1)
    outputs = local_out + jnp.einsum(
        "hbtk,hbvk->hbtv", start_map, block_starts, precision=lax.Precision.HIGHEST
    )
    outputs = outputs.transpose(1, 2, 0, 3).reshape(length, heads, size)
    centered = outputs - jnp.mean(outputs, axis=-1, keepdims=True)
    variance = jnp.mean(centered * centered, axis=-1, keepdims=True)
    grouped = centered * lax.rsqrt(variance + GROUP_FLOOR) * group_gain.reshape(heads, size)
    state_out = (grouped.reshape(length, heads * size) * jax.nn.silu(gate_state)).astype(
        jnp.bfloat16
    )
    local_mix = jnp.concatenate([conv_out, state_out], axis=1)
    moved = lax.all_to_all(local_mix, "tp", split_axis=0, concat_axis=1, tiled=True)
    conv_rows, state_rows = (
        lax.all_gather(output_conv, "tp", axis=0, tiled=True),
        lax.all_gather(output_state, "tp", axis=0, tiled=True),
    )
    groups = lax.axis_size("tp")
    joined = jnp.concatenate(
        [conv_rows.reshape(groups, channels, -1), state_rows.reshape(groups, heads * size, -1)],
        axis=1,
    )
    joined = joined.reshape(groups * (channels + heads * size), -1)
    mixed = jnp.dot(
        moved,
        lax.all_gather(joined, ("sp", "fs"), axis=1, tiled=True),
        preferred_element_type=jnp.float32,
    )
    return mixed.astype(jnp.bfloat16).reshape(1, -1, width)


def halves(array):
    high = array.astype(jnp.bfloat16)
    low = (array - high.astype(jnp.float32)).astype(jnp.bfloat16)
    return (high, low)


def product(left, right, dims=((1,), (0,))):
    def one(a, b):
        return lax.dot_general(a, b, (dims, ((), ())), preferred_element_type=jnp.float32)

    return one(left[0], right[0]) + (one(left[0], right[1]) + one(left[1], right[0]))


STATES = 5


def layer_kernel(
    span,
    tokens_ref,
    query_ref,
    key_ref,
    value_ref,
    decay_ref,
    gate_ref,
    conv_value_hbm,
    conv_admit_hbm,
    conv_gate_hbm,
    norm_gain_hbm,
    base_hbm,
    strength_hbm,
    group_gain_hbm,
    conv_gain_hbm,
    pace_hbm,
    begin_hbm,
    taps_hbm,
    point_ref,
    out_conv_ref,
    out_state_ref,
    out_ref,
    sequence,
    weights,
    packed,
    conv_pack,
    gate_pack,
    paces,
    gains,
    wout,
    proj,
    pace_col,
    local_ref,
    map_ref,
    carry_ref,
    add_ref,
    conv_ref,
    state_buf,
    side_buf,
    joined,
    sides,
    result,
    t_send,
    t_recv,
    x_send,
    x_recv,
    p_send,
    p_recv,
    w_send,
    w_recv,
    y_send,
    y_recv,
    c_send,
    c_recv,
    r_send,
    r_recv,
    g_send,
    g_recv,
    o_send,
    o_recv,
    oz_send,
    oz_recv,
    oy_send,
    oy_recv,
    on_send,
    on_recv,
    or_send,
    or_recv,
    es_send,
    es_recv,
    ec_send,
    ec_recv,
    xs_send,
    xs_recv,
    xc_send,
    xc_recv,
    f_send,
    f_recv,
    own_sem,
    tokens_in,
    point_in,
    fetched,
    conv_value_ref,
    conv_admit_ref,
    conv_gate_ref,
    norm_gain_ref,
    base_ref,
    strength_ref,
    group_gain_ref,
    conv_gain_ref,
    pace_ref,
    begin_ref,
    taps_ref,
):
    f32 = jnp.float32
    bf16 = jnp.bfloat16
    along = paces.shape[0]
    place = lax.axis_index("sp")
    seat = lax.axis_index("fs")
    side = lax.axis_index("tp")
    other = 1 - side
    near = seat + 1 - 2 * lax.rem(seat, 2)
    far = lax.rem(seat + 2, 4)
    beyond = lax.rem(near + 2, 4)
    row_y = lax.div(seat, 2)
    mine = lax.rem(seat, 2) == side

    length, width = tokens_ref.shape[1:]
    half = length // 2
    total = along * length
    parts = next(n for n in (6, 3, 2, 1) if half % (16 * n) == 0)
    chunk = half // parts
    depth = query_ref.shape[0]
    wide = query_ref.shape[1] // along
    channels = conv_value_ref.shape[1] // along
    size = begin_ref.shape[-1]
    heads = wide // size
    conv_rows = out_conv_ref.shape[0]
    state_rows = out_state_ref.shape[0]
    joint = conv_rows + state_rows
    columns = out_conv_ref.shape[1]
    conv_at = STATES * wide

    pending = []

    def ahead(steps):
        return lax.rem(place + steps, along)

    def behind(steps):
        return lax.rem(place + along - steps, along)

    def aligned(value, size_of):
        return pl.multiple_of(value * size_of, size_of)

    def remote(source, target, send_sem, recv_sem, where):
        return pltpu.make_async_remote_copy(
            src_ref=source,
            dst_ref=target,
            send_sem=send_sem,
            recv_sem=recv_sem,
            device_id=where,
            device_id_type=pl.DeviceIdType.MESH,
        )

    def guarded(valid, action):
        if valid is None:
            action()
        else:
            pl.when(valid)(action)

    def send(source, target, send_sem, recv_sem, where, valid=None, lone=False):
        copy = remote(source, target, send_sem, recv_sem, where)
        guarded(valid, copy.start)
        if lone:
            pending.append((valid, copy))

    def sent(whole, send_sem, where, valid=None):
        pending.append((valid, remote(whole, whole, send_sem, send_sem, where)))

    def arrive(target, send_sem, recv_sem, where, valid=None):
        guarded(valid, remote(target, target, send_sem, recv_sem, where).wait_recv)

    barrier = pltpu.get_barrier_semaphore()
    partners = [{"sp": ahead(s)} for s in range(1, along)]
    partners += [{"fs": near}, {"fs": far}, {"tp": other}]
    for partner in partners:
        pl.semaphore_signal(
            barrier, inc=1, device_id=partner, device_id_type=pl.DeviceIdType.MESH
        )

    state_refs = (query_ref, key_ref, value_ref, decay_ref, gate_ref)

    def rows_of(sp_at, fs_at):
        return pl.ds(aligned(sp_at * 4 + fs_at, depth), depth)

    def packed_of(sp_at, fs_at):
        return pl.ds(aligned(sp_at * 4 + fs_at, depth // 2), depth // 2)

    def fetch(source, target, at):
        pltpu.make_async_copy(source, target, fetched.at[at]).start()

    def fetched_all(target, at):
        pltpu.make_async_copy(target, target, fetched.at[at]).wait()

    own_rows = rows_of(place, seat)
    fetch(tokens_ref.at[0], tokens_in, 0)
    for at, ref in enumerate(state_refs):
        fetch(
            ref.at[:, pl.ds(aligned(place, wide), wide)],
            weights.at[own_rows, pl.ds(at * wide, wide)],
            1,
        )
    fetch(point_ref, point_in, 2)
    small = (
        (conv_value_hbm, conv_value_ref),
        (conv_admit_hbm, conv_admit_ref),
        (conv_gate_hbm, conv_gate_ref),
        (norm_gain_hbm, norm_gain_ref),
        (base_hbm, base_ref),
        (strength_hbm, strength_ref),
        (group_gain_hbm, group_gain_ref),
        (conv_gain_hbm, conv_gain_ref),
        (pace_hbm, pace_ref),
        (begin_hbm, begin_ref),
        (taps_hbm, taps_ref),
    )
    for at, (source, target) in enumerate(small):
        fetch(source, target, 4 + at)

    def small_in(first, last):
        for at in range(first, last):
            fetched_all(small[at][1], 4 + at)

    small_in(0, 3)
    for at in range(along):
        cut = slice(at * channels, (at + 1) * channels)
        conv_pack[at] = jnp.concatenate(
            [conv_value_ref[:, cut].astype(f32), conv_admit_ref[:, cut].astype(f32)], axis=1
        ).astype(bf16)
        gate_pack[at] = jnp.concatenate(
            [
                conv_gate_ref[: depth // 2, cut].astype(f32),
                conv_gate_ref[depth // 2 :, cut].astype(f32),
            ],
            axis=1,
        ).astype(bf16)
    weights[own_rows, conv_at : conv_at + 2 * channels] = conv_pack[place]
    packed[packed_of(place, seat), :] = gate_pack[place]

    tile = 32

    def normalise(turn, _):
        floats = tokens_in[pl.ds(aligned(turn, tile), tile), :].astype(f32)
        inverse = lax.rsqrt(jnp.mean(floats * floats, axis=1, keepdims=True) + NORM_FLOOR)
        at = pl.ds(pl.multiple_of(place * length + turn * tile, tile), tile)
        sequence[at, :] = (floats * inverse * norm_gain_ref[...]).astype(bf16)
        return 0

    def own_block(at):
        return wout.at[:, pl.ds(aligned(at, columns), columns)]

    pl.semaphore_wait(barrier, len(partners))

    def tokens_at(sp_at, side_at, part):
        first = sp_at * length + side_at * half + part * chunk
        return sequence.at[pl.ds(pl.multiple_of(first, 16), chunk)]

    hops = (
        ({"sp": ahead(1)}, lambda d: place >= d, lambda d: behind(d), place < along - 1),
        ({"sp": behind(1)}, lambda d: place + d < along, lambda d: ahead(d), place > 0),
    )

    def half_of(sp_at, side_at):
        first = sp_at * length + side_at * half
        return sequence.at[pl.ds(pl.multiple_of(first, 16), half)]

    own_slot = (place, along)
    def out_piece(side_at, at):
        cut = pl.ds(aligned(at, columns), columns)
        return (
            wout.at[pl.ds(aligned(side_at, joint), conv_rows), cut],
            wout.at[pl.ds(pl.multiple_of(side_at * joint + conv_rows, 16), state_rows), cut],
        )

    own_at = place * 2 + row_y
    theirs = jnp.logical_not(mine)
    def out_half(side_at):
        return wout.at[pl.ds(aligned(side_at, joint), joint), pl.ds(aligned(own_at, columns), columns)]

    sent(out_half(side), o_send.at[0], {"tp": other}, theirs)
    def piece(sp_at, fs_at, at):
        rows = rows_of(sp_at, fs_at)
        if at < STATES:
            return weights.at[rows, pl.ds(at * wide, wide)]
        if at == STATES:
            return weights.at[rows, pl.ds(conv_at, 2 * channels)]
        return packed.at[packed_of(sp_at, fs_at)]

    groups = ((0, 1, 2, 3, 4, 5), (6,))
    kinds = range(len(groups))
    gate_at = conv_at + 2 * channels

    def grouped(sp_at, fs_at, which):
        rows = rows_of(sp_at, fs_at)
        if which == 0:
            return weights.at[rows, pl.ds(0, gate_at)]
        return packed.at[packed_of(sp_at, fs_at)]

    for way, (onward, _, _, open_end) in enumerate(hops):
        sent(half_of(place, side), t_send.at[own_slot[way]], onward, open_end)

    edge = (place == 0) | (place == along - 1)
    inside = jnp.logical_not(edge)

    def tokens_on(d, chosen, here_if):
        for part in chosen:
            for onward, valid, source, open_end in hops:
                at = source(d)
                ready = valid(d) & here_if
                here = tokens_at(at, side, part)
                arrive(here, t_send.at[at], t_recv.at[at, part], onward, ready)
                if d < along - 1:
                    send(here, here, t_send.at[at], t_recv.at[at, part], onward, ready & open_end)
                send(here, here, x_send.at[0], x_recv.at[at], {"tp": other}, ready)

    for d in range(1, along - 1):
        for onward, valid, source, open_end in hops:
            at = source(d)
            sent(half_of(at, side), t_send.at[at], onward, valid(d) & open_end)
    sent(sequence.at[pl.ds(0, (along - 1) * half)], x_send.at[0], {"tp": other})

    def pass_on(at, which, ready=None):
        here = grouped(at, seat, which)
        send(here, here, y_send.at[which], y_recv.at[at, which], {"fs": far}, ready)
        send(here, here, c_send.at[which], c_recv.at[which], {"fs": near}, ready)

    def spread(d, which):
        for onward, valid, source, _ in hops:
            at = source(d)
            here = grouped(at, seat, which)
            arrive(here, w_send.at[which], w_recv.at[at, which], onward, valid(d))
            pass_on(at, which, valid(d))

    def relay(d, which):
        for _, valid, source, _ in hops if d else hops[:1]:
            at = source(d) if d else place
            ready = valid(d) if d else None
            here = grouped(at, far, which)
            arrive(here, y_send.at[which], y_recv.at[at, which], {"fs": far}, ready)
            send(here, here, r_send.at[which], r_recv.at[which], {"fs": near}, ready)

    def several(count, which):
        if which == 0:
            return weights.at[pl.ds(0, count * depth), pl.ds(0, gate_at)]
        return packed.at[pl.ds(0, count * depth // 2)]

    def hand_out(way, d, which):
        target = (ahead, behind)[way](d)
        reach_of = (place + d < along, place >= d)[way]
        for at in groups[which]:
            if at < STATES:
                source = state_refs[at].at[:, pl.ds(aligned(target, wide), wide)]
            elif at == STATES:
                source = conv_pack.at[target]
            else:
                source = gate_pack.at[target]
            send(
                source,
                piece(place, seat, at),
                w_send.at[which],
                w_recv.at[place, which],
                {"sp": target},
                reach_of,
            )

    for d in range(1, along):
        for which in kinds:
            for way in range(2):
                hand_out(way, d, which)
    small_in(3, len(small))
    paces[place] = pace_ref[...]
    gains[side] = conv_gain_ref[...]
    fetched_all(tokens_in, 0)
    lax.fori_loop(0, length // tile, normalise, 0)
    fetched_all(weights.at[own_rows, pl.ds(0, conv_at)], 1)
    for which in kinds:
        pass_on(place, which)
    outward = (inside & (place * 2 >= along), inside & (place * 2 < along))

    def tokens_off(late):
        for part in range(parts):
            for way, (onward, _, _, open_end) in enumerate(hops):
                here = tokens_at(place, side, part)
                wanted = outward[way] if late else jnp.logical_not(outward[way])
                send(
                    here,
                    here,
                    t_send.at[own_slot[way]],
                    t_recv.at[place, part],
                    onward,
                    open_end & wanted,
                )

    tokens_off(False)
    for source, target in zip((out_conv_ref, out_state_ref), out_piece(side, own_at)):
        send(source, target, o_send.at[0], o_recv.at[0], {"tp": other}, theirs)
    for source, target in zip((out_conv_ref, out_state_ref), out_piece(side, own_at)):
        pl.when(mine)(pltpu.make_async_copy(source, target, fetched.at[3]).start)
    own_gain = gains.at[side]
    send(
        conv_gain_ref,
        own_gain,
        g_send.at[0],
        g_recv.at[0],
        {"tp": other},
        lone=True,
    )
    for which in kinds:
        sent(several(along - 1, which), w_send.at[which], {"sp": ahead(1)})
        sent(several(along, which), y_send.at[which], {"fs": far})
        sent(several(along, which), c_send.at[which], {"fs": near})
        sent(several(along, which), r_send.at[which], {"fs": near})
    order = sorted(range(1, along), key=lambda s: min(s, along - s))
    for s in order:
        send(pace_ref, paces.at[place], p_send.at[s], p_recv.at[s], {"sp": ahead(s)}, lone=True)

    third = [range(parts * k // 3, parts * (k + 1) // 3) for k in range(3)]

    def thirds(first, last):
        return [part for k in range(first, last) for part in third[k]]

    def spread_all(d):
        for which in kinds:
            spread(d, which)

    def relay_all(d):
        for which in kinds:
            relay(d, which)

    relay_all(0)
    tokens_off(True)
    spread_all(1)
    spread_all(2)
    relay_all(1)
    tokens_on(1, thirds(0, 2), edge)
    for d in range(3, along):
        spread_all(d)
    for d in range(2, along - 1):
        relay_all(d)
    tokens_on(1, thirds(2, 3), edge)
    tokens_on(1, thirds(0, 1), inside)
    relay_all(along - 1)
    tokens_on(2, thirds(0, 1), edge)
    tokens_on(1, thirds(1, 3), inside)

    def out_off():
        arrive(out_half(other), o_send.at[0], o_recv.at[0], {"tp": other}, mine)
        pl.when(mine)(
            pltpu.make_async_copy(out_half(side), out_half(side), fetched.at[3]).wait
        )
        for d in range(1, along):
            for part in range(2):
                here = own_part(own_at, part)
                for way in range(2):
                    target = (ahead, behind)[way](d)
                    reach_of = (place + d < along, place >= d)[way]
                    send(
                        here,
                        here,
                        oz_send.at[0],
                        oz_recv.at[place, part],
                        {"sp": target},
                        mine & reach_of if d == 1 else mine & reach_of & edge,
                    )

    def own_part(at, part):
        return wout.at[pl.ds(part * joint, joint), pl.ds(aligned(at, columns), columns)]

    def out_near(at, ready, part):
        here = own_part(at * 2 + row_y, part)
        send(here, here, oy_send.at[0], oy_recv.at[at, part], {"fs": far}, ready)
        send(here, here, on_send.at[0], on_recv.at[at], {"fs": near}, ready)

    def out_on(d, chosen=(0, 1)):
        for onward, valid, source, open_end in hops:
            at = source(d)
            ready = mine & valid(d)
            for part in chosen:
                arrive(
                    own_part(at * 2 + row_y, part), oz_send.at[0], oz_recv.at[at, part], onward, ready
                )
                if d == 1:
                    here = own_part(at * 2 + row_y, part)
                    between = (at > 0) & (at < along - 1) & open_end
                    send(
                        here,
                        here,
                        oz_send.at[0],
                        oz_recv.at[at, part],
                        onward,
                        ready & between,
                    )
                out_near(at, ready, part)

    def out_over(d, here_if=True):
        for _, valid, source, _ in hops if d else hops[:1]:
            at = source(d) if d else place
            ready = mine & valid(d) & here_if if d else mine
            for part in range(2):
                here = own_part(at * 2 + 1 - row_y, part)
                arrive(here, oy_send.at[0], oy_recv.at[at, part], {"fs": far}, ready)
                send(here, here, or_send.at[0], or_recv.at[at], {"fs": near}, ready)

    every = wout.at[:, pl.ds(0, along * columns)]

    def settled(which):
        arrive(several(along, which), c_send.at[which], c_recv.at[which], {"fs": near})
        arrive(several(along, which), r_send.at[which], r_recv.at[which], {"fs": near})

    for s in order:
        arrive(paces.at[behind(s)], p_send.at[s], p_recv.at[s], {"sp": ahead(s)})
    blocks = total // span
    row = lax.broadcasted_iota(jnp.int32, (span, span), 0)
    col = lax.broadcasted_iota(jnp.int32, (span, span), 1)
    eye = (row == col).astype(f32)
    for at in range(along):
        for part in range(length // span):
            line = paces[at][:, part * span : (part + 1) * span]
            first = at * length + part * span
            pace_col[first : first + span, :] = jnp.sum(eye * line, axis=1, keepdims=True)
    for which in kinds:
        settled(which)

    def unpack(turn, _):
        both = packed[pl.ds(aligned(turn, depth // 2), depth // 2), :].astype(f32)
        at = pl.ds(aligned(turn, depth), depth // 2)
        weights[at, gate_at : gate_at + channels] = both[:, :channels].astype(bf16)
        at = pl.ds(pl.multiple_of(turn * depth + depth // 2, depth // 2), depth // 2)
        weights[at, gate_at : gate_at + channels] = both[:, channels:].astype(bf16)
        return 0

    lax.fori_loop(0, along * 4, unpack, 0)


    begins = [begin_ref[0, place * heads + head] for head in range(heads)]
    own_cut = pl.ds(aligned(place, wide), wide)
    base = base_ref[:, own_cut]
    strength = strength_ref[:, own_cut]
    gain = group_gain_ref[:, own_cut]

    strict = (row > col).astype(f32)
    weak = (row >= col).astype(f32)
    masks = jnp.concatenate(
        [jnp.concatenate([strict, strict], axis=1), jnp.concatenate([weak, weak], axis=1)], axis=0
    )
    square = (
        lax.broadcasted_iota(jnp.int32, (size, size), 0)
        == lax.broadcasted_iota(jnp.int32, (size, size), 1)
    ).astype(f32)
    least = min(8, span)
    same = (lax.div(row, least) == lax.div(col, least)).astype(f32)
    merges = []
    reach = least
    while reach < span:
        merges.append(
            (
                (lax.div(row, 2 * reach) == lax.div(col, 2 * reach))
                & (lax.div(row, reach) != lax.div(col, reach))
            ).astype(f32)
        )
        reach = 2 * reach
    weak_bf = weak.astype(bf16)

    def step(turn):
        items = []
        for part in range(length // span):
            block = turn * (length // span) + part
            rows = pl.ds(pl.multiple_of(block * span, span), span)
            query = proj[rows, 0:wide].astype(f32)
            keys = proj[rows, wide : 2 * wide].astype(f32)
            values = proj[rows, 2 * wide : 3 * wide].astype(f32)
            decay_in = proj[rows, 3 * wide : 4 * wide].astype(f32)
            log_keep = -jnp.exp(base + jnp.tanh(decay_in)) * pace_col[rows, :]
            high = log_keep.astype(bf16)
            rest = log_keep - high.astype(f32)
            mid = rest.astype(bf16)
            low = (rest - mid.astype(f32)).astype(bf16)
            summed = (
                jnp.dot(weak_bf, high, preferred_element_type=f32)
                + jnp.dot(weak_bf, mid, preferred_element_type=f32)
                + jnp.dot(weak_bf, low, preferred_element_type=f32)
            )
            last = summed[span - 1 : span, :]
            lead = jnp.exp(summed - log_keep)
            grown = jnp.exp(summed)
            back = jnp.exp(-summed)
            tail = jnp.exp(last - summed)
            ended = jnp.exp(last)
            for head in range(heads):
                at = slice(head * size, (head + 1) * size)
                key = keys[:, at]
                unit = key * lax.rsqrt(
                    jnp.maximum(jnp.sum(key * key, axis=1, keepdims=True), 1.0)
                )
                write = unit * strength[:, at]
                lead_remove = -unit * lead[:, at]
                lead_query = query[:, at] * grown[:, at]
                items.append(
                    dict(
                        at=(block, head),
                        value=values[:, at],
                        lead_remove=lead_remove,
                        lead_query=lead_query,
                        left=jnp.concatenate([lead_remove, lead_query], axis=0),
                        right=jnp.concatenate([write * back[:, at], key * back[:, at]], axis=0),
                        tail_write=write * tail[:, at],
                        tail_key=key * tail[:, at],
                        ended=ended[:, at],
                    )
                )
        for item in items:
            item["pair"] = (
                product(halves(item["left"]), halves(item["right"]), ((1,), (1,))) * masks
            )
        for item in items:
            item["system"] = item["pair"][:span, :span]
            item["power"] = halves(item["system"] * same)
            item["inverse"] = eye + item["system"] * same
        reach = 2
        while reach < least:
            for item in items:
                item["power"] = halves(product(item["power"], item["power"]))
            for item in items:
                item["inverse"] = item["inverse"] + product(
                    halves(item["inverse"]), item["power"]
                )
            reach = 2 * reach
        for item in items:
            padded = jnp.concatenate([jnp.zeros_like(item["value"]), item["value"]], axis=0)
            item["mixed"] = product(halves(item["pair"]), halves(padded))
        for merge in merges:
            for item in items:
                item["inside"] = halves(item["inverse"])
                item["next"] = halves(product(halves(item["system"] * merge), item["inside"]))
            for item in items:
                item["inverse"] = item["inverse"] + product(item["inside"], item["next"])
        for item in items:
            right_side = jnp.concatenate([item["mixed"][:span], item["lead_remove"]], axis=1)
            item["solved"] = halves(product(halves(item["inverse"]), halves(right_side)))
        for item in items:
            block, head = item["at"]
            seen = product(halves(item["pair"][span:, :span]), item["solved"])
            local_ref[head, block] = seen[:, :size] + item["mixed"][span:]
            map_ref[head, block] = item["lead_query"] + seen[:, size:]
            carried = product(item["solved"], halves(item["tail_write"]), ((0,), (0,)))
            carry_ref[head, block] = carried[size:] + square * item["ended"]
            add_ref[head, block] = carried[:size] + product(
                halves(item["value"]), halves(item["tail_key"]), ((0,), (0,))
            )

    def rows_for(at):
        return pl.ds(at * length, length)

    def convolve():
        kernel = taps_ref.shape[0]
        lead_rows = conv_ref.shape[0] - total
        pair = pl.ds(aligned(lax.div(place * channels, 128), 128), 128)
        both_taps = taps_ref[:, pair]
        taps = jnp.where(
            lax.rem(place * channels, 128) == 0, both_taps[:, :channels], both_taps[:, 128 - channels :]
        )
        conv_ref[0:lead_rows, :] = jnp.zeros((lead_rows, channels), f32)
        for block in range(blocks):
            rows = pl.ds(block * span, span)
            value = proj[rows, conv_at : conv_at + channels].astype(f32)
            admit = proj[rows, conv_at + channels : conv_at + 2 * channels].astype(f32)
            conv_ref[pl.ds(lead_rows + block * span, span), :] = (
                (value * jax.nn.sigmoid(admit)).astype(bf16).astype(f32)
            )
        for block in range(blocks):
            summed = jnp.zeros((span, channels), f32)
            for tap in range(kernel):
                first = lead_rows - (kernel - 1) + block * span + tap
                summed = summed + taps[tap : tap + 1, :] * conv_ref[pl.ds(first, span), :]
            rows = pl.ds(block * span, span)
            gate = proj[rows, gate_at : gate_at + channels].astype(f32)
            side_buf[rows, :] = jnp.concatenate([summed, gate], axis=1).astype(bf16)

        for at in range(along):
            target = sides.at[side, place]

            @pl.when(place == at)
            def _():
                sides[side, place] = side_buf[rows_for(at), :]

            away = place != at
            send(
                side_buf.at[rows_for(at)], target, ec_send.at[0], ec_recv.at[place], {"sp": at}, away
            )
            send(
                side_buf.at[rows_for(at)],
                target,
                xc_send.at[0],
                xc_recv.at[0],
                {"tp": other},
                place == at,
            )

    tables = [sorted(range(along), key=lambda q: abs(q - p)) for p in range(along)]

    def turn_of(k):
        found = tables[0][k]
        for p in range(1, along):
            found = jnp.where(place == p, tables[p][k], found)
        return found

    def mix(k, between=None):
        at = turn_of(k)
        if k:
            arrive(half_of(at, other), x_send.at[0], x_recv.at[at], {"tp": other})
        rows = pl.ds(aligned(at, length), length)
        proj[rows, :] = jnp.dot(
            sequence[rows, :], weights[...], preferred_element_type=f32
        ).astype(bf16)
        if between is not None:
            between()
        step(at)

    tokens_on(2, thirds(1, 2), edge)
    tokens_on(2, thirds(0, 1), inside)
    mix(0)
    tokens_on(2, thirds(2, 3), edge)
    tokens_on(2, thirds(1, 3), inside)
    out_off()
    for part in range(2):
        out_near(place, mine, part)
    def first_far():
        for d in range(3, along):
            tokens_on(d, thirds(0, 1), edge)

    mix(1, first_far)
    for d in range(3, along):
        tokens_on(d, thirds(1, 2), edge)
    for k in range(2, along - 1):
        mix(k)
    for d in range(3, along):
        tokens_on(d, thirds(2, 3), edge)
    out_over(0)
    out_on(1)
    mix(along - 1)
    convolve()

    def joined_at(side_at, sp_at):
        first = side_at * joint + conv_rows + sp_at * wide
        return joined.at[:, pl.ds(pl.multiple_of(first, 128), wide)]

    states = list(begins)
    for block in range(blocks):
        rows = pl.ds(block * span, span)
        gate = proj[rows, 4 * wide : 5 * wide].astype(f32)
        pieces = []
        for head in range(heads):
            state = halves(states[head])
            out = local_ref[head, block] + product(
                halves(map_ref[head, block]), state, ((1,), (1,))
            )
            states[head] = product(state, halves(carry_ref[head, block])) + add_ref[head, block]
            centered = out - jnp.mean(out, axis=1, keepdims=True)
            variance = jnp.mean(centered * centered, axis=1, keepdims=True)
            pieces.append(centered * lax.rsqrt(variance + GROUP_FLOOR))
        scaled = jnp.concatenate(pieces, axis=1) * gain
        state_buf[rows, :] = (scaled * gate * jax.nn.sigmoid(gate)).astype(bf16)
        if (block + 1) * span % length == 0:
            at = (block + 1) * span // length - 1
            target = joined_at(side, place)

            @pl.when(place == at)
            def _():
                joined[:, pl.ds(
                    pl.multiple_of(side * joint + conv_rows + place * wide, 128), wide
                )] = state_buf[rows_for(at), :]

            source = state_buf.at[rows_for(at)]
            send(source, target, es_send.at[0], es_recv.at[place], {"sp": at}, place != at)
            send(
                source,
                target,
                xs_send.at[0],
                xs_recv.at[0],
                {"tp": other},
                place == at,
            )

    for d in range(2, along - 1):
        out_on(d)
    for s in order:
        here = sides.at[side, behind(s)]
        arrive(here, ec_send.at[0], ec_recv.at[behind(s)], {"sp": ahead(s)})
        send(here, here, xc_send.at[0], xc_recv.at[0], {"tp": other})

    out_on(along - 1)
    out_over(1)
    for s in order:
        here = joined_at(side, behind(s))
        arrive(here, es_send.at[0], es_recv.at[behind(s)], {"sp": ahead(s)})
        send(here, here, xs_send.at[0], xs_recv.at[0], {"tp": other})
    arrive(sides.at[other], xc_send.at[0], xc_recv.at[0], {"tp": other})
    arrive(gains.at[other], g_send.at[0], g_recv.at[0], {"tp": other})
    whole_gain = jnp.concatenate([gains[0], gains[1]], axis=1)
    piece_rows = next(n for n in (64, 48, 32, 16) if length % n == 0)

    def convolved(turn, _):
        at = pl.ds(aligned(turn, piece_rows), piece_rows)
        sums = jnp.concatenate(
            [
                sides[s, p, at, 0:channels].astype(f32)
                for s in range(2)
                for p in range(along)
            ],
            axis=1,
        )
        gates = jnp.concatenate(
            [
                sides[s, p, at, channels : 2 * channels].astype(f32)
                for s in range(2)
                for p in range(along)
            ],
            axis=1,
        )
        mean = jnp.mean(sums, axis=1, keepdims=True)
        spread_of = jnp.mean(sums * sums, axis=1, keepdims=True) - mean * mean
        shaped = jax.nn.silu(
            (sums - mean) * lax.rsqrt(spread_of + CHANNEL_FLOOR) * whole_gain
        ).astype(bf16)
        pointwise = jnp.dot(shaped, point_in[...], preferred_element_type=f32)
        conv_out = (pointwise * jax.nn.silu(gates)).astype(bf16)
        joined[at, 0:conv_rows] = conv_out[:, :conv_rows]
        joined[at, joint : joint + conv_rows] = conv_out[:, conv_rows:]
        return 0

    fetched_all(point_in, 2)
    lax.fori_loop(0, length // piece_rows, convolved, 0)

    arrive(state_buf, xs_send.at[0], xs_recv.at[0], {"tp": other})

    ours = pl.ds(pl.multiple_of(side * half, 16), half)
    others = pl.ds(pl.multiple_of(other * half, 16), half)

    def out_cut(at, side_at):
        return pl.ds(aligned(2 * at + side_at, columns), columns)

    for k in range(along):
        zone = turn_of(k)
        if 1 < k < along - 1:
            out_over(k, edge)
        if k == along - 1:
            for d in range(2, k):
                out_over(d, inside)
            out_over(k)
        arrive(
            own_block(zone * 2 + row_y), on_send.at[0], on_recv.at[zone], {"fs": near}, theirs
        )
        arrive(
            own_block(zone * 2 + 1 - row_y), or_send.at[0], or_recv.at[zone], {"fs": near}, theirs
        )
        cut = pl.ds(aligned(zone, 2 * columns), 2 * columns)
        result[:, cut] = jnp.dot(joined[...], wout[:, cut], preferred_element_type=f32).astype(bf16)
        for at in (zone * 2, zone * 2 + 1):
            piece_cut = pl.ds(aligned(at, columns), columns)
            send(
                result.at[others, piece_cut],
                out_ref.at[:, out_cut(at, side)],
                f_send.at[0],
                f_recv.at[0],
                {"tp": other},
            )
            pltpu.make_async_copy(
                result.at[ours, piece_cut], out_ref.at[:, out_cut(at, side)], own_sem.at[0]
            ).start()
    halfway = result.at[pl.ds(0, half)]
    arrive(halfway, f_send.at[0], f_recv.at[0], {"tp": other})
    pltpu.make_async_copy(halfway, halfway, own_sem.at[0]).wait()
    away_rows = pl.ds(0, (along - 1) * length)
    sent(side_buf.at[away_rows], ec_send.at[0], {"sp": ahead(1)})
    sent(state_buf.at[away_rows], es_send.at[0], {"sp": ahead(1)})
    sent(side_buf, xc_send.at[0], {"tp": other})
    sent(state_buf, xs_send.at[0], {"tp": other})
    sent(wout.at[:, pl.ds(0, (along - 1) * columns)], oz_send.at[0], {"sp": ahead(1)}, mine)
    sent(every, oy_send.at[0], {"fs": far}, mine)
    sent(every, on_send.at[0], {"fs": near}, mine)
    sent(every, or_send.at[0], {"fs": near}, mine)
    sent(halfway, f_send.at[0], {"tp": other})
    for valid, copy in pending:
        guarded(valid, copy.wait_send)


def fused_body(
    tokens,
    decay_pace,
    start_state,
    norm_gain,
    conv_value,
    conv_admit,
    conv_gate,
    state_query,
    state_key,
    state_value,
    state_decay,
    state_gate,
    conv_taps,
    conv_gain,
    point_weight,
    decay_base,
    correction,
    group_gain,
    output_conv,
    output_state,
):
    along = lax.axis_size("sp")
    _, length, width = tokens.shape
    depth, wide = state_query.shape[0], state_query.shape[1] // along
    channels = conv_value.shape[1] // along
    size = start_state.shape[-1]
    heads = wide // size
    total = along * length
    span = 64
    blocks = total // span
    kernel = conv_taps.shape[0]
    joint = output_conv.shape[0] + output_state.shape[0]
    columns = output_conv.shape[1]
    gain_lanes = conv_gain.shape[0]
    f32, bf16 = jnp.float32, jnp.bfloat16
    half = length // 2
    parts = next(n for n in (6, 3, 2, 1) if half % (16 * n) == 0)
    lead_rows = -(-(kernel - 1) // 8) * 8
    dma = pltpu.SemaphoreType.DMA
    maps = pltpu.VMEM((heads, blocks, size, size), f32)
    wout_blocks = along * 2

    def both(*shape):
        return [dma(shape), dma(shape)]

    mixed = pl.pallas_call(
        functools.partial(layer_kernel, span),
        out_shape=jax.ShapeDtypeStruct((half, width), bf16),
        in_specs=[pl.BlockSpec(memory_space=pl.ANY)] * 20,
        out_specs=pl.BlockSpec(memory_space=pl.ANY),
        scratch_shapes=[
            pltpu.VMEM((total, width), bf16),
            pltpu.VMEM((width, 5 * wide + 3 * channels), bf16),
            pltpu.VMEM((width // 2, 2 * channels), bf16),
            pltpu.VMEM((along, depth, 2 * channels), bf16),
            pltpu.VMEM((along, depth // 2, 2 * channels), bf16),
            pltpu.VMEM((along, 1, length), f32),
            pltpu.VMEM((2, 1, gain_lanes), f32),
            pltpu.VMEM((2 * joint, wout_blocks * columns), bf16),
            pltpu.VMEM((total, 5 * wide + 3 * channels), bf16),
            pltpu.VMEM((total, 1), f32),
            pltpu.VMEM((heads, blocks, span, size), f32),
            pltpu.VMEM((heads, blocks, span, size), f32),
            maps,
            maps,
            pltpu.VMEM((lead_rows + total, channels), f32),
            pltpu.VMEM((total, wide), bf16),
            pltpu.VMEM((total, 2 * channels), bf16),
            pltpu.VMEM((length, 2 * joint), bf16),
            pltpu.VMEM((2, along, length, 2 * channels), bf16),
            pltpu.VMEM((length, wout_blocks * columns), bf16),
        ]
        + [dma((along + 1,)), dma((along, parts))]
        + [dma((1,)), dma((along,))]
        + both(along)
        + [dma((2,)), dma((along, 2))]
        + [dma((2,)), dma((along, 2))]
        + both(2)
        + both(2)
        + both(1)
        + both(1)
        + [dma((1,)), dma((along, 2))]
        + [dma((1,)), dma((along, 2))]
        + [dma((1,)), dma((along,))]
        + [dma((1,)), dma((along,))]
        + [dma((1,)), dma((along,))]
        + [dma((1,)), dma((along,))]
        + both(1)
        + both(1)
        + both(1)
        + [dma((1,))]
        + [
            pltpu.VMEM((length, width), bf16),
            pltpu.VMEM(point_weight.shape, bf16),
            dma((15,)),
            pltpu.VMEM(conv_value.shape, bf16),
            pltpu.VMEM(conv_admit.shape, bf16),
            pltpu.VMEM(conv_gate.shape, bf16),
            pltpu.VMEM((1, width), f32),
            pltpu.VMEM((1, decay_base.shape[0]), f32),
            pltpu.VMEM((1, correction.shape[0]), f32),
            pltpu.VMEM((1, group_gain.shape[0]), f32),
            pltpu.VMEM((1, gain_lanes), f32),
            pltpu.VMEM(decay_pace.shape, f32),
            pltpu.VMEM(start_state.shape, f32),
            pltpu.VMEM(conv_taps.shape, f32),
        ],
        compiler_params=pltpu.CompilerParams(
            collective_id=0, has_side_effects=True, vmem_limit_bytes=56 * 1024 * 1024
        ),
        cost_estimate=pl.CostEstimate(
            flops=60_000_000_000, bytes_accessed=8_000_000, transcendentals=0
        ),
        name="layer",
    )(
        tokens,
        state_query,
        state_key,
        state_value,
        state_decay,
        state_gate,
        conv_value,
        conv_admit,
        conv_gate,
        norm_gain[None],
        decay_base[None],
        correction[None],
        group_gain[None],
        conv_gain[None],
        decay_pace,
        start_state,
        conv_taps,
        point_weight,
        output_conv,
        output_state,
    )
    return mixed.reshape(1, half, width)


def dispatch(*arrays):
    along = lax.axis_size("sp")
    tokens, start_state, conv_value, query, output_conv, output_state = (
        arrays[0],
        arrays[2],
        arrays[4],
        arrays[7],
        arrays[18],
        arrays[19],
    )
    depth, width = query.shape[0], tokens.shape[2]
    size = start_state.shape[-1]
    fits = (
        along == 4
        and lax.axis_size("fs") == 4
        and lax.axis_size("tp") == 2
        and tokens.shape[1] % 64 == 0
        and tokens.shape[0] == 1
        and start_state.shape[1] % along == 0
        and size == 64
        and query.shape[1] == along * 128
        and conv_value.shape[1] == along * 64
        and depth % 32 == 0
        and depth * along * 4 == width
        and output_conv.shape[0] == along * 64
        and output_state.shape[0] == along * 128
        and output_conv.shape[1] == 128
        and width == along * 4 * 128
    )
    return (fused_body if fits else body)(*arrays)


def solution(mesh):
    return jax.shard_map(
        dispatch,
        mesh=mesh,
        in_specs=(
            P("fs", "sp", None),
            P("fs", "sp"),
            P("fs", "tp", None, None),
            P(),
            P(("sp", "fs"), "tp"),
            P(("sp", "fs"), "tp"),
            P(("sp", "fs"), "tp"),
            P(("sp", "fs"), "tp"),
            P(("sp", "fs"), "tp"),
            P(("sp", "fs"), "tp"),
            P(("sp", "fs"), "tp"),
            P(("sp", "fs"), "tp"),
            P(None, "tp"),
            P("tp"),
            P(),
            P("tp"),
            P("tp"),
            P("tp"),
            P("tp", ("sp", "fs")),
            P("tp", ("sp", "fs")),
        ),
        out_specs=P("fs", ("sp", "tp"), None),
        check_vma=False,
    )
```
